32 devices in a mesh: grp: 2 (over y), sp: 4 (over z), tp: 4 (over x, core).
Axes of the slice: x: 2, y: 2, z: 4, core: 2. Of those that a mesh axis runs over, the one named last changes fastest.
Arguments:
- tokens: bfloat16 [256, 8, 2048], P(('sp', 'tp'), 'grp'), parts along dimension 1, may hold values from -6 to 6
- norm_gain: float32 [2048], replicated, may hold values from 0.1 to 1.9
- w_query: bfloat16 [2048, 2048], P('sp', 'tp'), may hold values from -0.125 to 0.125
- w_value: bfloat16 [2048, 2048], P('sp', 'tp'), may hold values from -0.125 to 0.125
- w_fwd_gate: bfloat16 [2048, 2048], P('sp', 'tp'), may hold values from -0.125 to 0.125
- w_bwd_gate: bfloat16 [2048, 2048], P('sp', 'tp'), may hold values from -0.125 to 0.125
- w_out_gate: bfloat16 [2048, 2048], P('sp', 'tp'), may hold values from -0.125 to 0.125
- floor_gap: float32 [2, 2048], P(None, 'tp'), may hold values from 0.00078125 to 0.1
- decay_shift: float32 [256, 8, 2048], P('sp', 'grp', 'tp'), parts along dimension 1, may hold values from -1.1 to 0
- head_gain: float32 [128], replicated, may hold values from 0.1 to 1.9
- w_out: bfloat16 [2048, 2048], P('tp', 'sp'), may hold values from -0.125 to 0.125
Outputs:
- layer_out: bfloat16 [256, 8, 2048], P(('sp', 'tp'), 'grp'), parts along dimension 1
The draws below stay inside these ranges and needn't reach their ends.
There are 2 independent parts, one for each index of `grp`. The reference program is written for one: setup_inputs(seed, part) draws one part's arguments, and reference() takes and returns one part's arrays. A program takes and returns all parts, laid end to end along the dimension named above; an argument that names none is the same for every part. Nothing has to cross between parts.
All inputs are finite; a program needn't handle non-finite values.
Results may differ from the reference program's by a relative error of at most 0.013.
Values may be sent and summed in bfloat16 or wider, within the bound.
A program may use at most 128 MiB of HBM per device.

```python
import math
import jax
import jax.numpy as jnp
from jax import lax

D = 2048
HEADS = 16
KEY = 128
VAL = 128
SEQS = 4
SPAN = 64
TOKENS = 256
N_TP = 4


def draw_floor_gap(key, part):
    key_order, key_count, key_slow, key_fast = jax.random.split(key, 4)
    head_ranks = jax.random.permutation(key_order, HEADS)
    slow_count = jax.random.randint(key_count, (), 2, HEADS - 1)
    slow_heads = jnp.repeat(head_ranks < slow_count, KEY)[None, :]
    slow_gap = jnp.exp(jax.random.uniform(key_slow, (2, HEADS * KEY), jnp.float32, math.log(0.2), math.log(0.8))) / TOKENS
    fast_gap = jnp.exp(jax.random.uniform(key_fast, (2, HEADS * KEY), jnp.float32, math.log(0.03), math.log(0.1)))
    return jnp.where(slow_heads, slow_gap, fast_gap).astype(jnp.float32)


def draw_decay_shift(key, part):
    key_block, key_chan, key_place, key_depth = jax.random.split(key, 4)
    block_rate = jnp.exp(jax.random.uniform(key_block, (TOKENS // SPAN, SEQS, 1), jnp.float32, math.log(0.5), math.log(2.0)))
    channel_rate = jnp.exp(jax.random.uniform(key_chan, (1, 1, HEADS * KEY), jnp.float32, math.log(0.3), 0.0))
    stable_regime = -(0.5 / TOKENS) * jnp.repeat(block_rate, SPAN, axis=0) * channel_rate
    seat_indices = jax.random.randint(key_place, (2, SEQS), 0, TOKENS)
    layer_tiers = jax.random.uniform(key_depth, (2, SEQS), jnp.float32, math.log(0.6), math.log(0.8))
    location_indices = jnp.arange(TOKENS)[:, None]
    cluster_tally = jnp.where(location_indices == seat_indices[0][None, :], layer_tiers[0][None, :], 0.0)
    cluster_tally = cluster_tally + jnp.where(location_indices == seat_indices[1][None, :], layer_tiers[1][None, :], 0.0)
    return (stable_regime + cluster_tally[:, :, None]).astype(jnp.float32)


def steps_of(key, extent, cuts, least, top_value):
    factor_of, own = 1.0, jax.random.fold_in(key, 6)
    for position, parts in cuts:
        draws = jnp.exp(jax.random.uniform(jax.random.fold_in(own, position), (parts,), jnp.float32, least / len(cuts), top_value / len(cuts)))
        factor_of = factor_of * jnp.repeat(draws, extent[position] // parts).reshape([-1 if axis == position else 1 for axis in range(len(extent))])
    return factor_of


def gaussian(stream_key, extent, deviation, reach, cuts=(), dtype=jnp.bfloat16):
    level = steps_of(stream_key, extent, cuts, -0.22, 0.18) if cuts else 1.0
    entries = jax.random.normal(stream_key, extent, jnp.float32) * deviation * level
    return jnp.minimum(jnp.maximum(entries, -reach), reach).astype(dtype)


def setup_inputs(seed: int = 0, part: int = 0) -> dict:
    splits = jax.random.split(jax.random.key(seed), 12)
    part_splits = jax.random.split(jax.random.fold_in(splits[11], part), 12)
    tokens = gaussian(part_splits[0], (TOKENS, SEQS, D), 1.0, 6.0, ((0, 16),))
    norm_gain = jnp.clip(1.0 + 0.18 * jax.random.normal(splits[1], (D,), jnp.float32), 0.1, 1.9)
    w_query = gaussian(splits[2], (D, HEADS * KEY), D ** -0.5, 0.125, ((0, 4), (1, 4)))
    w_value = gaussian(splits[3], (D, HEADS * VAL), D ** -0.5, 0.125, ((0, 4), (1, 4)))
    w_fwd_gate = gaussian(splits[4], (D, HEADS * KEY), D ** -0.5, 0.125, ((0, 4), (1, 4)))
    w_bwd_gate = gaussian(splits[5], (D, HEADS * KEY), D ** -0.5, 0.125, ((0, 4), (1, 4)))
    w_out_gate = gaussian(splits[6], (D, HEADS * VAL), D ** -0.5, 0.125, ((0, 4), (1, 4)))
    floor_gap = draw_floor_gap(jax.random.fold_in(splits[11], 71), part)
    decay_shift = draw_decay_shift(jax.random.fold_in(jax.random.fold_in(splits[11], part), 71), part)
    head_gain = jnp.clip(1.0 + 0.18 * jax.random.normal(splits[9], (VAL,), jnp.float32), 0.1, 1.9)
    w_out = gaussian(splits[10], (HEADS * VAL, D), (HEADS * VAL) ** -0.5, 0.125, ((0, 4), (1, 4)))
    return {"tokens": tokens, "norm_gain": norm_gain, "w_query": w_query, "w_value": w_value, "w_fwd_gate": w_fwd_gate, "w_bwd_gate": w_bwd_gate, "w_out_gate": w_out_gate, "floor_gap": floor_gap, "decay_shift": decay_shift, "head_gain": head_gain, "w_out": w_out}


norm_eps = 1e-06
highest = lax.Precision.HIGHEST

def chain_scan(queries, key_cols, values, log_decay, backward):

    def advance(carry_state, inputs):
        query_now, key_now, value_now, decay_now = inputs
        carry_state = jnp.exp(decay_now)[..., None] * carry_state + key_now[..., None] * value_now[..., None, :]
        return (carry_state, jnp.einsum('bhk,bhke->bhe', query_now, carry_state, precision=highest))
    start_state = jnp.zeros((SEQS, HEADS, KEY, VAL), jnp.float32)
    _, outputs = lax.scan(advance, start_state, (queries, key_cols, values, log_decay), reverse=backward)
    return outputs

def reference(tokens, norm_gain, w_query, w_value, w_fwd_gate, w_bwd_gate, w_out_gate, floor_gap, decay_shift, head_gain, w_out):
    token_f32 = tokens.astype(jnp.float32)
    scale_rows = lax.rsqrt(lax.optimization_barrier(jnp.mean(token_f32 * token_f32, axis=-1, keepdims=True)) + norm_eps)
    normed = (token_f32 * scale_rows * norm_gain.astype(jnp.float32)).astype(jnp.bfloat16)
    flat_rows = normed.reshape(TOKENS * SEQS, D)

    def project(matrix):
        rounded = jnp.dot(flat_rows, matrix, preferred_element_type=jnp.float32).astype(jnp.bfloat16)
        return lax.optimization_barrier(rounded).astype(jnp.float32)
    queries = jax.nn.silu(project(w_query)).reshape(TOKENS, SEQS, HEADS, KEY)
    values = project(w_value).reshape(TOKENS, SEQS, HEADS, VAL)
    shift = decay_shift.reshape(TOKENS, SEQS, HEADS, KEY)
    gap_fwd = floor_gap[0].reshape(HEADS, KEY)
    gap_bwd = floor_gap[1].reshape(HEADS, KEY)
    key_fwd = gap_fwd * jax.nn.sigmoid(-project(w_fwd_gate).reshape(TOKENS, SEQS, HEADS, KEY))
    key_bwd = gap_bwd * jax.nn.sigmoid(-project(w_bwd_gate).reshape(TOKENS, SEQS, HEADS, KEY))
    decay_fwd = jnp.log1p(-key_fwd) + shift
    decay_bwd = jnp.log1p(-key_bwd) + shift
    combined = chain_scan(queries, key_fwd, values, decay_fwd, False) + chain_scan(queries, key_bwd, values, decay_bwd, True)
    head_normed = combined * lax.rsqrt(lax.optimization_barrier(jnp.mean(combined * combined, axis=-1, keepdims=True)) + norm_eps) * head_gain.astype(jnp.float32)
    gate_value = jax.nn.silu(project(w_out_gate))
    mixed = (head_normed.reshape(TOKENS * SEQS, HEADS * VAL) * gate_value).astype(jnp.bfloat16)
    group_width = HEADS * VAL // N_TP
    accumulated_total = jnp.zeros((TOKENS * SEQS, D), jnp.float32)
    for tp_group in range(N_TP):
        first_column = tp_group * group_width
        partial_value = jnp.dot(mixed[:, first_column:first_column + group_width], w_out[first_column:first_column + group_width], preferred_element_type=jnp.float32).astype(jnp.bfloat16)
        accumulated_total = accumulated_total + lax.optimization_barrier(partial_value).astype(jnp.float32)
    return accumulated_total.astype(jnp.bfloat16).reshape(TOKENS, SEQS, D)
```

```python
import functools

import jax
import jax.numpy as jnp
from jax import lax
from jax.experimental import pallas as pl
from jax.experimental.pallas import tpu as pltpu
from jax.sharding import PartitionSpec as P

KEY = 128
VAL = 128
BLOCK = 64


norm_eps = 1e-06
highest = lax.Precision.HIGHEST


def carried_in(x, axis, join, neutral, backward):
    count = lax.axis_size(axis)
    place = lax.axis_index(axis)
    ahead = count - 1 - place if backward else place
    gathered = jax.tree.map(
        lambda a, kind: lax.all_gather(a.astype(kind), axis), x, (jnp.bfloat16, jnp.bfloat16)
    )
    state = jax.tree.map(lambda a, e: jnp.zeros_like(a) + jnp.asarray(e, a.dtype), x, neutral)

    def one(turn, state):
        source = count - 1 - turn if backward else turn
        return join(
            state,
            jax.tree.map(
                lambda a, own: lax.dynamic_index_in_dim(a, source, 0, False).astype(own.dtype),
                gathered,
                x,
            ),
        )

    return lax.fori_loop(0, ahead, one, state)


def split_blocks(array):
    return array.reshape(array.shape[0] // BLOCK, BLOCK, *array.shape[1:])


def prepare_chain(queries, key_cols, values, log_decay):
    query_blocks = split_blocks(queries)
    key_blocks = split_blocks(key_cols)
    value_blocks = split_blocks(values)
    running = jnp.cumsum(split_blocks(log_decay), axis=1)
    block_end = running[:, -1]
    block_state = jnp.einsum(
        "nsbhk,nsbhe->nbhke",
        key_blocks * jnp.exp(block_end[:, None] - running),
        value_blocks,
        precision=highest,
    )
    carry_state = jnp.zeros_like(block_state[0])
    log_total = jnp.zeros_like(block_end[0])
    offsets = [log_total]
    carry_state = jnp.exp(block_end[0])[..., None] * carry_state + block_state[0]
    log_total = block_end[0]
    return (
        query_blocks,
        key_blocks,
        value_blocks,
        running,
        block_state,
        jnp.stack(offsets),
        log_total,
        carry_state,
    )


def local_pass(chain, carry_state):
    query_blocks, key_blocks, value_blocks, running, block_state = (
        chain[0],
        chain[1],
        chain[2],
        chain[3],
        chain[4],
    )
    block_len = running.shape[1]
    earlier_mask = jnp.arange(block_len)[:, None] >= jnp.arange(block_len)[None, :]
    here = running[0]
    anchor = here[:1]
    query_scaled = query_blocks[0] * jnp.exp(here - anchor)
    key_scaled = key_blocks[0] * jnp.exp(anchor - here)
    scores = jnp.einsum("tbhk,sbhk->bhts", query_scaled, key_scaled, precision=highest)
    scores = jnp.where(earlier_mask, scores, 0.0)
    within = jnp.einsum("bhts,sbhe->tbhe", scores, value_blocks[0], precision=highest)
    carried = jnp.einsum(
        "tbhk,bhke->tbhe", query_blocks[0] * jnp.exp(here), carry_state, precision=highest
    )
    outputs = within + carried
    return outputs


def combine(earlier, later):
    return (earlier[0] + later[0], jnp.exp(later[0])[..., None] * earlier[1] + later[1])


def group_sums(flat_mixed, weight_lines, group_count):
    group_width = flat_mixed.shape[1] // group_count
    accumulated_total = jnp.zeros((flat_mixed.shape[0], weight_lines.shape[1]), jnp.float32)
    for tp_group in range(group_count):
        first_column = tp_group * group_width
        partial_value = jnp.dot(
            flat_mixed[:, first_column : first_column + group_width],
            weight_lines[first_column : first_column + group_width],
            preferred_element_type=jnp.float32,
        ).astype(jnp.bfloat16)
        accumulated_total = accumulated_total + lax.optimization_barrier(partial_value).astype(
            jnp.float32
        )
    return accumulated_total


def shards(
    tokens,
    norm_gain,
    w_query,
    w_value,
    w_fwd_gate,
    w_bwd_gate,
    w_out_gate,
    floor_gap,
    decay_shift,
    head_gain,
    w_out,
):
    token_f32 = tokens.astype(jnp.float32)
    scale_rows = lax.rsqrt(jnp.mean(token_f32 * token_f32, axis=-1, keepdims=True) + norm_eps)
    normed = (token_f32 * scale_rows * norm_gain).astype(jnp.bfloat16)
    weights = (
        lax.all_gather(w_query, "sp", axis=0, tiled=True),
        lax.all_gather(w_value, "sp", axis=0, tiled=True),
        lax.all_gather(w_fwd_gate, "sp", axis=0, tiled=True),
        lax.all_gather(w_bwd_gate, "sp", axis=0, tiled=True),
        lax.all_gather(w_out_gate, "sp", axis=0, tiled=True),
    )
    piece_rows = lax.all_gather(normed, "tp", axis=0, tiled=True)
    flat_rows = piece_rows.reshape(-1, piece_rows.shape[2])
    columns = [
        jnp.dot(flat_rows, matrix, preferred_element_type=jnp.float32).astype(jnp.bfloat16)
        for matrix in weights
    ]
    projected = lax.optimization_barrier(
        jnp.concatenate(columns, axis=1).reshape(piece_rows.shape[0], piece_rows.shape[1], -1)
    )
    key_width = w_query.shape[1]
    value_width = w_value.shape[1]
    heads_here = key_width // KEY
    extent_rows = projected.shape[0]
    seq_count = projected.shape[1]
    bounds_list = [
        0,
        key_width,
        key_width + value_width,
        2 * key_width + value_width,
        3 * key_width + value_width,
        3 * key_width + 2 * value_width,
    ]

    def section_part(position, feature_lanes):
        picked = projected[:, :, bounds_list[position] : bounds_list[position + 1]].astype(
            jnp.float32
        )
        return picked.reshape(extent_rows, seq_count, heads_here, feature_lanes)

    queries = jax.nn.silu(section_part(0, KEY))
    values = section_part(1, VAL)
    shift = decay_shift.reshape(extent_rows, seq_count, heads_here, KEY)
    key_fwd = floor_gap[0].reshape(heads_here, KEY) * jax.nn.sigmoid(-section_part(2, KEY))
    key_bwd = floor_gap[1].reshape(heads_here, KEY) * jax.nn.sigmoid(-section_part(3, KEY))
    decay_fwd = jnp.log1p(-key_fwd) + shift
    decay_bwd = jnp.log1p(-key_bwd) + shift
    fwd_chain = prepare_chain(queries, key_fwd, values, decay_fwd)
    bwd_chain = prepare_chain(queries[::-1], key_bwd[::-1], values[::-1], decay_bwd[::-1])
    identity_pair = (jnp.zeros_like(fwd_chain[6]), jnp.zeros_like(fwd_chain[7]))
    fwd_in = carried_in((fwd_chain[6], fwd_chain[7]), "sp", combine, identity_pair, False)[1]
    bwd_in = carried_in((bwd_chain[6], bwd_chain[7]), "sp", combine, identity_pair, True)[1]
    out_fwd = local_pass(fwd_chain, fwd_in)
    out_bwd = local_pass(bwd_chain, bwd_in)
    combined = out_fwd + out_bwd[::-1]
    head_normed = (
        combined
        * lax.rsqrt(jnp.mean(combined * combined, axis=-1, keepdims=True) + norm_eps)
        * head_gain
    )
    gate_value = jax.nn.silu(projected[:, :, bounds_list[4] : bounds_list[5]].astype(jnp.float32))
    mixed = (head_normed.reshape(extent_rows, seq_count, value_width) * gate_value).astype(
        jnp.bfloat16
    )
    token_rows = lax.all_to_all(mixed, "tp", split_axis=0, concat_axis=2, tiled=True)
    flat_mixed = token_rows.reshape(-1, token_rows.shape[2])
    group_count = lax.axis_size("tp")
    w_columns = lax.all_gather(w_out, "sp", axis=1, tiled=True)
    w_full = lax.all_gather(w_columns, "tp", axis=0, tiled=True)
    accumulated_total = group_sums(flat_mixed, w_full, group_count)
    result = accumulated_total.reshape(token_rows.shape[0], token_rows.shape[1], -1)
    return result.astype(jnp.bfloat16)


MESH = pl.DeviceIdType.MESH
CORES = 2
PIECES = 2


def recur_one(proj_ref, shift_ref, gap_ref, gain_ref, out_ref, i, own):
    f32 = jnp.float32
    bf16 = jnp.bfloat16
    length = proj_ref.shape[1]

    def cols(p):
        return proj_ref[i, :, p * KEY : (p + 1) * KEY]

    queries = cols(0).astype(f32)
    queries = queries * jax.nn.sigmoid(queries)
    values = cols(1)
    shift = shift_ref[i].astype(f32)
    row = lax.broadcasted_iota(jnp.int32, (length, length), 0)
    col = lax.broadcasted_iota(jnp.int32, (length, length), 1)
    near = row // BLOCK == col // BLOCK
    row = lax.broadcasted_iota(jnp.int32, (BLOCK, BLOCK), 0)
    col_b = lax.broadcasted_iota(jnp.int32, (BLOCK, BLOCK), 1)
    seen = [row >= col_b, row <= col_b]
    row_l = lax.broadcasted_iota(jnp.int32, (length, length), 0)
    order = [row_l >= col, row_l <= col]
    blocks = length // BLOCK
    keys, here = [], []
    for d in range(2):
        key = gap_ref[d : d + 1, own] * jax.nn.sigmoid(-cols(2 + d).astype(f32))
        decay = jnp.log1p(-key) + shift
        high = decay.astype(bf16)
        rest = decay - high.astype(f32)
        middle = rest.astype(bf16)
        low = (rest - middle.astype(f32)).astype(bf16)
        tri = jnp.where(jnp.logical_and(near, order[d]), 1.0, 0.0).astype(bf16)
        sums = jnp.dot(
            tri, jnp.concatenate([high, middle, low], axis=1), preferred_element_type=f32
        )
        here.append(sums[:, :KEY] + (sums[:, KEY : 2 * KEY] + sums[:, 2 * KEY :]))
        keys.append(key)
    state = [None, None]
    outs = [[None, None] for _ in range(blocks)]
    for step in range(blocks):
        for d in range(2):
            n = step if d == 0 else blocks - 1 - step
            at = slice(n * BLOCK, (n + 1) * BLOCK)
            q, k, v, h = queries[at], keys[d][at], values[at], here[d][at]
            edge = h[BLOCK - 1 : BLOCK] if d == 0 else h[0:1]
            anchor = h[BLOCK // 2 : BLOCK // 2 + 1]
            scores = lax.dot_general(
                (q * jnp.exp(h - anchor)).astype(bf16),
                (k * jnp.exp(anchor - h)).astype(bf16),
                (((1,), (1,)), ((), ())),
                preferred_element_type=f32,
            )
            scores = jnp.where(seen[d], scores, 0.0).astype(bf16)
            out = jnp.dot(scores, v, preferred_element_type=f32)
            if state[d] is not None:
                out = out + lax.dot_general(
                    (q * jnp.exp(h)).astype(bf16),
                    state[d].astype(bf16),
                    (((1,), (1,)), ((), ())),
                    preferred_element_type=f32,
                )
            outs[n][d] = out
            if step < blocks - 1:
                fresh = lax.dot_general(
                    v,
                    (k * jnp.exp(edge - h)).astype(bf16),
                    (((0,), (0,)), ((), ())),
                    preferred_element_type=f32,
                )
                state[d] = fresh if state[d] is None else state[d] * jnp.exp(edge) + fresh
    for n in range(blocks):
        combined = outs[n][0] + outs[n][1]
        scale = lax.rsqrt(jnp.mean(combined * combined, axis=-1, keepdims=True) + norm_eps)
        out_ref[i, n * BLOCK : (n + 1) * BLOCK] = combined * scale * gain_ref[...]


def layer_kernel(
    sizes,
    token_ref,
    norm_ref,
    shift_ref,
    wq_ref,
    wv_ref,
    wf_ref,
    wb_ref,
    wg_ref,
    gap_ref,
    gain_ref,
    w_ref,
    out_ref,
    rows_in,
    wide,
    raw_shift,
    own_shift,
    shifts,
    acts,
    weights,
    proj,
    summed,
    mixed,
    heads,
    matrix,
    partial,
    landed,
    load_sem,
    own_sem,
    az_sem,
    ax_sem,
    ac_sem,
    wz_sem,
    wy_sem,
    sz_sem,
    oz_sem,
    oy_sem,
    oc_sem,
    m_sem,
    p_sem,
):
    bf16 = jnp.bfloat16
    f32 = jnp.float32
    n_grp, n_sp, n_tp = sizes
    n_x = n_tp // CORES
    g = lax.axis_index("grp")
    s = lax.axis_index("sp")
    t = lax.axis_index("tp")
    x = t // CORES
    c = t % CORES
    twin = x * CORES + (1 - c)
    across = (1 - x) * CORES + c
    seqs = acts.shape[0]
    span = token_ref.shape[0]
    positions = n_tp * span
    depth = wq_ref.shape[0]
    half = depth // n_grp
    width = w_ref.shape[1]
    lot = seqs // PIECES
    sources = (wq_ref, wv_ref, wf_ref, wb_ref, wg_ref)
    count = len(sources)
    last = n_sp - 1
    z_at = [lax.rem(s + k, n_sp) for k in range(n_sp)]
    z_from = [lax.rem(s + n_sp - k, n_sp) for k in range(n_sp)]
    core_at = [c, 1 - c]

    def lanes(where, size=KEY):
        return pl.ds(pl.multiple_of(where * size, size), size)

    def remote(src, dst, sems, index, peer):
        return pltpu.make_async_remote_copy(
            src_ref=src,
            dst_ref=dst,
            send_sem=sems.at[(0, *index)],
            recv_sem=sems.at[(1, *index)],
            device_id=peer,
            device_id_type=MESH,
        )

    def inside(place):
        return jnp.logical_and(place >= 0, place < n_sp)

    def step_of(up):
        return 1 if up else -1

    def slot(up, d):
        return 1 + d if up else n_sp + d

    def sends(up, d):
        return jnp.logical_and(inside(s + step_of(up)), inside(s - step_of(up) * d))

    def gets(up, d):
        return inside(s - step_of(up) * (d + 1))

    def each(d, visit):
        for up in (True, False):

            @pl.when(gets(up, d))
            def _():
                visit(up, d, s - step_of(up) * (d + 1))

    sent = []

    def go(copy):
        copy.start()
        sent.append(copy)
        return copy

    load_rows = pltpu.make_async_copy(token_ref, rows_in, load_sem.at[0])
    load_shift = pltpu.make_async_copy(shift_ref, raw_shift, load_sem.at[1])
    load_rows.start()
    load_shift.start()
    peers = [(g, z_at[k], x * CORES + core_at[o]) for k in range(n_sp) for o in range(CORES)]
    peers = peers[1:] + [(g, s, across), (1 - g, s, t)]
    barrier = pltpu.get_barrier_semaphore()
    for peer in peers:
        pl.semaphore_signal(barrier, inc=1, device_id=peer, device_id_type=MESH)
    mine = [
        pltpu.make_async_copy(
            w.at[:, lanes(s)],
            weights.at[pl.ds(pl.multiple_of(s * depth, depth), depth), pl.ds(p * KEY, KEY)],
            own_sem.at[p],
        )
        for p, w in enumerate(sources)
    ]
    w_rows = pl.ds(pl.multiple_of(c * depth, depth), depth)
    w_own = pltpu.make_async_copy(w_ref, matrix.at[w_rows, lanes(s, width)], own_sem.at[count])
    for copy in mine:
        copy.start()
    w_own.start()

    here_rows = pl.ds(pl.multiple_of((s * n_tp + t) * span, span), span)
    load_rows.wait()
    rows = rows_in[...].astype(f32)
    scale = lax.rsqrt(jnp.mean(rows * rows, axis=-1, keepdims=True) + norm_eps)
    wide[...] = rows * scale * norm_ref[...]
    for q in range(seqs):
        acts[q, here_rows, :] = wide[:, q, :].astype(bf16)
    pl.semaphore_wait(barrier, len(peers))

    def block(where_s, where_t, piece):
        at = pl.ds(pl.multiple_of((where_s * n_tp + where_t) * span, span), span)
        return acts.at[pl.ds(piece * lot, lot), at, :]

    def act_z(up, d, piece):
        here = block(s - step_of(up) * d, t, piece)
        return remote(here, here, az_sem, (slot(up, d) - 1, piece), (g, s + step_of(up), t))

    def act_x(index, origin, piece):
        here = block(origin, t, piece)
        return remote(here, here, ax_sem, (index, piece), (g, s, across))

    def act_c(far, index, origin, piece):
        here = block(origin, across if far else t, piece)
        return remote(here, here, ac_sem, (far, index, piece), (g, s, twin))

    for piece in range(PIECES):
        for up in (True, False):

            @pl.when(sends(up, 0))
            def _():
                act_z(up, 0, piece).start()

        act_x(0, s, piece).start()
    for piece in range(PIECES):
        act_c(0, 0, s, piece).start()

    load_shift.wait()
    for q in range(seqs):
        values = raw_shift[:, q, :].astype(bf16)
        for k in range(n_sp):
            own_shift[k, q] = values[:, k * KEY : (k + 1) * KEY]
    place = pl.ds(pl.multiple_of(s * positions, positions), positions)
    shifts[:, place, :] = own_shift[s]

    part = pl.ds(pl.multiple_of(g * half, half), half)

    def w_rows_of(where_s, where_g):
        return pl.ds(pl.multiple_of(where_s * depth + where_g * half, half), half)

    def w_z(k, p):
        return remote(
            sources[p].at[part, lanes(z_at[k])],
            weights.at[w_rows_of(s, g), pl.ds(p * KEY, KEY)],
            wz_sem,
            (k - 1, p),
            (g, z_at[k], t),
        )

    def w_y(k, p):
        here = weights.at[w_rows_of(z_from[k], g), pl.ds(p * KEY, KEY)]
        return remote(here, here, wy_sem, (k - 1, p), (1 - g, s, t))

    def s_z(k):
        return remote(own_shift.at[z_at[k]], shifts.at[:, place, :], sz_sem, (k - 1,), (g, z_at[k], t))

    def o_block(where_s, where_g, where_c):
        at = pl.ds(pl.multiple_of(where_c * depth + where_g * half, half), half)
        return matrix.at[at, lanes(where_s, width)]

    def o_z(up, d):
        origin = s - step_of(up) * d
        here = o_block(origin, g, c)
        src = w_ref.at[part, :] if d == 0 else here
        return remote(src, here, oz_sem, (slot(up, d) - 1,), (g, s + step_of(up), t))

    def o_y(index, origin):
        here = o_block(origin, g, c)
        return remote(here, here, oy_sem, (index - 1,), (1 - g, s, t))

    def o_c(far, index, origin):
        here = o_block(origin, 1 - g if far else g, c)
        return remote(here, here, oc_sem, (far, index), (g, s, twin))

    def o_own():
        at = matrix.at[w_rows, lanes(s, width)]
        return remote(w_ref, at, oc_sem, (0, 0), (g, s, twin))

    def issue(up):
        def ahead(visit):
            for k in range(1, n_sp):
                go_up = s + k < n_sp

                @pl.when(go_up if up else jnp.logical_not(go_up))
                def _():
                    visit(k)

        for p in range(count - 1):
            ahead(lambda k: w_z(k, p).start())
        ahead(lambda k: s_z(k).start())

        @pl.when(sends(up, 0))
        def _():
            o_z(up, 0).start()

        ahead(lambda k: w_z(k, count - 1).start())

    for up in (True, False):

        @pl.when(s == (0 if up else last))
        def _():
            issue(up)

    for d in range(last):
        for piece in range(PIECES):

            def arrived(up, d, origin):
                act_z(up, d, piece).wait_recv()
                if d + 1 < last:

                    @pl.when(sends(up, d + 1))
                    def _():
                        act_z(up, d + 1, piece).start()

                act_x(slot(up, d), origin, piece).start()
                act_c(0, slot(up, d), origin, piece).start()

            each(d, arrived)
        if d + 1 < last:
            for up in (True, False):

                @pl.when(s == (d + 1 if up else last - 1 - d))
                def _():
                    issue(up)

    o_own().start()

    def relay(index, origin):
        for piece in range(PIECES):
            act_x(index, origin, piece).wait_recv()
            act_c(1, index, origin, piece).start()

    def swap(p):
        for k in range(1, n_sp):
            w_z(k, p).wait_recv()
            go(w_y(k, p))

    relay(0, s)
    for d in range(last):
        each(d, lambda up, d, origin: relay(slot(up, d), origin))
        if d < 2:
            swap(d)

    def joined(index, origin):
        for piece in range(PIECES):
            for far in range(2):
                act_c(far, index, origin, piece).wait_recv()

    joined(0, s)
    for d in range(last):
        each(d, lambda up, d, origin: joined(slot(up, d), origin))
    for copy in mine:
        copy.wait()

    def project(first, end):
        for p in range(first, end):
            for k in range(1, n_sp):
                w_y(k, p).wait_recv()
        at = slice(first * KEY, end * KEY)

        def one(q, carry):
            proj[q, :, at] = jnp.dot(
                acts[q], weights[:, at], preferred_element_type=f32
            ).astype(bf16)
            return carry

        lax.fori_loop(0, seqs, one, 0)

    def o_arrived(up, d, origin):
        o_z(up, d).wait_recv()
        if d + 1 < last:

            @pl.when(sends(up, d + 1))
            def _():
                o_z(up, d + 1).start()

        o_y(slot(up, d), origin).start()
        o_c(0, slot(up, d), origin).start()

    def o_swapped(up, d, origin):
        o_y(slot(up, d), origin).wait_recv()
        o_c(1, slot(up, d), origin).start()

    def recur(q, carry):
        recur_one(proj, shifts, gap_ref, gain_ref, summed, q, lanes(s))
        return carry

    swap(2)
    project(0, 2)
    swap(3)
    project(2, 4)
    for k in range(1, n_sp):
        s_z(k).wait_recv()
    lax.fori_loop(0, seqs // 2, recur, 0)
    each(0, o_arrived)
    swap(4)
    lax.fori_loop(seqs // 2, seqs, recur, 0)
    each(1, o_arrived)
    each(0, o_swapped)
    project(4, 5)

    targets = [(k, o) for k in range(n_sp) for o in range(CORES) if k or o]

    def m_move(q, k, o):
        return remote(
            mixed.at[q, z_at[k], :, core_at[o]],
            heads.at[:, q, :, lanes(c * n_sp + s, VAL)],
            m_sem,
            (q, k, o),
            (g, z_at[k], x * CORES + core_at[o]),
        )

    def mix(q, carry):
        gate = proj[q, :, 4 * KEY : 5 * KEY].astype(f32)
        value = (summed[q] * (gate * jax.nn.sigmoid(gate))).astype(bf16)
        mixed[q] = value.reshape(n_sp, n_x, CORES, span, VAL)
        heads[:, q, :, lanes(c * n_sp + s, VAL)] = mixed[q, s, :, c]
        for k, o in targets:
            m_move(q, k, o).start()
        return carry

    lax.fori_loop(0, seqs, mix, 0)
    for d in range(2, last):
        each(d, o_arrived)
    for d in range(1, last):
        each(d, o_swapped)
    w_own.wait()
    o_own().wait_recv()

    def o_joined(up, d, origin):
        for far in range(2):
            o_c(far, slot(up, d), origin).wait_recv()

    for d in range(last):
        each(d, o_joined)

    strips = matrix.shape[1] // width

    def p_move(h, n):
        both = pl.ds(h * lot, lot)
        at = pl.ds(n * width, width)
        return remote(
            partial.at[1 - x, both, :, at],
            landed.at[both, :, at],
            p_sem,
            (h, n),
            (g, s, across),
        )

    for h in range(PIECES):
        both = slice(h * lot, (h + 1) * lot)
        for q in range(h * lot, (h + 1) * lot):
            for k, o in targets:
                m_move(q, k, o).wait_recv()
        lines = heads[:, both].reshape(n_x * lot * span, -1)
        for n in range(strips):
            at = slice(n * width, (n + 1) * width)
            partial[:, both, :, at] = (
                jnp.dot(lines, matrix[:, at], preferred_element_type=f32)
                .astype(bf16)
                .reshape(n_x, lot, span, width)
            )
            go(p_move(h, n))
    for h in range(PIECES):
        for n in range(strips):
            p_move(h, n).wait_recv()
        for q in range(h * lot, (h + 1) * lot):
            wide[:, q, :] = partial[x, q].astype(f32) + landed[q].astype(f32)
    out_ref[...] = wide[...].astype(bf16)

    for copy in sent:
        copy.wait_send()
    for k in range(1, n_sp):
        s_z(k).wait_send()
        for p in range(count):
            w_z(k, p).wait_send()
    o_own().wait_send()
    for piece in range(PIECES):
        act_x(0, s, piece).wait_send()
        for far in range(2):
            act_c(far, 0, s, piece).wait_send()
    for d in range(last):
        for up in (True, False):

            @pl.when(sends(up, d))
            def _():
                o_z(up, d).wait_send()
                for piece in range(PIECES):
                    act_z(up, d, piece).wait_send()

        def gone(up, d, origin):
            o_y(slot(up, d), origin).wait_send()
            for far in range(2):
                o_c(far, slot(up, d), origin).wait_send()
            for piece in range(PIECES):
                act_x(slot(up, d), origin, piece).wait_send()
                for far in range(2):
                    act_c(far, slot(up, d), origin, piece).wait_send()

        each(d, gone)

    def drain(q, carry):
        for k, o in targets:
            m_move(q, k, o).wait_send()
        return carry

    lax.fori_loop(0, seqs, drain, 0)


def layer(sizes, tokens, norm_gain, shift, sources, gap, gain, w_out):
    n_grp, n_sp, n_tp = sizes
    n_x = n_tp // CORES
    span, seqs, model = tokens.shape
    length = n_sp * n_tp * span
    count = len(sources)
    depth, width = w_out.shape
    slots = 2 * n_sp - 1
    strips = n_sp
    dma = pltpu.SemaphoreType.DMA
    hbm = pl.BlockSpec(memory_space=pltpu.HBM)
    vmem = pl.BlockSpec(memory_space=pltpu.VMEM)
    bf16 = jnp.bfloat16
    return pl.pallas_call(
        functools.partial(layer_kernel, sizes),
        out_shape=jax.ShapeDtypeStruct((span, seqs, n_sp * width), bf16),
        in_specs=[hbm, vmem] + [hbm] * (1 + count) + [vmem, vmem, hbm],
        out_specs=vmem,
        scratch_shapes=[
            pltpu.VMEM(tokens.shape, bf16),
            pltpu.VMEM(tokens.shape, jnp.float32),
            pltpu.VMEM(shift.shape, shift.dtype),
            pltpu.VMEM((n_sp, seqs, n_tp * span, KEY), bf16),
            pltpu.VMEM((seqs, length, KEY), bf16),
            pltpu.VMEM((seqs, length, model), bf16),
            pltpu.VMEM((model, count * KEY), bf16),
            pltpu.VMEM((seqs, length, count * KEY), bf16),
            pltpu.VMEM((seqs, length, VAL), jnp.float32),
            pltpu.VMEM((seqs, n_sp, n_x, CORES, span, VAL), bf16),
            pltpu.VMEM((n_x, seqs, span, CORES * depth), bf16),
            pltpu.VMEM((CORES * depth, n_sp * width), bf16),
            pltpu.VMEM((n_x, seqs, span, n_sp * width), bf16),
            pltpu.VMEM((seqs, span, n_sp * width), bf16),
            dma((2,)),
            dma((count + 1,)),
            dma((2, slots - 1, PIECES)),
            dma((2, slots, PIECES)),
            dma((2, 2, slots, PIECES)),
            dma((2, n_sp - 1, count)),
            dma((2, n_sp - 1, count)),
            dma((2, n_sp - 1)),
            dma((2, slots - 1)),
            dma((2, slots - 1)),
            dma((2, 2, slots)),
            dma((2, seqs, n_sp, CORES)),
            dma((2, PIECES, strips)),
        ],
        compiler_params=pltpu.CompilerParams(
            collective_id=0, has_side_effects=True, vmem_limit_bytes=56 * 1024 * 1024
        ),
    )(tokens, norm_gain, shift, *sources, gap, gain, w_out)


def head_shards(
    sizes,
    tokens,
    norm_gain,
    w_query,
    w_value,
    w_fwd_gate,
    w_bwd_gate,
    w_out_gate,
    floor_gap,
    decay_shift,
    head_gain,
    w_out,
):
    return layer(
        sizes,
        tokens,
        norm_gain.reshape(1, 1, -1),
        decay_shift,
        (w_query, w_value, w_fwd_gate, w_bwd_gate, w_out_gate),
        floor_gap,
        head_gain.reshape(1, VAL),
        w_out,
    )


def by_heads(mesh):
    n_sp, n_tp = mesh.shape["sp"], mesh.shape["tp"]

    def run(*arrays):
        tokens, w_query = arrays[0], arrays[2]
        heads_here = w_query.shape[1] // KEY // n_tp
        span = tokens.shape[0] // (n_sp * n_tp)
        sizes = (mesh.shape["grp"], n_sp, n_tp)
        fits = heads_here == n_sp and n_sp > 2 and n_tp == 2 * CORES and span % 16 == 0
        fits = fits and sizes[0] == 2 and tokens.shape[1] // sizes[0] % PIECES == 0
        fits = fits and tokens.shape[0] % BLOCK == 0 and tokens.shape[0] <= 512
        body = functools.partial(head_shards, sizes) if fits else shards
        return mapped(body, mesh)(*arrays)

    return run


def mapped(body, mesh):
    return jax.shard_map(
        body,
        mesh=mesh,
        in_specs=(
            P(("sp", "tp"), "grp", None),
            P(),
            P("sp", "tp"),
            P("sp", "tp"),
            P("sp", "tp"),
            P("sp", "tp"),
            P("sp", "tp"),
            P(None, "tp"),
            P("sp", "grp", "tp"),
            P(),
            P("tp", "sp"),
        ),
        out_specs=P(("sp", "tp"), "grp", None),
        check_vma=False,
    )


def solution(mesh):
    return by_heads(mesh)
```

```python
import functools

import jax
import jax.numpy as jnp
from jax import lax
from jax.experimental import pallas as pl
from jax.experimental.pallas import tpu as pltpu
from jax.sharding import PartitionSpec as P

KEY = 128
VAL = 128
BLOCK = 64


norm_eps = 1e-06
highest = lax.Precision.HIGHEST


def carried_in(x, axis, join, neutral, backward):
    count = lax.axis_size(axis)
    place = lax.axis_index(axis)
    ahead = count - 1 - place if backward else place
    gathered = jax.tree.map(
        lambda a, kind: lax.all_gather(a.astype(kind), axis), x, (jnp.bfloat16, jnp.bfloat16)
    )
    state = jax.tree.map(lambda a, e: jnp.zeros_like(a) + jnp.asarray(e, a.dtype), x, neutral)

    def one(turn, state):
        source = count - 1 - turn if backward else turn
        return join(
            state,
            jax.tree.map(
                lambda a, own: lax.dynamic_index_in_dim(a, source, 0, False).astype(own.dtype),
                gathered,
                x,
            ),
        )

    return lax.fori_loop(0, ahead, one, state)


def split_blocks(array):
    return array.reshape(array.shape[0] // BLOCK, BLOCK, *array.shape[1:])


def prepare_chain(queries, key_cols, values, log_decay):
    query_blocks = split_blocks(queries)
    key_blocks = split_blocks(key_cols)
    value_blocks = split_blocks(values)
    running = jnp.cumsum(split_blocks(log_decay), axis=1)
    block_end = running[:, -1]
    block_state = jnp.einsum(
        "nsbhk,nsbhe->nbhke",
        key_blocks * jnp.exp(block_end[:, None] - running),
        value_blocks,
        precision=highest,
    )
    carry_state = jnp.zeros_like(block_state[0])
    log_total = jnp.zeros_like(block_end[0])
    offsets = [log_total]
    carry_state = jnp.exp(block_end[0])[..., None] * carry_state + block_state[0]
    log_total = block_end[0]
    return (
        query_blocks,
        key_blocks,
        value_blocks,
        running,
        block_state,
        jnp.stack(offsets),
        log_total,
        carry_state,
    )


def local_pass(chain, carry_state):
    query_blocks, key_blocks, value_blocks, running, block_state = (
        chain[0],
        chain[1],
        chain[2],
        chain[3],
        chain[4],
    )
    block_len = running.shape[1]
    earlier_mask = jnp.arange(block_len)[:, None] >= jnp.arange(block_len)[None, :]
    here = running[0]
    anchor = here[:1]
    query_scaled = query_blocks[0] * jnp.exp(here - anchor)
    key_scaled = key_blocks[0] * jnp.exp(anchor - here)
    scores = jnp.einsum("tbhk,sbhk->bhts", query_scaled, key_scaled, precision=highest)
    scores = jnp.where(earlier_mask, scores, 0.0)
    within = jnp.einsum("bhts,sbhe->tbhe", scores, value_blocks[0], precision=highest)
    carried = jnp.einsum(
        "tbhk,bhke->tbhe", query_blocks[0] * jnp.exp(here), carry_state, precision=highest
    )
    outputs = within + carried
    return outputs


def combine(earlier, later):
    return (earlier[0] + later[0], jnp.exp(later[0])[..., None] * earlier[1] + later[1])


def group_sums(flat_mixed, weight_lines, group_count):
    group_width = flat_mixed.shape[1] // group_count
    accumulated_total = jnp.zeros((flat_mixed.shape[0], weight_lines.shape[1]), jnp.float32)
    for tp_group in range(group_count):
        first_column = tp_group * group_width
        partial_value = jnp.dot(
            flat_mixed[:, first_column : first_column + group_width],
            weight_lines[first_column : first_column + group_width],
            preferred_element_type=jnp.float32,
        ).astype(jnp.bfloat16)
        accumulated_total = accumulated_total + lax.optimization_barrier(partial_value).astype(
            jnp.float32
        )
    return accumulated_total


def shards(
    tokens,
    norm_gain,
    w_query,
    w_value,
    w_fwd_gate,
    w_bwd_gate,
    w_out_gate,
    floor_gap,
    decay_shift,
    head_gain,
    w_out,
):
    token_f32 = tokens.astype(jnp.float32)
    scale_rows = lax.rsqrt(jnp.mean(token_f32 * token_f32, axis=-1, keepdims=True) + norm_eps)
    normed = (token_f32 * scale_rows * norm_gain).astype(jnp.bfloat16)
    weights = (
        lax.all_gather(w_query, "sp", axis=0, tiled=True),
        lax.all_gather(w_value, "sp", axis=0, tiled=True),
        lax.all_gather(w_fwd_gate, "sp", axis=0, tiled=True),
        lax.all_gather(w_bwd_gate, "sp", axis=0, tiled=True),
        lax.all_gather(w_out_gate, "sp", axis=0, tiled=True),
    )
    piece_rows = lax.all_gather(normed, "tp", axis=0, tiled=True)
    flat_rows = piece_rows.reshape(-1, piece_rows.shape[2])
    columns = [
        jnp.dot(flat_rows, matrix, preferred_element_type=jnp.float32).astype(jnp.bfloat16)
        for matrix in weights
    ]
    projected = lax.optimization_barrier(
        jnp.concatenate(columns, axis=1).reshape(piece_rows.shape[0], piece_rows.shape[1], -1)
    )
    key_width = w_query.shape[1]
    value_width = w_value.shape[1]
    heads_here = key_width // KEY
    extent_rows = projected.shape[0]
    seq_count = projected.shape[1]
    bounds_list = [
        0,
        key_width,
        key_width + value_width,
        2 * key_width + value_width,
        3 * key_width + value_width,
        3 * key_width + 2 * value_width,
    ]

    def section_part(position, feature_lanes):
        picked = projected[:, :, bounds_list[position] : bounds_list[position + 1]].astype(
            jnp.float32
        )
        return picked.reshape(extent_rows, seq_count, heads_here, feature_lanes)

    queries = jax.nn.silu(section_part(0, KEY))
    values = section_part(1, VAL)
    shift = decay_shift.reshape(extent_rows, seq_count, heads_here, KEY)
    key_fwd = floor_gap[0].reshape(heads_here, KEY) * jax.nn.sigmoid(-section_part(2, KEY))
    key_bwd = floor_gap[1].reshape(heads_here, KEY) * jax.nn.sigmoid(-section_part(3, KEY))
    decay_fwd = jnp.log1p(-key_fwd) + shift
    decay_bwd = jnp.log1p(-key_bwd) + shift
    fwd_chain = prepare_chain(queries, key_fwd, values, decay_fwd)
    bwd_chain = prepare_chain(queries[::-1], key_bwd[::-1], values[::-1], decay_bwd[::-1])
    identity_pair = (jnp.zeros_like(fwd_chain[6]), jnp.zeros_like(fwd_chain[7]))
    fwd_in = carried_in((fwd_chain[6], fwd_chain[7]), "sp", combine, identity_pair, False)[1]
    bwd_in = carried_in((bwd_chain[6], bwd_chain[7]), "sp", combine, identity_pair, True)[1]
    out_fwd = local_pass(fwd_chain, fwd_in)
    out_bwd = local_pass(bwd_chain, bwd_in)
    combined = out_fwd + out_bwd[::-1]
    head_normed = (
        combined
        * lax.rsqrt(jnp.mean(combined * combined, axis=-1, keepdims=True) + norm_eps)
        * head_gain
    )
    gate_value = jax.nn.silu(projected[:, :, bounds_list[4] : bounds_list[5]].astype(jnp.float32))
    mixed = (head_normed.reshape(extent_rows, seq_count, value_width) * gate_value).astype(
        jnp.bfloat16
    )
    token_rows = lax.all_to_all(mixed, "tp", split_axis=0, concat_axis=2, tiled=True)
    flat_mixed = token_rows.reshape(-1, token_rows.shape[2])
    group_count = lax.axis_size("tp")
    w_columns = lax.all_gather(w_out, "sp", axis=1, tiled=True)
    w_full = lax.all_gather(w_columns, "tp", axis=0, tiled=True)
    accumulated_total = group_sums(flat_mixed, w_full, group_count)
    result = accumulated_total.reshape(token_rows.shape[0], token_rows.shape[1], -1)
    return result.astype(jnp.bfloat16)


MESH = pl.DeviceIdType.MESH
CORES = 2
PIECES = 2
scope = jax.named_scope


def recur_one(proj_ref, shift_ref, gap_ref, gain_ref, out_ref, i, own):
    f32 = jnp.float32
    bf16 = jnp.bfloat16
    length = proj_ref.shape[1]

    def cols(p):
        return proj_ref[i, :, p * KEY : (p + 1) * KEY]

    queries = cols(0).astype(f32)
    queries = queries * jax.nn.sigmoid(queries)
    values = cols(1)
    shift = shift_ref[i].astype(f32)
    row = lax.broadcasted_iota(jnp.int32, (length, length), 0)
    col = lax.broadcasted_iota(jnp.int32, (length, length), 1)
    near = row // BLOCK == col // BLOCK
    row = lax.broadcasted_iota(jnp.int32, (BLOCK, BLOCK), 0)
    col_b = lax.broadcasted_iota(jnp.int32, (BLOCK, BLOCK), 1)
    seen = [row >= col_b, row <= col_b]
    row_l = lax.broadcasted_iota(jnp.int32, (length, length), 0)
    order = [row_l >= col, row_l <= col]
    blocks = length // BLOCK
    keys, here = [], []
    for d in range(2):
        key = gap_ref[d : d + 1, own] * jax.nn.sigmoid(-cols(2 + d).astype(f32))
        decay = jnp.log1p(-key) + shift
        high = decay.astype(bf16)
        rest = decay - high.astype(f32)
        middle = rest.astype(bf16)
        low = (rest - middle.astype(f32)).astype(bf16)
        tri = jnp.where(jnp.logical_and(near, order[d]), 1.0, 0.0).astype(bf16)
        sums = jnp.dot(
            tri, jnp.concatenate([high, middle, low], axis=1), preferred_element_type=f32
        )
        here.append(sums[:, :KEY] + (sums[:, KEY : 2 * KEY] + sums[:, 2 * KEY :]))
        keys.append(key)
    state = [None, None]
    outs = [[None, None] for _ in range(blocks)]
    for step in range(blocks):
        for d in range(2):
            n = step if d == 0 else blocks - 1 - step
            at = slice(n * BLOCK, (n + 1) * BLOCK)
            q, k, v, h = queries[at], keys[d][at], values[at], here[d][at]
            edge = h[BLOCK - 1 : BLOCK] if d == 0 else h[0:1]
            anchor = h[BLOCK // 2 : BLOCK // 2 + 1]
            scores = lax.dot_general(
                (q * jnp.exp(h - anchor)).astype(bf16),
                (k * jnp.exp(anchor - h)).astype(bf16),
                (((1,), (1,)), ((), ())),
                preferred_element_type=f32,
            )
            scores = jnp.where(seen[d], scores, 0.0).astype(bf16)
            out = jnp.dot(scores, v, preferred_element_type=f32)
            if state[d] is not None:
                out = out + lax.dot_general(
                    (q * jnp.exp(h)).astype(bf16),
                    state[d].astype(bf16),
                    (((1,), (1,)), ((), ())),
                    preferred_element_type=f32,
                )
            outs[n][d] = out
            if step < blocks - 1:
                fresh = lax.dot_general(
                    v,
                    (k * jnp.exp(edge - h)).astype(bf16),
                    (((0,), (0,)), ((), ())),
                    preferred_element_type=f32,
                )
                state[d] = fresh if state[d] is None else state[d] * jnp.exp(edge) + fresh
    for n in range(blocks):
        out_ref[n * BLOCK : (n + 1) * BLOCK] = outs[n][0] + outs[n][1]
    combined = out_ref[...]
    normed = combined * lax.rsqrt(jnp.mean(combined * combined, axis=-1, keepdims=True) + norm_eps)
    gate = cols(4).astype(f32)
    return (normed * gain_ref[...] * (gate * jax.nn.sigmoid(gate))).astype(bf16)


def layer_kernel(
    sizes,
    token_ref,
    norm_ref,
    shift_ref,
    wq_ref,
    wv_ref,
    wf_ref,
    wb_ref,
    wg_ref,
    gap_ref,
    gain_ref,
    w_ref,
    out_ref,
    rows_in,
    wide,
    raw_shift,
    own_shift,
    shifts,
    acts,
    weights,
    proj,
    summed,
    mixed,
    heads,
    matrix,
    partial,
    landed,
    load_sem,
    az_out,
    az_in,
    ax_out,
    ax_in,
    ac_out,
    ac_in,
    wz_out,
    wz_in,
    wy_out,
    wy_in,
    sz_out,
    sz_in,
    oz_out,
    oz_in,
    oy_out,
    oy_in,
    oc_out,
    oc_in,
    m_out,
    m_in,
    p_out,
    p_in,
):
    bf16 = jnp.bfloat16
    f32 = jnp.float32
    n_grp, n_sp, n_tp = sizes
    n_x = n_tp // CORES
    g = lax.axis_index("grp")
    s = lax.axis_index("sp")
    t = lax.axis_index("tp")
    x = t // CORES
    c = t % CORES
    twin = x * CORES + (1 - c)
    across = (1 - x) * CORES + c
    seqs = acts.shape[0]
    span = token_ref.shape[0]
    positions = n_tp * span
    depth = wq_ref.shape[0]
    half = depth // n_grp
    width = w_ref.shape[1]
    lot = seqs // PIECES
    bit = half // PIECES
    sources = (wq_ref, wv_ref, wf_ref, wb_ref, wg_ref)
    count = len(sources)
    groups = ((0, 2), (2, 4), (4, 5))
    last = n_sp - 1
    z_at = [lax.rem(s + k, n_sp) for k in range(n_sp)]
    z_from = [lax.rem(s + n_sp - k, n_sp) for k in range(n_sp)]
    core_at = [c, 1 - c]

    def span_at(where, size):
        return pl.ds(pl.multiple_of(where * size, size), size)

    def lanes(where, size=KEY):
        return span_at(where, size)

    def remote(src, dst, out_sem, in_sem, peer):
        return pltpu.make_async_remote_copy(
            src_ref=src,
            dst_ref=dst,
            send_sem=out_sem,
            recv_sem=in_sem,
            device_id=peer,
            device_id_type=MESH,
        )

    def tally(ref, out_sem, in_sem):
        return remote(ref, ref, out_sem, in_sem, (g, s, twin))

    def inside(place):
        return jnp.logical_and(place >= 0, place < n_sp)

    def step_of(up):
        return 1 if up else -1

    def slot(up, d):
        return 1 + d if up else n_sp + d

    def end(up):
        return 0 if up else last

    def sends(up, d):
        return jnp.logical_and(inside(s + step_of(up)), inside(s - step_of(up) * d))

    def gets(up, d):
        return inside(s - step_of(up) * (d + 1))

    def each(d, visit):
        for up in (True, False):

            @pl.when(gets(up, d))
            def _():
                visit(up, d, s - step_of(up) * (d + 1))

    load_rows = pltpu.make_async_copy(token_ref, rows_in, load_sem.at[0])
    load_shift = pltpu.make_async_copy(shift_ref, raw_shift, load_sem.at[1])
    load_rows.start()
    load_shift.start()
    peers = [(g, z_at[k], x * CORES + core_at[o]) for k in range(n_sp) for o in range(CORES)]
    peers = peers[1:] + [(g, s, across), (1 - g, s, t)]
    barrier = pltpu.get_barrier_semaphore()
    for peer in peers:
        pl.semaphore_signal(barrier, inc=1, device_id=peer, device_id_type=MESH)
    own_rows = span_at(s, depth)
    for p, w in enumerate(sources):
        pltpu.make_async_copy(
            w.at[:, lanes(s)], weights.at[own_rows, pl.ds(p * KEY, KEY)], load_sem.at[2]
        ).start()
    w_rows = span_at(c, depth)
    w_own = pltpu.make_async_copy(w_ref, matrix.at[w_rows, lanes(s, width)], load_sem.at[3])
    w_own.start()

    here_rows = span_at(s * n_tp + t, span)
    with scope("wait_rows"):
        load_rows.wait()
    rows = rows_in[...].astype(f32)
    scale = lax.rsqrt(jnp.mean(rows * rows, axis=-1, keepdims=True) + norm_eps)
    wide[...] = rows * scale * norm_ref[...]
    for q in range(seqs):
        acts[q, here_rows, :] = wide[:, q, :].astype(bf16)
    with scope("barrier"):
        pl.semaphore_wait(barrier, len(peers))

    def block(where_s, where_t):
        return acts.at[:, span_at(where_s * n_tp + where_t, span), :]

    def act_z(up, d, piece):
        at = span_at((s - step_of(up) * d) * n_tp + t, span)
        here = acts.at[pl.ds(piece * lot, lot), at, :]
        index = slot(up, d) - 1
        peer = (g, s + step_of(up), t)
        return remote(here, here, az_out.at[index], az_in.at[index, piece], peer)

    def act_x(index, origin):
        here = block(origin, t)
        return remote(here, here, ax_out, ax_in.at[index], (g, s, across))

    def act_c(far, origin):
        here = block(origin, across if far else t)
        return remote(here, here, ac_out, ac_in, (g, s, twin))

    part = span_at(g, half)

    def w_cols(group):
        first, stop = groups[group]
        return pl.ds(first * KEY, (stop - first) * KEY)

    def w_z(k, group, p):
        src = sources[p].at[part, lanes(z_at[k])]
        dst = weights.at[span_at(s * n_grp + g, half), pl.ds(p * KEY, KEY)]
        return remote(src, dst, wz_out, wz_in.at[k - 1, group], (g, z_at[k], t))

    def w_block(k, group):
        return weights.at[span_at(z_from[k] * n_grp + g, half), w_cols(group)]

    def w_y(k, group):
        here = w_block(k, group)
        return remote(here, here, wy_out, wy_in.at[group], (1 - g, s, t))

    place = span_at(s, positions)

    def s_z(k):
        return remote(own_shift.at[z_at[k]], shifts.at[:, place, :], sz_out, sz_in, (g, z_at[k], t))

    def o_block(where_s, where_g, where_c, piece):
        at = pl.multiple_of(where_c * depth + where_g * half + piece * bit, bit)
        return matrix.at[pl.ds(at, bit), lanes(where_s, width)]

    def o_z(up, d, piece):
        here = o_block(s - step_of(up) * d, g, c, piece)
        src = w_ref.at[span_at(g * PIECES + piece, bit), :] if d == 0 else here
        index = slot(up, d) - 1
        peer = (g, s + step_of(up), t)
        return remote(src, here, oz_out.at[index], oz_in.at[index, piece], peer)

    def o_y(index, origin, piece):
        here = o_block(origin, g, c, piece)
        return remote(here, here, oy_out, oy_in.at[index - 1, piece], (1 - g, s, t))

    def o_c(far, index, origin, piece):
        here = o_block(origin, 1 - g if far else g, c, piece)
        return remote(here, here, oc_out, oc_in.at[index], (g, s, twin))

    def ahead(up, groups_now):
        for hop in range(1, n_sp):
            k = hop if up else n_sp - hop
            go_up = s + k < n_sp

            @pl.when(go_up if up else jnp.logical_not(go_up))
            def _():
                for group in groups_now:
                    if group is None:
                        s_z(k).start()
                    else:
                        for p in range(*groups[group]):
                            w_z(k, group, p).start()

    def o_first(up):
        @pl.when(sends(up, 0))
        def _():
            for piece in range(PIECES):
                o_z(up, 0, piece).start()

    def issue(up):
        pl.when(s == end(up))(lambda: o_first(up))
        ahead(up, range(len(groups)))

        @pl.when(s != end(up))
        def _():
            ahead(up, (None,))
            o_first(up)

    def issue_rest():
        for up in (True, False):

            @pl.when(s == end(up))
            def _():
                ahead(up, (None,))

    for piece in range(PIECES):
        for up in (True, False):

            @pl.when(sends(up, 0))
            def _():
                act_z(up, 0, piece).start()

    act_x(0, s).start()
    act_c(0, s).start()
    with scope("wait_shift_load"):
        load_shift.wait()
    for q in range(seqs):
        values = raw_shift[:, q, :].astype(bf16)
        for k in range(n_sp):
            own_shift[k, q] = values[:, k * KEY : (k + 1) * KEY]
    shifts[:, place, :] = own_shift[s]
    for up in (True, False):

        @pl.when(s == end(up))
        def _():
            issue(up)

    for d in range(last):
        for piece in range(PIECES):

            def arrived(up, d, origin):
                act_z(up, d, piece).wait_recv()
                if d + 1 < last:

                    @pl.when(sends(up, d + 1))
                    def _():
                        act_z(up, d + 1, piece).start()

                if piece == PIECES - 1:
                    act_x(slot(up, d), origin).start()
                    act_c(0, origin).start()

            with scope(f"act_z{d}_{piece}"):
                each(d, arrived)
        if d + 1 < last:
            for up in (True, False):

                @pl.when(s == (d + 1 if up else last - 1 - d))
                def _():
                    issue(up)

    o_own = remote(w_ref, matrix.at[w_rows, lanes(s, width)], oc_out, oc_in.at[0], (g, s, twin))
    o_own.start()

    def relay(index, origin):
        act_x(index, origin).wait_recv()
        act_c(1, origin).start()

    def swap(up, d, origin):
        k = d + 1 if up else last - d
        for group in range(len(groups)):
            tally(w_block(k, group), wz_out, wz_in.at[k - 1, group]).wait_recv()
            w_y(k, group).start()

    def o_take(up, d, origin):
        for piece in range(PIECES):
            o_z(up, d, piece).wait_recv()
            if d + 1 < last:

                @pl.when(sends(up, d + 1))
                def _():
                    o_z(up, d + 1, piece).start()

            o_y(slot(up, d), origin, piece).start()
            o_c(0, slot(up, d), origin, piece).start()

    def take_early(up):
        for piece in range(PIECES):
            o_z(up, 0, piece).wait_recv()
            o_y(slot(up, 0), s - step_of(up), piece).start()
            o_c(0, slot(up, 0), s - step_of(up), piece).start()

    def o_swapped(up, d, origin):
        for piece in range(PIECES):
            o_y(slot(up, d), origin, piece).wait_recv()
            o_c(1, slot(up, d), origin, piece).start()

    def neighbour(up):
        return s == (1 if up else last - 1)

    with scope("take_early"):
        for up in (True, False):
            pl.when(neighbour(up))(lambda: take_early(up))
    with scope("swap_near"):
        each(0, swap)
    with scope("relay"):
        relay(0, s)
        for d in range(last):
            each(d, lambda up, d, origin: relay(slot(up, d), origin))
    for d in range(last - 1, 0, -1):
        with scope(f"swap_far{d}"):
            each(d, swap)
    issue_rest()

    with scope("joined"):
        tally(acts.at[pl.ds(0, seqs // CORES)], ac_out, ac_in).wait_recv()
        here = weights.at[own_rows, :]
        pltpu.make_async_copy(here, here, load_sem.at[2]).wait()

    def project(group):
        with scope(f"wait_w{group}"):
            block = weights.at[pl.ds(0, last * half), w_cols(group)]
            tally(block, wy_out, wy_in.at[group]).wait_recv()
        at = slice(groups[group][0] * KEY, groups[group][1] * KEY)

        def one(q, carry):
            proj[q, :, at] = jnp.dot(
                acts[q], weights[:, at], preferred_element_type=f32
            ).astype(bf16)
            return carry

        with scope(f"project{group}"):
            lax.fori_loop(0, seqs, one, 0)

    project(0)
    with scope("act_drain"):
        tally(acts.at[:, pl.ds(0, n_sp * span), :], ax_out, ax_in.at[0]).wait_send()
        tally(acts.at[pl.ds(0, seqs // CORES)], ac_out, ac_in).wait_send()
        for d in range(last):
            for up in (True, False):

                @pl.when(sends(up, d))
                def _():
                    index = slot(up, d) - 1
                    tally(block(s, t), az_out.at[index], az_in.at[index, 0]).wait_send()

    project(1)
    project(2)
    with scope("wait_shift"):
        tally(shifts.at[:, pl.ds(0, last * positions), :], sz_out, sz_in).wait_recv()

    targets = [(k, o) for k in range(n_sp) for o in range(CORES) if k or o]

    def m_move(q, k, o):
        return remote(
            mixed.at[q, z_at[k], :, core_at[o]],
            heads.at[:, q, :, lanes(c * n_sp + s, VAL)],
            m_out,
            m_in,
            (g, z_at[k], x * CORES + core_at[o]),
        )

    def recur(q, carry):
        value = recur_one(proj, shifts, gap_ref, gain_ref, summed, q, lanes(s))
        mixed[q] = value.reshape(n_sp, n_x, CORES, span, VAL)
        heads[:, q, :, lanes(c * n_sp + s, VAL)] = mixed[q, s, :, c]
        for k, o in targets:
            m_move(q, k, o).start()
        return carry

    with scope("recur"):
        lax.fori_loop(0, seqs, recur, 0)
    with scope("forward"):
        for up in (True, False):

            @pl.when(jnp.logical_and(neighbour(up), sends(up, 1)))
            def _():
                for piece in range(PIECES):
                    o_z(up, 1, piece).start()

    with scope("take_late"):
        for up in (True, False):

            @pl.when(jnp.logical_and(gets(up, 0), jnp.logical_not(neighbour(up))))
            def _():
                o_take(up, 0, s - step_of(up))

    with scope("w_drain"):
        tally(own_shift.at[pl.ds(0, last)], sz_out, sz_in).wait_send()
        every = weights.at[pl.ds(0, last * half), :]
        tally(every, wz_out, wz_in.at[0, 0]).wait_send()
        tally(every, wy_out, wy_in.at[0]).wait_send()
    for d in range(1, last):
        with scope(f"o_swapped{d - 1}"):
            each(d - 1, o_swapped)
        with scope(f"o_pass{d}"):
            each(d, o_take)
    w_own.wait()

    def p_move(index, origin):
        at = lanes(origin, width)
        peer = (g, s, across)
        return remote(partial.at[1 - x, :, :, at], landed.at[:, :, at], p_out, p_in.at[index], peer)

    def strip(index, origin):
        at = lanes(origin, width)
        tally(matrix.at[pl.ds(0, depth), at], oc_out, oc_in.at[index]).wait_recv()
        lines = heads[...].reshape(n_x * seqs * span, -1)
        partial[:, :, :, at] = (
            jnp.dot(lines, matrix[:, at], preferred_element_type=f32)
            .astype(bf16)
            .reshape(n_x, seqs, span, width)
        )
        p_move(index, origin).start()

    def o_strip(up, d, origin):
        strip(slot(up, d), origin)

    all_mixed = tally(heads.at[:, :, :, pl.ds(0, len(targets) * VAL)], m_out, m_in)
    with scope("wait_m"):
        all_mixed.wait_recv()
    with scope("own_strip"):
        strip(0, s)
    for d in range(last - 1):
        with scope(f"strip{d}"):
            each(d, o_strip)
    with scope(f"o_swapped{last - 1}"):
        each(last - 1, o_swapped)
    with scope(f"strip{last - 1}"):
        each(last - 1, o_strip)

    def finish(index, origin):
        p_move(index, origin).wait_recv()
        at = lanes(origin, width)
        total = partial[x, :, :, at].astype(f32) + landed[:, :, at].astype(f32)
        out_ref[:, :, at] = total.astype(bf16)

    with scope("finish"):
        finish(0, s)
        for d in range(last):
            each(d, lambda up, d, origin: finish(slot(up, d), origin))
    with scope("drain"):
        all_mixed.wait_send()
        strips = matrix.at[pl.ds(0, half), pl.ds(0, last * width)]
        tally(strips, oy_out, oy_in.at[0, 0]).wait_send()
        tally(matrix.at[pl.ds(0, depth), :], oc_out, oc_in.at[0]).wait_send()
        tally(landed, p_out, p_in.at[0]).wait_send()
        for d in range(last):
            for up in (True, False):

                @pl.when(sends(up, d))
                def _():
                    index = slot(up, d) - 1
                    here = matrix.at[pl.ds(0, half), pl.ds(0, width)]
                    tally(here, oz_out.at[index], oz_in.at[index, 0]).wait_send()


def layer(sizes, tokens, norm_gain, shift, sources, gap, gain, w_out):
    n_grp, n_sp, n_tp = sizes
    n_x = n_tp // CORES
    span, seqs, model = tokens.shape
    length = n_sp * n_tp * span
    count = len(sources)
    depth, width = w_out.shape
    slots = 2 * n_sp - 1
    dma = pltpu.SemaphoreType.DMA
    hbm = pl.BlockSpec(memory_space=pltpu.HBM)
    vmem = pl.BlockSpec(memory_space=pltpu.VMEM)
    bf16 = jnp.bfloat16
    return pl.pallas_call(
        functools.partial(layer_kernel, sizes),
        out_shape=jax.ShapeDtypeStruct((seqs, span, n_sp * width), bf16),
        in_specs=[hbm, vmem] + [hbm] * (1 + count) + [vmem, vmem, hbm],
        out_specs=vmem,
        scratch_shapes=[
            pltpu.VMEM(tokens.shape, bf16),
            pltpu.VMEM(tokens.shape, jnp.float32),
            pltpu.VMEM(shift.shape, shift.dtype),
            pltpu.VMEM((n_sp, seqs, n_tp * span, KEY), bf16),
            pltpu.VMEM((seqs, length, KEY), bf16),
            pltpu.VMEM((seqs, length, model), bf16),
            pltpu.VMEM((model, count * KEY), bf16),
            pltpu.VMEM((seqs, length, count * KEY), bf16),
            pltpu.VMEM((length, VAL), jnp.float32),
            pltpu.VMEM((seqs, n_sp, n_x, CORES, span, VAL), bf16),
            pltpu.VMEM((n_x, seqs, span, CORES * depth), bf16),
            pltpu.VMEM((CORES * depth, n_sp * width), bf16),
            pltpu.VMEM((n_x, seqs, span, n_sp * width), bf16),
            pltpu.VMEM((seqs, span, n_sp * width), bf16),
            dma((4,)),
            dma((slots - 1,)),
            dma((slots - 1, PIECES)),
            dma,
            dma((slots,)),
            dma,
            dma,
            dma,
            dma((n_sp - 1, 3)),
            dma,
            dma((3,)),
            dma,
            dma,
            dma((slots - 1,)),
            dma((slots - 1, PIECES)),
            dma,
            dma((slots - 1, PIECES)),
            dma,
            dma((slots,)),
            dma,
            dma,
            dma,
            dma((slots,)),
        ],
        compiler_params=pltpu.CompilerParams(
            collective_id=0, has_side_effects=True, vmem_limit_bytes=56 * 1024 * 1024
        ),
    )(tokens, norm_gain, shift, *sources, gap, gain, w_out)


def head_shards(
    sizes,
    tokens,
    norm_gain,
    w_query,
    w_value,
    w_fwd_gate,
    w_bwd_gate,
    w_out_gate,
    floor_gap,
    decay_shift,
    head_gain,
    w_out,
):
    return layer(
        sizes,
        tokens,
        norm_gain.reshape(1, 1, -1),
        decay_shift,
        (w_query, w_value, w_fwd_gate, w_bwd_gate, w_out_gate),
        floor_gap,
        head_gain.reshape(1, VAL),
        w_out,
    ).transpose(1, 0, 2)


def by_heads(mesh):
    n_sp, n_tp = mesh.shape["sp"], mesh.shape["tp"]

    def run(*arrays):
        tokens, w_query = arrays[0], arrays[2]
        heads_here = w_query.shape[1] // KEY // n_tp
        span = tokens.shape[0] // (n_sp * n_tp)
        sizes = (mesh.shape["grp"], n_sp, n_tp)
        fits = heads_here == n_sp and n_sp > 2 and n_tp == 2 * CORES and span % 16 == 0
        fits = fits and sizes[0] == 2 and tokens.shape[1] // sizes[0] % PIECES == 0
        fits = fits and tokens.shape[0] % BLOCK == 0 and tokens.shape[0] <= 512
        body = functools.partial(head_shards, sizes) if fits else shards
        return mapped(body, mesh)(*arrays)

    return run


def mapped(body, mesh):
    return jax.shard_map(
        body,
        mesh=mesh,
        in_specs=(
            P(("sp", "tp"), "grp", None),
            P(),
            P("sp", "tp"),
            P("sp", "tp"),
            P("sp", "tp"),
            P("sp", "tp"),
            P("sp", "tp"),
            P(None, "tp"),
            P("sp", "grp", "tp"),
            P(),
            P("tp", "sp"),
        ),
        out_specs=P(("sp", "tp"), "grp", None),
        check_vma=False,
    )


def solution(mesh):
    return by_heads(mesh)
```

```python
import functools

import jax
import jax.numpy as jnp
from jax import lax
from jax.experimental import pallas as pl
from jax.experimental.pallas import tpu as pltpu
from jax.sharding import PartitionSpec as P

KEY = 128
VAL = 128
BLOCK = 64


norm_eps = 1e-06
highest = lax.Precision.HIGHEST


def carried_in(x, axis, join, neutral, backward):
    count = lax.axis_size(axis)
    place = lax.axis_index(axis)
    ahead = count - 1 - place if backward else place
    gathered = jax.tree.map(
        lambda a, kind: lax.all_gather(a.astype(kind), axis), x, (jnp.bfloat16, jnp.bfloat16)
    )
    state = jax.tree.map(lambda a, e: jnp.zeros_like(a) + jnp.asarray(e, a.dtype), x, neutral)

    def one(turn, state):
        source = count - 1 - turn if backward else turn
        return join(
            state,
            jax.tree.map(
                lambda a, own: lax.dynamic_index_in_dim(a, source, 0, False).astype(own.dtype),
                gathered,
                x,
            ),
        )

    return lax.fori_loop(0, ahead, one, state)


def split_blocks(array):
    return array.reshape(array.shape[0] // BLOCK, BLOCK, *array.shape[1:])


def prepare_chain(queries, key_cols, values, log_decay):
    query_blocks = split_blocks(queries)
    key_blocks = split_blocks(key_cols)
    value_blocks = split_blocks(values)
    running = jnp.cumsum(split_blocks(log_decay), axis=1)
    block_end = running[:, -1]
    block_state = jnp.einsum(
        "nsbhk,nsbhe->nbhke",
        key_blocks * jnp.exp(block_end[:, None] - running),
        value_blocks,
        precision=highest,
    )
    carry_state = jnp.zeros_like(block_state[0])
    log_total = jnp.zeros_like(block_end[0])
    offsets = [log_total]
    carry_state = jnp.exp(block_end[0])[..., None] * carry_state + block_state[0]
    log_total = block_end[0]
    return (
        query_blocks,
        key_blocks,
        value_blocks,
        running,
        block_state,
        jnp.stack(offsets),
        log_total,
        carry_state,
    )


def local_pass(chain, carry_state):
    query_blocks, key_blocks, value_blocks, running, block_state = (
        chain[0],
        chain[1],
        chain[2],
        chain[3],
        chain[4],
    )
    block_len = running.shape[1]
    earlier_mask = jnp.arange(block_len)[:, None] >= jnp.arange(block_len)[None, :]
    here = running[0]
    anchor = here[:1]
    query_scaled = query_blocks[0] * jnp.exp(here - anchor)
    key_scaled = key_blocks[0] * jnp.exp(anchor - here)
    scores = jnp.einsum("tbhk,sbhk->bhts", query_scaled, key_scaled, precision=highest)
    scores = jnp.where(earlier_mask, scores, 0.0)
    within = jnp.einsum("bhts,sbhe->tbhe", scores, value_blocks[0], precision=highest)
    carried = jnp.einsum(
        "tbhk,bhke->tbhe", query_blocks[0] * jnp.exp(here), carry_state, precision=highest
    )
    outputs = within + carried
    return outputs


def combine(earlier, later):
    return (earlier[0] + later[0], jnp.exp(later[0])[..., None] * earlier[1] + later[1])


def group_sums(flat_mixed, weight_lines, group_count):
    group_width = flat_mixed.shape[1] // group_count
    accumulated_total = jnp.zeros((flat_mixed.shape[0], weight_lines.shape[1]), jnp.float32)
    for tp_group in range(group_count):
        first_column = tp_group * group_width
        partial_value = jnp.dot(
            flat_mixed[:, first_column : first_column + group_width],
            weight_lines[first_column : first_column + group_width],
            preferred_element_type=jnp.float32,
        ).astype(jnp.bfloat16)
        accumulated_total = accumulated_total + lax.optimization_barrier(partial_value).astype(
            jnp.float32
        )
    return accumulated_total


def shards(
    tokens,
    norm_gain,
    w_query,
    w_value,
    w_fwd_gate,
    w_bwd_gate,
    w_out_gate,
    floor_gap,
    decay_shift,
    head_gain,
    w_out,
):
    token_f32 = tokens.astype(jnp.float32)
    scale_rows = lax.rsqrt(jnp.mean(token_f32 * token_f32, axis=-1, keepdims=True) + norm_eps)
    normed = (token_f32 * scale_rows * norm_gain).astype(jnp.bfloat16)
    weights = (
        lax.all_gather(w_query, "sp", axis=0, tiled=True),
        lax.all_gather(w_value, "sp", axis=0, tiled=True),
        lax.all_gather(w_fwd_gate, "sp", axis=0, tiled=True),
        lax.all_gather(w_bwd_gate, "sp", axis=0, tiled=True),
        lax.all_gather(w_out_gate, "sp", axis=0, tiled=True),
    )
    piece_rows = lax.all_gather(normed, "tp", axis=0, tiled=True)
    flat_rows = piece_rows.reshape(-1, piece_rows.shape[2])
    columns = [
        jnp.dot(flat_rows, matrix, preferred_element_type=jnp.float32).astype(jnp.bfloat16)
        for matrix in weights
    ]
    projected = lax.optimization_barrier(
        jnp.concatenate(columns, axis=1).reshape(piece_rows.shape[0], piece_rows.shape[1], -1)
    )
    key_width = w_query.shape[1]
    value_width = w_value.shape[1]
    heads_here = key_width // KEY
    extent_rows = projected.shape[0]
    seq_count = projected.shape[1]
    bounds_list = [
        0,
        key_width,
        key_width + value_width,
        2 * key_width + value_width,
        3 * key_width + value_width,
        3 * key_width + 2 * value_width,
    ]

    def section_part(position, feature_lanes):
        picked = projected[:, :, bounds_list[position] : bounds_list[position + 1]].astype(
            jnp.float32
        )
        return picked.reshape(extent_rows, seq_count, heads_here, feature_lanes)

    queries = jax.nn.silu(section_part(0, KEY))
    values = section_part(1, VAL)
    shift = decay_shift.reshape(extent_rows, seq_count, heads_here, KEY)
    key_fwd = floor_gap[0].reshape(heads_here, KEY) * jax.nn.sigmoid(-section_part(2, KEY))
    key_bwd = floor_gap[1].reshape(heads_here, KEY) * jax.nn.sigmoid(-section_part(3, KEY))
    decay_fwd = jnp.log1p(-key_fwd) + shift
    decay_bwd = jnp.log1p(-key_bwd) + shift
    fwd_chain = prepare_chain(queries, key_fwd, values, decay_fwd)
    bwd_chain = prepare_chain(queries[::-1], key_bwd[::-1], values[::-1], decay_bwd[::-1])
    identity_pair = (jnp.zeros_like(fwd_chain[6]), jnp.zeros_like(fwd_chain[7]))
    fwd_in = carried_in((fwd_chain[6], fwd_chain[7]), "sp", combine, identity_pair, False)[1]
    bwd_in = carried_in((bwd_chain[6], bwd_chain[7]), "sp", combine, identity_pair, True)[1]
    out_fwd = local_pass(fwd_chain, fwd_in)
    out_bwd = local_pass(bwd_chain, bwd_in)
    combined = out_fwd + out_bwd[::-1]
    head_normed = (
        combined
        * lax.rsqrt(jnp.mean(combined * combined, axis=-1, keepdims=True) + norm_eps)
        * head_gain
    )
    gate_value = jax.nn.silu(projected[:, :, bounds_list[4] : bounds_list[5]].astype(jnp.float32))
    mixed = (head_normed.reshape(extent_rows, seq_count, value_width) * gate_value).astype(
        jnp.bfloat16
    )
    token_rows = lax.all_to_all(mixed, "tp", split_axis=0, concat_axis=2, tiled=True)
    flat_mixed = token_rows.reshape(-1, token_rows.shape[2])
    group_count = lax.axis_size("tp")
    w_columns = lax.all_gather(w_out, "sp", axis=1, tiled=True)
    w_full = lax.all_gather(w_columns, "tp", axis=0, tiled=True)
    accumulated_total = group_sums(flat_mixed, w_full, group_count)
    result = accumulated_total.reshape(token_rows.shape[0], token_rows.shape[1], -1)
    return result.astype(jnp.bfloat16)


MESH = pl.DeviceIdType.MESH
CORES = 2
PIECES = 2
BITS = 4
EARLY = 2
HOLD = 5
scope = jax.named_scope


def recur_one(proj_ref, shift_ref, gap_ref, gain_ref, out_ref, i, own):
    f32 = jnp.float32
    bf16 = jnp.bfloat16
    length = proj_ref.shape[1]

    def cols(p):
        return proj_ref[i, :, p * KEY : (p + 1) * KEY]

    queries = cols(0).astype(f32)
    queries = queries * jax.nn.sigmoid(queries)
    values = cols(1)
    shift = shift_ref[i].astype(f32)
    row = lax.broadcasted_iota(jnp.int32, (length, length), 0)
    col = lax.broadcasted_iota(jnp.int32, (length, length), 1)
    near = row // BLOCK == col // BLOCK
    row = lax.broadcasted_iota(jnp.int32, (BLOCK, BLOCK), 0)
    col_b = lax.broadcasted_iota(jnp.int32, (BLOCK, BLOCK), 1)
    seen = [row >= col_b, row <= col_b]
    row_l = lax.broadcasted_iota(jnp.int32, (length, length), 0)
    order = [row_l >= col, row_l <= col]
    blocks = length // BLOCK
    keys, here = [], []
    for d in range(2):
        key = gap_ref[d : d + 1, own] * jax.nn.sigmoid(-cols(2 + d).astype(f32))
        decay = jnp.log1p(-key) + shift
        high = decay.astype(bf16)
        rest = decay - high.astype(f32)
        middle = rest.astype(bf16)
        low = (rest - middle.astype(f32)).astype(bf16)
        tri = jnp.where(jnp.logical_and(near, order[d]), 1.0, 0.0).astype(bf16)
        sums = jnp.dot(
            tri, jnp.concatenate([high, middle, low], axis=1), preferred_element_type=f32
        )
        here.append(sums[:, :KEY] + (sums[:, KEY : 2 * KEY] + sums[:, 2 * KEY :]))
        keys.append(key)
    state = [None, None]
    outs = [[None, None] for _ in range(blocks)]
    for step in range(blocks):
        for d in range(2):
            n = step if d == 0 else blocks - 1 - step
            at = slice(n * BLOCK, (n + 1) * BLOCK)
            q, k, v, h = queries[at], keys[d][at], values[at], here[d][at]
            edge = h[BLOCK - 1 : BLOCK] if d == 0 else h[0:1]
            anchor = h[BLOCK // 2 : BLOCK // 2 + 1]
            scores = lax.dot_general(
                (q * jnp.exp(h - anchor)).astype(bf16),
                (k * jnp.exp(anchor - h)).astype(bf16),
                (((1,), (1,)), ((), ())),
                preferred_element_type=f32,
            )
            scores = jnp.where(seen[d], scores, 0.0).astype(bf16)
            out = jnp.dot(scores, v, preferred_element_type=f32)
            if state[d] is not None:
                out = out + lax.dot_general(
                    (q * jnp.exp(h)).astype(bf16),
                    state[d].astype(bf16),
                    (((1,), (1,)), ((), ())),
                    preferred_element_type=f32,
                )
            outs[n][d] = out
            if step < blocks - 1:
                fresh = lax.dot_general(
                    v,
                    (k * jnp.exp(edge - h)).astype(bf16),
                    (((0,), (0,)), ((), ())),
                    preferred_element_type=f32,
                )
                state[d] = fresh if state[d] is None else state[d] * jnp.exp(edge) + fresh
    for n in range(blocks):
        out_ref[n * BLOCK : (n + 1) * BLOCK] = outs[n][0] + outs[n][1]
    combined = out_ref[...]
    normed = combined * lax.rsqrt(jnp.mean(combined * combined, axis=-1, keepdims=True) + norm_eps)
    gate = cols(4).astype(f32)
    return (normed * gain_ref[...] * (gate * jax.nn.sigmoid(gate))).astype(bf16)


def layer_kernel(
    sizes,
    token_ref,
    norm_ref,
    shift_ref,
    wq_ref,
    wv_ref,
    wf_ref,
    wb_ref,
    wg_ref,
    gap_ref,
    gain_ref,
    w_ref,
    out_ref,
    rows_in,
    wide,
    raw_shift,
    own_shift,
    shifts,
    acts,
    weights,
    begun,
    proj,
    summed,
    mixed,
    heads,
    matrix,
    partial,
    landed,
    load_sem,
    az_out,
    az_in,
    ax_out,
    ax_in,
    ac_out,
    ac_in,
    wz_out,
    wz_in,
    wy_out,
    wy_in,
    sz_out,
    sz_in,
    oz_out,
    oz_in,
    oy_out,
    oy_in,
    oc_out,
    oc_in,
    m_out,
    m_in,
    p_out,
    p_in,
):
    bf16 = jnp.bfloat16
    f32 = jnp.float32
    n_grp, n_sp, n_tp = sizes
    n_x = n_tp // CORES
    g = lax.axis_index("grp")
    s = lax.axis_index("sp")
    t = lax.axis_index("tp")
    x = t // CORES
    c = t % CORES
    twin = x * CORES + (1 - c)
    across = (1 - x) * CORES + c
    seqs = acts.shape[0]
    span = token_ref.shape[0]
    positions = n_tp * span
    depth = wq_ref.shape[0]
    half = depth // n_grp
    width = w_ref.shape[1]
    lot = seqs // PIECES
    bit = half // BITS
    sources = (wq_ref, wv_ref, wf_ref, wb_ref, wg_ref)
    count = len(sources)
    groups = ((0, 2), (2, 4), (4, 5))
    last = n_sp - 1
    z_at = [lax.rem(s + k, n_sp) for k in range(n_sp)]
    z_from = [lax.rem(s + n_sp - k, n_sp) for k in range(n_sp)]
    core_at = [c, 1 - c]

    def span_at(where, size):
        return pl.ds(pl.multiple_of(where * size, size), size)

    def lanes(where, size=KEY):
        return span_at(where, size)

    def remote(src, dst, out_sem, in_sem, peer):
        return pltpu.make_async_remote_copy(
            src_ref=src,
            dst_ref=dst,
            send_sem=out_sem,
            recv_sem=in_sem,
            device_id=peer,
            device_id_type=MESH,
        )

    def tally(ref, out_sem, in_sem):
        return remote(ref, ref, out_sem, in_sem, (g, s, twin))

    def inside(place):
        return jnp.logical_and(place >= 0, place < n_sp)

    def step_of(up):
        return 1 if up else -1

    def slot(up, d):
        return 1 + d if up else n_sp + d

    def end(up):
        return 0 if up else last

    def sends(up, d):
        return jnp.logical_and(inside(s + step_of(up)), inside(s - step_of(up) * d))

    def gets(up, d):
        return inside(s - step_of(up) * (d + 1))

    def each(d, visit):
        for up in (True, False):

            @pl.when(gets(up, d))
            def _():
                visit(up, d, s - step_of(up) * (d + 1))

    load_rows = pltpu.make_async_copy(token_ref, rows_in, load_sem.at[0])
    load_shift = pltpu.make_async_copy(shift_ref, raw_shift, load_sem.at[1])
    load_rows.start()
    load_shift.start()
    peers = [(g, z_at[k], x * CORES + core_at[o]) for k in range(n_sp) for o in range(CORES)]
    peers = peers[1:] + [(g, s, across), (1 - g, s, t)]
    barrier = pltpu.get_barrier_semaphore()
    for peer in peers:
        pl.semaphore_signal(barrier, inc=1, device_id=peer, device_id_type=MESH)
    own_rows = span_at(s, depth)
    for p, w in enumerate(sources):
        pltpu.make_async_copy(
            w.at[:, lanes(s)], weights.at[own_rows, pl.ds(p * KEY, KEY)], load_sem.at[2]
        ).start()
    w_rows = span_at(c, depth)
    w_own = pltpu.make_async_copy(w_ref, matrix.at[w_rows, lanes(s, width)], load_sem.at[3])
    w_own.start()

    here_rows = span_at(s * n_tp + t, span)
    with scope("wait_rows"):
        load_rows.wait()
    rows = rows_in[...].astype(f32)
    scale = lax.rsqrt(jnp.mean(rows * rows, axis=-1, keepdims=True) + norm_eps)
    wide[...] = rows * scale * norm_ref[...]
    for q in range(seqs):
        acts[q, here_rows, :] = wide[:, q, :].astype(bf16)
    with scope("barrier"):
        pl.semaphore_wait(barrier, len(peers))

    def block(where_s, where_t):
        return acts.at[:, span_at(where_s * n_tp + where_t, span), :]

    def act_z(up, d, piece):
        at = span_at((s - step_of(up) * d) * n_tp + t, span)
        here = acts.at[pl.ds(piece * lot, lot), at, :]
        index = slot(up, d) - 1
        peer = (g, s + step_of(up), t)
        return remote(here, here, az_out.at[index], az_in.at[index, piece], peer)

    def act_x(index, origin):
        here = block(origin, t)
        return remote(here, here, ax_out, ax_in.at[index], (g, s, across))

    def act_c(far, origin):
        here = block(origin, across if far else t)
        return remote(here, here, ac_out, ac_in, (g, s, twin))

    part = span_at(g, half)

    def w_z(k, p):
        src = sources[p].at[part, lanes(z_at[k])]
        dst = weights.at[span_at(s * n_grp + g, half), pl.ds(p * KEY, KEY)]
        return remote(src, dst, wz_out, wz_in.at[k - 1, p], (g, z_at[k], t))

    def w_block(k, p):
        return weights.at[span_at(z_from[k] * n_grp + g, half), pl.ds(p * KEY, KEY)]

    def w_y(k, p, index):
        here = w_block(k, p)
        return remote(here, here, wy_out, wy_in.at[index], (1 - g, s, t))

    place = span_at(s, positions)

    def s_z(k):
        return remote(own_shift.at[z_at[k]], shifts.at[:, place, :], sz_out, sz_in, (g, z_at[k], t))

    def o_block(where_s, where_g, where_c, piece):
        at = pl.multiple_of(where_c * depth + where_g * half + piece * bit, bit)
        return matrix.at[pl.ds(at, bit), lanes(where_s, width)]

    def o_z(up, d, piece):
        here = o_block(s - step_of(up) * d, g, c, piece)
        src = w_ref.at[span_at(g * BITS + piece, bit), :] if d == 0 else here
        index = slot(up, d) - 1
        peer = (g, s + step_of(up), t)
        return remote(src, here, oz_out.at[index], oz_in.at[index, piece], peer)

    def o_y(index, origin, piece):
        here = o_block(origin, g, c, piece)
        return remote(here, here, oy_out, oy_in.at[index - 1, piece], (1 - g, s, t))

    def o_c(far, index, origin, piece):
        here = o_block(origin, 1 - g if far else g, c, piece)
        return remote(here, here, oc_out, oc_in.at[index], (g, s, twin))

    def ahead(up, hops, groups_now):
        for hop in hops:
            k = hop if up else n_sp - hop
            go_up = s + k < n_sp

            @pl.when(go_up if up else jnp.logical_not(go_up))
            def _():
                for group in groups_now:
                    if group is None:
                        s_z(k).start()
                    else:
                        for p in range(*groups[group]):
                            w_z(k, p).start()

    every_group = range(len(groups))
    every_hop = range(1, n_sp)

    def neighbour(up):
        return s == (1 if up else last - 1)

    def o_first(up, pieces):
        @pl.when(sends(up, 0))
        def _():
            for piece in pieces:
                o_z(up, 0, piece).start()

    def issue(up):
        @pl.when(s == end(up))
        def _():
            o_first(up, range(BITS))
            ahead(up, (1,), every_group)

        @pl.when(neighbour(not up))
        def _():
            ahead(up, every_hop[::-1], every_group)
            o_first(up, range(BITS))
            ahead(up, every_hop, (None,))

        @pl.when(neighbour(up))
        def _():
            ahead(up, every_hop[::-1], every_group)
            o_first(up, range(EARLY))
            ahead(up, every_hop, (None,))
            o_first(up, range(EARLY, BITS))

    def issue_far():
        for up in (True, False):

            @pl.when(s == end(up))
            def _():
                ahead(up, every_hop[1:], every_group)
                ahead(up, every_hop, (None,))

    for piece in range(PIECES):
        for up in (True, False):

            @pl.when(sends(up, 0))
            def _():
                act_z(up, 0, piece).start()

    act_x(0, s).start()
    act_c(0, s).start()
    with scope("wait_shift_load"):
        load_shift.wait()
    for q in range(seqs):
        values = raw_shift[:, q, :].astype(bf16)
        for k in range(n_sp):
            own_shift[k, q] = values[:, k * KEY : (k + 1) * KEY]
    shifts[:, place, :] = own_shift[s]
    for up in (True, False):

        @pl.when(s == end(up))
        def _():
            issue(up)

    def swap(d, groups_now, match=True, late=False):
        for up in (True, False):

            @pl.when(jnp.logical_and(gets(up, d), match))
            def _():
                k = d + 1 if up else last - d
                for group in groups_now:
                    for p in range(*groups[group]):
                        tally(w_block(k, p), wz_out, wz_in.at[k - 1, p]).wait_recv()
                        w_y(k, p, 1 + group if late else 0).start()

    at_end = jnp.logical_or(s == 0, s == last)
    late_source = jnp.where(at_end, last - s, lax.rem(s + 2, n_sp))

    def swap_late(group):
        swap(last - 1, (group,), at_end, True)
        swap(last - 2, (group,), jnp.logical_not(at_end), True)

    for d in range(last):
        if d == last - 1:
            with scope("swap_end"):
                for hop in range(last - 2, 0, -1):
                    swap(hop, every_group, at_end)
        for piece in range(PIECES):

            def arrived(up, d, origin):
                act_z(up, d, piece).wait_recv()
                if d + 1 < last:

                    @pl.when(sends(up, d + 1))
                    def _():
                        act_z(up, d + 1, piece).start()

                if piece == PIECES - 1:
                    act_x(slot(up, d), origin).start()
                    act_c(0, origin).start()

            with scope(f"act_z{d}_{piece}"):
                each(d, arrived)
        if d + 1 < last:
            for up in (True, False):

                @pl.when(s == (d + 1 if up else last - 1 - d))
                def _():
                    issue(up)

    o_own = remote(w_ref, matrix.at[w_rows, lanes(s, width)], oc_out, oc_in.at[0], (g, s, twin))
    o_own.start()

    def relay(index, origin):
        act_x(index, origin).wait_recv()
        act_c(1, origin).start()

    def o_take(up, d, origin, pieces=range(BITS)):
        for piece in pieces:
            o_z(up, d, piece).wait_recv()
            if d + 1 < last:

                @pl.when(sends(up, d + 1))
                def _():
                    o_z(up, d + 1, piece).start()

            o_y(slot(up, d), origin, piece).start()
            o_c(0, slot(up, d), origin, piece).start()

    def o_swapped(up, d, origin):
        for piece in range(BITS):
            o_y(slot(up, d), origin, piece).wait_recv()
            o_c(1, slot(up, d), origin, piece).start()

    with scope("take_early"):
        for up in (True, False):

            @pl.when(neighbour(up))
            def _():
                o_take(up, 0, s - step_of(up))

    with scope("swap_near0"):
        swap(0, every_group[:1])
    issue_far()
    with scope("swap_near1"):
        swap(0, every_group[1:])
    with scope("relay"):
        relay(0, s)
        for d in range(last):
            each(d, lambda up, d, origin: relay(slot(up, d), origin))

    def take_late(pieces, where):
        for up in (True, False):
            match = jnp.logical_and(gets(up, 0), jnp.logical_not(neighbour(up)))

            @pl.when(jnp.logical_and(match, where))
            def _():
                o_take(up, 0, s - step_of(up), pieces)

    def project(group):
        at = slice(groups[group][0] * KEY, groups[group][1] * KEY)
        from_late = span_at(late_source, depth)
        with scope(f"wait_w{group}"):
            block = weights.at[pl.ds(0, half), at]
            tally(block, wy_out, wy_in.at[1 + group]).wait_recv()

        def one(q, carry):
            more = jnp.dot(
                acts[q, :, from_late], weights[from_late, at], preferred_element_type=f32
            )
            proj[q, :, at] = (begun[q, :, at] + more).astype(bf16)
            return carry

        with scope(f"project{group}"):
            lax.fori_loop(0, seqs, one, 0)

    def begin(q, carry):
        total = None
        for i in range(1, n_sp):
            rows_now = span_at(lax.rem(late_source + i, n_sp), depth)
            more = jnp.dot(acts[q, :, rows_now], weights[rows_now, :], preferred_element_type=f32)
            total = more if total is None else total + more
        begun[q] = total
        return carry

    with scope("joined"):
        tally(acts.at[pl.ds(0, seqs // CORES)], ac_out, ac_in).wait_recv()
        here = weights.at[own_rows, :]
        pltpu.make_async_copy(here, here, load_sem.at[2]).wait()
    with scope("wait_w"):
        tally(weights.at[pl.ds(0, (last - 1) * half), :], wy_out, wy_in.at[0]).wait_recv()
    with scope("take_part_end"):
        take_late(range(BITS // 2), at_end)
    with scope("begin"):
        lax.fori_loop(0, seqs, begin, 0)
    for group in every_group:
        with scope(f"swap_late{group}"):
            swap_late(group)
    with scope("take_rest_end"):
        take_late(range(BITS // 2, BITS), at_end)
    project(0)
    project(1)
    with scope("act_drain"):
        tally(acts.at[:, pl.ds(0, n_sp * span), :], ax_out, ax_in.at[0]).wait_send()
        tally(acts.at[pl.ds(0, seqs // CORES)], ac_out, ac_in).wait_send()
        for d in range(last):
            for up in (True, False):

                @pl.when(sends(up, d))
                def _():
                    index = slot(up, d) - 1
                    tally(block(s, t), az_out.at[index], az_in.at[index, 0]).wait_send()

    with scope("take_part"):
        take_late(range(EARLY), jnp.logical_not(at_end))
    project(2)
    with scope("wait_shift"):
        tally(shifts.at[:, pl.ds(0, last * positions), :], sz_out, sz_in).wait_recv()

    targets = [(k, o) for k in range(n_sp) for o in range(CORES) if k or o]

    def m_move(q, k, o):
        return remote(
            mixed.at[q, z_at[k], :, core_at[o]],
            heads.at[:, q, :, lanes(c * n_sp + s, VAL)],
            m_out,
            m_in.at[q // lot],
            (g, z_at[k], x * CORES + core_at[o]),
        )

    def send_mixed(seqs_now, held):
        for k, o in targets:
            crossing = jnp.logical_and(at_end, jnp.abs(z_at[k] - s) > HOLD)

            @pl.when(crossing if held else jnp.logical_not(crossing))
            def _():
                for q in seqs_now:
                    m_move(q, k, o).start()

    def recur(pair, carry):
        for i in range(2):
            q = 2 * pair + i
            value = recur_one(proj, shifts, gap_ref, gain_ref, summed.at[i], q, lanes(s))
            mixed[q] = value.reshape(n_sp, n_x, CORES, span, VAL)
            heads[:, q, :, lanes(c * n_sp + s, VAL)] = mixed[q, s, :, c]
        send_mixed(range(2 * pair, 2 * pair + 2), False)
        return carry

    def take_second(pieces, where):
        for up in (True, False):

            @pl.when(jnp.logical_and(gets(up, 1), where))
            def _():
                o_take(up, 1, s - 2 * step_of(up), pieces)

    def take_third(pieces):
        each(last - 1, lambda up, d, origin: o_take(up, d, origin, pieces))

    for pair in range(seqs // 2):
        with scope(f"recur{pair}"):
            recur(pair, 0)
        if pair == 0:
            with scope("take_second"):
                take_second(range(EARLY), at_end)
    with scope("take_late"):
        take_late(range(EARLY, BITS), jnp.logical_not(at_end))
    with scope("w_drain"):
        tally(own_shift.at[pl.ds(0, last)], sz_out, sz_in).wait_send()
        every = weights.at[pl.ds(0, last * half), :]
        tally(every, wz_out, wz_in.at[0, 0]).wait_send()
        tally(every, wy_out, wy_in.at[0]).wait_send()
    w_own.wait()

    def p_move(index, origin, rows_now, part):
        at = lanes(origin, width)
        return remote(
            partial.at[1 - x, rows_now, :, at],
            landed.at[rows_now, :, at],
            p_out,
            p_in.at[index, part],
            (g, s, across),
        )

    every_seq = (slice(0, seqs),)
    lots = tuple(slice(h * lot, (h + 1) * lot) for h in range(PIECES))

    def strip(index, origin, rows_now, part):
        at = lanes(origin, width)
        lines = heads[:, rows_now].reshape(-1, heads.shape[-1])
        partial[:, rows_now, :, at] = (
            jnp.dot(lines, matrix[:, at], preferred_element_type=f32)
            .astype(bf16)
            .reshape(n_x, -1, span, width)
        )
        p_move(index, origin, rows_now, part).start()

    def arrived_strip(index, origin):
        at = lanes(origin, width)
        tally(matrix.at[pl.ds(0, depth), at], oc_out, oc_in.at[index]).wait_recv()

    def own_strip(part):
        strip(0, s, lots[part], part)

    def near_strip(part):
        def visit(up, d, origin):
            if part == 0:
                arrived_strip(slot(up, d), origin)
            strip(slot(up, d), origin, lots[part], part)

        each(0, visit)

    def far_strip(up, d, origin):
        arrived_strip(slot(up, d), origin)
        strip(slot(up, d), origin, every_seq[0], 0)

    def mixed_in(part):
        here = heads.at[:, pl.ds(0, lot), :, pl.ds(0, len(targets) * VAL)]
        tally(here, m_out, m_in.at[part]).wait_recv()

    with scope("o_pass1"):
        take_second(range(EARLY, BITS), at_end)
        send_mixed(range(seqs), True)
        take_second(range(BITS), jnp.logical_not(at_end))
    with scope("o_pass2a"):
        take_third(range(BITS // 2))
    with scope("o_swapped0"):
        each(0, o_swapped)
    with scope("wait_m0"):
        mixed_in(0)
    with scope("own_strip0"):
        arrived_strip(0, s)
        own_strip(0)
    with scope("near_strip0"):
        near_strip(0)
    with scope("o_pass2b"):
        take_third(range(BITS // 2, BITS))
    with scope("wait_m1"):
        for part in range(1, PIECES):
            mixed_in(part)
    with scope("strips1"):
        for part in range(1, PIECES):
            own_strip(part)
            near_strip(part)
    for d in range(1, last):
        with scope(f"o_swapped{d}"):
            each(d, o_swapped)
        with scope(f"strip{d}"):
            each(d, far_strip)

    def finish(index, origin, parts):
        for part, rows_now in enumerate(parts):
            p_move(index, origin, rows_now, part).wait_recv()
            at = lanes(origin, width)
            total = partial[x, rows_now, :, at].astype(f32) + landed[rows_now, :, at].astype(f32)
            out_ref[rows_now, :, at] = total.astype(bf16)

    with scope("finish"):
        finish(0, s, lots)
        for d in range(last):
            parts = every_seq if d else lots
            each(d, lambda up, d, origin: finish(slot(up, d), origin, parts))
    with scope("drain"):
        here = heads.at[:, :, :, pl.ds(0, len(targets) * VAL)]
        tally(here, m_out, m_in.at[0]).wait_send()
        strips = matrix.at[pl.ds(0, half), pl.ds(0, last * width)]
        tally(strips, oy_out, oy_in.at[0, 0]).wait_send()
        tally(matrix.at[pl.ds(0, depth), :], oc_out, oc_in.at[0]).wait_send()
        tally(landed, p_out, p_in.at[0, 0]).wait_send()
        for d in range(last):
            for up in (True, False):

                @pl.when(sends(up, d))
                def _():
                    index = slot(up, d) - 1
                    here = matrix.at[pl.ds(0, half), pl.ds(0, width)]
                    tally(here, oz_out.at[index], oz_in.at[index, 0]).wait_send()


def layer(sizes, tokens, norm_gain, shift, sources, gap, gain, w_out):
    n_grp, n_sp, n_tp = sizes
    n_x = n_tp // CORES
    span, seqs, model = tokens.shape
    length = n_sp * n_tp * span
    count = len(sources)
    depth, width = w_out.shape
    slots = 2 * n_sp - 1
    dma = pltpu.SemaphoreType.DMA
    hbm = pl.BlockSpec(memory_space=pltpu.HBM)
    vmem = pl.BlockSpec(memory_space=pltpu.VMEM)
    bf16 = jnp.bfloat16
    return pl.pallas_call(
        functools.partial(layer_kernel, sizes),
        out_shape=jax.ShapeDtypeStruct((seqs, span, n_sp * width), bf16),
        in_specs=[hbm, vmem] + [hbm] * (1 + count) + [vmem, vmem, hbm],
        out_specs=vmem,
        scratch_shapes=[
            pltpu.VMEM(tokens.shape, bf16),
            pltpu.VMEM(tokens.shape, jnp.float32),
            pltpu.VMEM(shift.shape, shift.dtype),
            pltpu.VMEM((n_sp, seqs, n_tp * span, KEY), bf16),
            pltpu.VMEM((seqs, length, KEY), bf16),
            pltpu.VMEM((seqs, length, model), bf16),
            pltpu.VMEM((model, count * KEY), bf16),
            pltpu.VMEM((seqs, length, count * KEY), jnp.float32),
            pltpu.VMEM((seqs, length, count * KEY), bf16),
            pltpu.VMEM((2, length, VAL), jnp.float32),
            pltpu.VMEM((seqs, n_sp, n_x, CORES, span, VAL), bf16),
            pltpu.VMEM((n_x, seqs, span, CORES * depth), bf16),
            pltpu.VMEM((CORES * depth, n_sp * width), bf16),
            pltpu.VMEM((n_x, seqs, span, n_sp * width), bf16),
            pltpu.VMEM((seqs, span, n_sp * width), bf16),
            dma((4,)),
            dma((slots - 1,)),
            dma((slots - 1, PIECES)),
            dma,
            dma((slots,)),
            dma,
            dma,
            dma,
            dma((n_sp - 1, count)),
            dma,
            dma((4,)),
            dma,
            dma,
            dma((slots - 1,)),
            dma((slots - 1, BITS)),
            dma,
            dma((slots - 1, BITS)),
            dma,
            dma((slots,)),
            dma,
            dma((PIECES,)),
            dma,
            dma((slots, PIECES)),
        ],
        compiler_params=pltpu.CompilerParams(
            collective_id=0, has_side_effects=True, vmem_limit_bytes=56 * 1024 * 1024
        ),
    )(tokens, norm_gain, shift, *sources, gap, gain, w_out)


def head_shards(
    sizes,
    tokens,
    norm_gain,
    w_query,
    w_value,
    w_fwd_gate,
    w_bwd_gate,
    w_out_gate,
    floor_gap,
    decay_shift,
    head_gain,
    w_out,
):
    return layer(
        sizes,
        tokens,
        norm_gain.reshape(1, 1, -1),
        decay_shift,
        (w_query, w_value, w_fwd_gate, w_bwd_gate, w_out_gate),
        floor_gap,
        head_gain.reshape(1, VAL),
        w_out,
    ).transpose(1, 0, 2)


def by_heads(mesh):
    n_sp, n_tp = mesh.shape["sp"], mesh.shape["tp"]

    def run(*arrays):
        tokens, w_query = arrays[0], arrays[2]
        heads_here = w_query.shape[1] // KEY // n_tp
        span = tokens.shape[0] // (n_sp * n_tp)
        sizes = (mesh.shape["grp"], n_sp, n_tp)
        fits = heads_here == n_sp and n_sp == CORES * 2 and n_tp == 2 * CORES and span % 16 == 0
        fits = fits and sizes[0] == 2 and tokens.shape[1] // sizes[0] % PIECES == 0
        fits = fits and tokens.shape[0] % BLOCK == 0 and tokens.shape[0] <= 512
        body = functools.partial(head_shards, sizes) if fits else shards
        return mapped(body, mesh)(*arrays)

    return run


def mapped(body, mesh):
    return jax.shard_map(
        body,
        mesh=mesh,
        in_specs=(
            P(("sp", "tp"), "grp", None),
            P(),
            P("sp", "tp"),
            P("sp", "tp"),
            P("sp", "tp"),
            P("sp", "tp"),
            P("sp", "tp"),
            P(None, "tp"),
            P("sp", "grp", "tp"),
            P(),
            P("tp", "sp"),
        ),
        out_specs=P(("sp", "tp"), "grp", None),
        check_vma=False,
    )


def solution(mesh):
    return by_heads(mesh)
```

```python
import functools

import jax
import jax.numpy as jnp
from jax import lax
from jax.experimental import pallas as pl
from jax.experimental.pallas import tpu as pltpu
from jax.sharding import PartitionSpec as P

KEY = 128
VAL = 128
BLOCK = 64


norm_eps = 1e-06
highest = lax.Precision.HIGHEST


def carried_in(x, axis, join, neutral, backward):
    count = lax.axis_size(axis)
    place = lax.axis_index(axis)
    ahead = count - 1 - place if backward else place
    gathered = jax.tree.map(
        lambda a, kind: lax.all_gather(a.astype(kind), axis), x, (jnp.bfloat16, jnp.bfloat16)
    )
    state = jax.tree.map(lambda a, e: jnp.zeros_like(a) + jnp.asarray(e, a.dtype), x, neutral)

    def one(turn, state):
        source = count - 1 - turn if backward else turn
        return join(
            state,
            jax.tree.map(
                lambda a, own: lax.dynamic_index_in_dim(a, source, 0, False).astype(own.dtype),
                gathered,
                x,
            ),
        )

    return lax.fori_loop(0, ahead, one, state)


def split_blocks(array):
    return array.reshape(array.shape[0] // BLOCK, BLOCK, *array.shape[1:])


def prepare_chain(queries, key_cols, values, log_decay):
    query_blocks = split_blocks(queries)
    key_blocks = split_blocks(key_cols)
    value_blocks = split_blocks(values)
    running = jnp.cumsum(split_blocks(log_decay), axis=1)
    block_end = running[:, -1]
    block_state = jnp.einsum(
        "nsbhk,nsbhe->nbhke",
        key_blocks * jnp.exp(block_end[:, None] - running),
        value_blocks,
        precision=highest,
    )
    carry_state = jnp.zeros_like(block_state[0])
    log_total = jnp.zeros_like(block_end[0])
    offsets = [log_total]
    carry_state = jnp.exp(block_end[0])[..., None] * carry_state + block_state[0]
    log_total = block_end[0]
    return (
        query_blocks,
        key_blocks,
        value_blocks,
        running,
        block_state,
        jnp.stack(offsets),
        log_total,
        carry_state,
    )


def local_pass(chain, carry_state):
    query_blocks, key_blocks, value_blocks, running, block_state = (
        chain[0],
        chain[1],
        chain[2],
        chain[3],
        chain[4],
    )
    block_len = running.shape[1]
    earlier_mask = jnp.arange(block_len)[:, None] >= jnp.arange(block_len)[None, :]
    here = running[0]
    anchor = here[:1]
    query_scaled = query_blocks[0] * jnp.exp(here - anchor)
    key_scaled = key_blocks[0] * jnp.exp(anchor - here)
    scores = jnp.einsum("tbhk,sbhk->bhts", query_scaled, key_scaled, precision=highest)
    scores = jnp.where(earlier_mask, scores, 0.0)
    within = jnp.einsum("bhts,sbhe->tbhe", scores, value_blocks[0], precision=highest)
    carried = jnp.einsum(
        "tbhk,bhke->tbhe", query_blocks[0] * jnp.exp(here), carry_state, precision=highest
    )
    outputs = within + carried
    return outputs


def combine(earlier, later):
    return (earlier[0] + later[0], jnp.exp(later[0])[..., None] * earlier[1] + later[1])


def group_sums(flat_mixed, weight_lines, group_count):
    group_width = flat_mixed.shape[1] // group_count
    accumulated_total = jnp.zeros((flat_mixed.shape[0], weight_lines.shape[1]), jnp.float32)
    for tp_group in range(group_count):
        first_column = tp_group * group_width
        partial_value = jnp.dot(
            flat_mixed[:, first_column : first_column + group_width],
            weight_lines[first_column : first_column + group_width],
            preferred_element_type=jnp.float32,
        ).astype(jnp.bfloat16)
        accumulated_total = accumulated_total + lax.optimization_barrier(partial_value).astype(
            jnp.float32
        )
    return accumulated_total


def shards(
    tokens,
    norm_gain,
    w_query,
    w_value,
    w_fwd_gate,
    w_bwd_gate,
    w_out_gate,
    floor_gap,
    decay_shift,
    head_gain,
    w_out,
):
    token_f32 = tokens.astype(jnp.float32)
    scale_rows = lax.rsqrt(jnp.mean(token_f32 * token_f32, axis=-1, keepdims=True) + norm_eps)
    normed = (token_f32 * scale_rows * norm_gain).astype(jnp.bfloat16)
    weights = (
        lax.all_gather(w_query, "sp", axis=0, tiled=True),
        lax.all_gather(w_value, "sp", axis=0, tiled=True),
        lax.all_gather(w_fwd_gate, "sp", axis=0, tiled=True),
        lax.all_gather(w_bwd_gate, "sp", axis=0, tiled=True),
        lax.all_gather(w_out_gate, "sp", axis=0, tiled=True),
    )
    piece_rows = lax.all_gather(normed, "tp", axis=0, tiled=True)
    flat_rows = piece_rows.reshape(-1, piece_rows.shape[2])
    columns = [
        jnp.dot(flat_rows, matrix, preferred_element_type=jnp.float32).astype(jnp.bfloat16)
        for matrix in weights
    ]
    projected = lax.optimization_barrier(
        jnp.concatenate(columns, axis=1).reshape(piece_rows.shape[0], piece_rows.shape[1], -1)
    )
    key_width = w_query.shape[1]
    value_width = w_value.shape[1]
    heads_here = key_width // KEY
    extent_rows = projected.shape[0]
    seq_count = projected.shape[1]
    bounds_list = [
        0,
        key_width,
        key_width + value_width,
        2 * key_width + value_width,
        3 * key_width + value_width,
        3 * key_width + 2 * value_width,
    ]

    def section_part(position, feature_lanes):
        picked = projected[:, :, bounds_list[position] : bounds_list[position + 1]].astype(
            jnp.float32
        )
        return picked.reshape(extent_rows, seq_count, heads_here, feature_lanes)

    queries = jax.nn.silu(section_part(0, KEY))
    values = section_part(1, VAL)
    shift = decay_shift.reshape(extent_rows, seq_count, heads_here, KEY)
    key_fwd = floor_gap[0].reshape(heads_here, KEY) * jax.nn.sigmoid(-section_part(2, KEY))
    key_bwd = floor_gap[1].reshape(heads_here, KEY) * jax.nn.sigmoid(-section_part(3, KEY))
    decay_fwd = jnp.log1p(-key_fwd) + shift
    decay_bwd = jnp.log1p(-key_bwd) + shift
    fwd_chain = prepare_chain(queries, key_fwd, values, decay_fwd)
    bwd_chain = prepare_chain(queries[::-1], key_bwd[::-1], values[::-1], decay_bwd[::-1])
    identity_pair = (jnp.zeros_like(fwd_chain[6]), jnp.zeros_like(fwd_chain[7]))
    fwd_in = carried_in((fwd_chain[6], fwd_chain[7]), "sp", combine, identity_pair, False)[1]
    bwd_in = carried_in((bwd_chain[6], bwd_chain[7]), "sp", combine, identity_pair, True)[1]
    out_fwd = local_pass(fwd_chain, fwd_in)
    out_bwd = local_pass(bwd_chain, bwd_in)
    combined = out_fwd + out_bwd[::-1]
    head_normed = (
        combined
        * lax.rsqrt(jnp.mean(combined * combined, axis=-1, keepdims=True) + norm_eps)
        * head_gain
    )
    gate_value = jax.nn.silu(projected[:, :, bounds_list[4] : bounds_list[5]].astype(jnp.float32))
    mixed = (head_normed.reshape(extent_rows, seq_count, value_width) * gate_value).astype(
        jnp.bfloat16
    )
    token_rows = lax.all_to_all(mixed, "tp", split_axis=0, concat_axis=2, tiled=True)
    flat_mixed = token_rows.reshape(-1, token_rows.shape[2])
    group_count = lax.axis_size("tp")
    w_columns = lax.all_gather(w_out, "sp", axis=1, tiled=True)
    w_full = lax.all_gather(w_columns, "tp", axis=0, tiled=True)
    accumulated_total = group_sums(flat_mixed, w_full, group_count)
    result = accumulated_total.reshape(token_rows.shape[0], token_rows.shape[1], -1)
    return result.astype(jnp.bfloat16)


MESH = pl.DeviceIdType.MESH
CORES = 2
PIECES = 2
BITS = 4
EARLY = 3
FREE = 1
scope = jax.named_scope


def recur_one(proj_ref, shift_ref, gap_ref, gain_ref, out_ref, i, own):
    f32 = jnp.float32
    bf16 = jnp.bfloat16
    length = proj_ref.shape[1]

    def cols(p):
        return proj_ref[i, :, p * KEY : (p + 1) * KEY]

    queries = cols(0).astype(f32)
    queries = queries * jax.nn.sigmoid(queries)
    values = cols(1)
    shift = shift_ref[i].astype(f32)
    row = lax.broadcasted_iota(jnp.int32, (length, length), 0)
    col = lax.broadcasted_iota(jnp.int32, (length, length), 1)
    near = row // BLOCK == col // BLOCK
    row = lax.broadcasted_iota(jnp.int32, (BLOCK, BLOCK), 0)
    col_b = lax.broadcasted_iota(jnp.int32, (BLOCK, BLOCK), 1)
    seen = [row >= col_b, row <= col_b]
    row_l = lax.broadcasted_iota(jnp.int32, (length, length), 0)
    order = [row_l >= col, row_l <= col]
    blocks = length // BLOCK
    keys, here = [], []
    for d in range(2):
        key = gap_ref[d : d + 1, own] * jax.nn.sigmoid(-cols(2 + d).astype(f32))
        decay = jnp.log1p(-key) + shift
        high = decay.astype(bf16)
        rest = decay - high.astype(f32)
        middle = rest.astype(bf16)
        low = (rest - middle.astype(f32)).astype(bf16)
        tri = jnp.where(jnp.logical_and(near, order[d]), 1.0, 0.0).astype(bf16)
        sums = jnp.dot(
            tri, jnp.concatenate([high, middle, low], axis=1), preferred_element_type=f32
        )
        here.append(sums[:, :KEY] + (sums[:, KEY : 2 * KEY] + sums[:, 2 * KEY :]))
        keys.append(key)
    state = [None, None]
    outs = [[None, None] for _ in range(blocks)]
    for step in range(blocks):
        for d in range(2):
            n = step if d == 0 else blocks - 1 - step
            at = slice(n * BLOCK, (n + 1) * BLOCK)
            q, k, v, h = queries[at], keys[d][at], values[at], here[d][at]
            edge = h[BLOCK - 1 : BLOCK] if d == 0 else h[0:1]
            anchor = h[BLOCK // 2 : BLOCK // 2 + 1]
            scores = lax.dot_general(
                (q * jnp.exp(h - anchor)).astype(bf16),
                (k * jnp.exp(anchor - h)).astype(bf16),
                (((1,), (1,)), ((), ())),
                preferred_element_type=f32,
            )
            scores = jnp.where(seen[d], scores, 0.0).astype(bf16)
            out = jnp.dot(scores, v, preferred_element_type=f32)
            if state[d] is not None:
                out = out + lax.dot_general(
                    (q * jnp.exp(h)).astype(bf16),
                    state[d].astype(bf16),
                    (((1,), (1,)), ((), ())),
                    preferred_element_type=f32,
                )
            outs[n][d] = out
            if step < blocks - 1:
                fresh = lax.dot_general(
                    v,
                    (k * jnp.exp(edge - h)).astype(bf16),
                    (((0,), (0,)), ((), ())),
                    preferred_element_type=f32,
                )
                state[d] = fresh if state[d] is None else state[d] * jnp.exp(edge) + fresh
    for n in range(blocks):
        out_ref[n * BLOCK : (n + 1) * BLOCK] = outs[n][0] + outs[n][1]
    combined = out_ref[...]
    normed = combined * lax.rsqrt(jnp.mean(combined * combined, axis=-1, keepdims=True) + norm_eps)
    gate = cols(4).astype(f32)
    return (normed * gain_ref[...] * (gate * jax.nn.sigmoid(gate))).astype(bf16)


def layer_kernel(
    sizes,
    token_ref,
    norm_ref,
    shift_ref,
    wq_ref,
    wv_ref,
    wf_ref,
    wb_ref,
    wg_ref,
    gap_ref,
    gain_ref,
    w_ref,
    out_ref,
    rows_in,
    wide,
    raw_shift,
    own_shift,
    shifts,
    acts,
    weights,
    begun,
    proj,
    summed,
    mixed,
    heads,
    matrix,
    partial,
    landed,
    load_sem,
    az_out,
    az_in,
    ax_out,
    ax_in,
    ac_out,
    ac_in,
    wz_out,
    wz_in,
    wy_out,
    wy_in,
    sz_out,
    sz_in,
    oz_out,
    oz_in,
    oy_out,
    oy_in,
    oc_out,
    oc_in,
    m_out,
    m_in,
    p_out,
    p_in,
):
    bf16 = jnp.bfloat16
    f32 = jnp.float32
    n_grp, n_sp, n_tp = sizes
    n_x = n_tp // CORES
    g = lax.axis_index("grp")
    s = lax.axis_index("sp")
    t = lax.axis_index("tp")
    x = t // CORES
    c = t % CORES
    twin = x * CORES + (1 - c)
    across = (1 - x) * CORES + c
    seqs = acts.shape[0]
    span = token_ref.shape[0]
    positions = n_tp * span
    depth = wq_ref.shape[0]
    half = depth // n_grp
    width = w_ref.shape[1]
    lot = seqs // PIECES
    bit = half // BITS
    sources = (wq_ref, wv_ref, wf_ref, wb_ref, wg_ref)
    count = len(sources)
    groups = ((0, 2), (2, 4), (4, 5))
    last = n_sp - 1
    z_at = [lax.rem(s + k, n_sp) for k in range(n_sp)]
    z_from = [lax.rem(s + n_sp - k, n_sp) for k in range(n_sp)]
    core_at = [c, 1 - c]

    def span_at(where, size):
        return pl.ds(pl.multiple_of(where * size, size), size)

    def lanes(where, size=KEY):
        return span_at(where, size)

    def remote(src, dst, out_sem, in_sem, peer):
        return pltpu.make_async_remote_copy(
            src_ref=src,
            dst_ref=dst,
            send_sem=out_sem,
            recv_sem=in_sem,
            device_id=peer,
            device_id_type=MESH,
        )

    def tally(ref, out_sem, in_sem):
        return remote(ref, ref, out_sem, in_sem, (g, s, twin))

    def inside(place):
        return jnp.logical_and(place >= 0, place < n_sp)

    def step_of(up):
        return 1 if up else -1

    def slot(up, d):
        return 1 + d if up else n_sp + d

    def end(up):
        return 0 if up else last

    def sends(up, d):
        return jnp.logical_and(inside(s + step_of(up)), inside(s - step_of(up) * d))

    def gets(up, d):
        return inside(s - step_of(up) * (d + 1))

    def each(d, visit):
        for up in (True, False):

            @pl.when(gets(up, d))
            def _():
                visit(up, d, s - step_of(up) * (d + 1))

    load_rows = pltpu.make_async_copy(token_ref, rows_in, load_sem.at[0])
    load_shift = pltpu.make_async_copy(shift_ref, raw_shift, load_sem.at[1])
    load_rows.start()
    load_shift.start()
    peers = [(g, z_at[k], x * CORES + core_at[o]) for k in range(n_sp) for o in range(CORES)]
    peers = peers[1:] + [(g, s, across), (1 - g, s, t)]
    barrier = pltpu.get_barrier_semaphore()
    for peer in peers:
        pl.semaphore_signal(barrier, inc=1, device_id=peer, device_id_type=MESH)
    own_rows = span_at(s, depth)
    for p, w in enumerate(sources):
        pltpu.make_async_copy(
            w.at[:, lanes(s)], weights.at[own_rows, pl.ds(p * KEY, KEY)], load_sem.at[2]
        ).start()
    w_rows = span_at(c, depth)
    w_own = pltpu.make_async_copy(w_ref, matrix.at[w_rows, lanes(s, width)], load_sem.at[3])
    w_own.start()

    here_rows = span_at(s * n_tp + t, span)
    with scope("wait_rows"):
        load_rows.wait()
    rows = rows_in[...].astype(f32)
    scale = lax.rsqrt(jnp.mean(rows * rows, axis=-1, keepdims=True) + norm_eps)
    wide[...] = rows * scale * norm_ref[...]
    for q in range(seqs):
        acts[q, here_rows, :] = wide[:, q, :].astype(bf16)
    with scope("barrier"):
        pl.semaphore_wait(barrier, len(peers))

    def block(where_s, where_t):
        return acts.at[:, span_at(where_s * n_tp + where_t, span), :]

    def act_z(up, d, piece):
        at = span_at((s - step_of(up) * d) * n_tp + t, span)
        here = acts.at[pl.ds(piece * lot, lot), at, :]
        index = slot(up, d) - 1
        peer = (g, s + step_of(up), t)
        return remote(here, here, az_out.at[index], az_in.at[index, piece], peer)

    def act_x(index, origin):
        here = block(origin, t)
        return remote(here, here, ax_out, ax_in.at[index], (g, s, across))

    def act_c(far, origin):
        here = block(origin, across if far else t)
        return remote(here, here, ac_out, ac_in, (g, s, twin))

    part = span_at(g, half)

    def w_z(k, p):
        src = sources[p].at[part, lanes(z_at[k])]
        dst = weights.at[span_at(s * n_grp + g, half), pl.ds(p * KEY, KEY)]
        return remote(src, dst, wz_out, wz_in.at[k - 1, p], (g, z_at[k], t))

    def w_block(k, p):
        return weights.at[span_at(z_from[k] * n_grp + g, half), pl.ds(p * KEY, KEY)]

    def w_y(k, p, index):
        here = w_block(k, p)
        return remote(here, here, wy_out, wy_in.at[index], (1 - g, s, t))

    place = span_at(s, positions)

    def s_z(k):
        return remote(own_shift.at[z_at[k]], shifts.at[:, place, :], sz_out, sz_in, (g, z_at[k], t))

    def o_block(where_s, where_g, where_c, piece):
        at = pl.multiple_of(where_c * depth + where_g * half + piece * bit, bit)
        return matrix.at[pl.ds(at, bit), lanes(where_s, width)]

    def o_z(up, d, piece):
        here = o_block(s - step_of(up) * d, g, c, piece)
        src = w_ref.at[span_at(g * BITS + piece, bit), :] if d == 0 else here
        index = slot(up, d) - 1
        peer = (g, s + step_of(up), t)
        return remote(src, here, oz_out.at[index], oz_in.at[index, piece], peer)

    def o_y(index, origin, piece):
        here = o_block(origin, g, c, piece)
        return remote(here, here, oy_out, oy_in.at[index - 1, piece], (1 - g, s, t))

    def o_c(far, index, origin, piece):
        here = o_block(origin, 1 - g if far else g, c, piece)
        return remote(here, here, oc_out, oc_in.at[index], (g, s, twin))

    def ahead(up, hops, groups_now):
        for hop in hops:
            k = hop if up else n_sp - hop
            go_up = s + k < n_sp

            @pl.when(go_up if up else jnp.logical_not(go_up))
            def _():
                for group in groups_now:
                    if group is None:
                        s_z(k).start()
                    else:
                        for p in range(*groups[group]):
                            w_z(k, p).start()

    every_group = range(len(groups))
    every_hop = range(1, n_sp)

    def neighbour(up):
        return s == (1 if up else last - 1)

    def o_first(up, pieces):
        @pl.when(sends(up, 0))
        def _():
            for piece in pieces:
                o_z(up, 0, piece).start()

    def issue(up):
        @pl.when(s == end(up))
        def _():
            o_first(up, range(BITS))
            ahead(up, (1,), every_group)

        @pl.when(neighbour(not up))
        def _():
            ahead(up, every_hop[::-1], every_group)
            o_first(up, range(BITS))
            ahead(up, every_hop, (None,))

        @pl.when(neighbour(up))
        def _():
            ahead(up, every_hop[::-1], every_group)
            o_first(up, range(EARLY))
            ahead(up, every_hop, (None,))
            o_first(up, range(EARLY, BITS))

    def issue_far():
        for up in (True, False):

            @pl.when(s == end(up))
            def _():
                ahead(up, every_hop[1:], every_group)
                ahead(up, every_hop, (None,))

    for piece in range(PIECES):
        for up in (True, False):

            @pl.when(sends(up, 0))
            def _():
                act_z(up, 0, piece).start()

    act_x(0, s).start()
    act_c(0, s).start()
    with scope("wait_shift_load"):
        load_shift.wait()
    for q in range(seqs):
        values = raw_shift[:, q, :].astype(bf16)
        for k in range(n_sp):
            own_shift[k, q] = values[:, k * KEY : (k + 1) * KEY]
    shifts[:, place, :] = own_shift[s]
    for up in (True, False):

        @pl.when(s == end(up))
        def _():
            issue(up)

    def swap(d, groups_now, match=True, late=False):
        for up in (True, False):

            @pl.when(jnp.logical_and(gets(up, d), match))
            def _():
                k = d + 1 if up else last - d
                for group in groups_now:
                    for p in range(*groups[group]):
                        tally(w_block(k, p), wz_out, wz_in.at[k - 1, p]).wait_recv()
                        w_y(k, p, 1 + group if late else 0).start()

    at_end = jnp.logical_or(s == 0, s == last)
    late_source = jnp.where(at_end, last - s, lax.rem(s + 2, n_sp))

    def swap_late(group):
        swap(last - 1, (group,), at_end, True)
        swap(last - 2, (group,), jnp.logical_not(at_end), True)

    for d in range(last):
        if d == last - 1:
            with scope("swap_end"):
                for hop in range(last - 2, 0, -1):
                    swap(hop, every_group, at_end)
        for piece in range(PIECES):

            def arrived(up, d, origin):
                act_z(up, d, piece).wait_recv()
                if d + 1 < last:

                    @pl.when(sends(up, d + 1))
                    def _():
                        act_z(up, d + 1, piece).start()

                if piece == PIECES - 1:
                    act_x(slot(up, d), origin).start()
                    act_c(0, origin).start()

            with scope(f"act_z{d}_{piece}"):
                each(d, arrived)
        if d + 1 < last:
            for up in (True, False):

                @pl.when(s == (d + 1 if up else last - 1 - d))
                def _():
                    issue(up)

    o_own = remote(w_ref, matrix.at[w_rows, lanes(s, width)], oc_out, oc_in.at[0], (g, s, twin))
    o_own.start()

    def relay(index, origin):
        act_x(index, origin).wait_recv()
        act_c(1, origin).start()

    def o_take(up, d, origin, pieces=range(BITS)):
        for piece in pieces:
            o_z(up, d, piece).wait_recv()
            if d + 1 < last:

                @pl.when(sends(up, d + 1))
                def _():
                    o_z(up, d + 1, piece).start()

            o_y(slot(up, d), origin, piece).start()
            o_c(0, slot(up, d), origin, piece).start()

    def o_swapped(up, d, origin):
        for piece in range(BITS):
            o_y(slot(up, d), origin, piece).wait_recv()
            o_c(1, slot(up, d), origin, piece).start()

    with scope("take_early"):
        for up in (True, False):

            @pl.when(neighbour(up))
            def _():
                o_take(up, 0, s - step_of(up))

    with scope("swap_near0"):
        swap(0, every_group[:1])
    issue_far()
    with scope("swap_near1"):
        swap(0, every_group[1:])
    with scope("relay"):
        relay(0, s)
        for d in range(last):
            each(d, lambda up, d, origin: relay(slot(up, d), origin))

    def take_late(pieces, where):
        for up in (True, False):
            match = jnp.logical_and(gets(up, 0), jnp.logical_not(neighbour(up)))

            @pl.when(jnp.logical_and(match, where))
            def _():
                o_take(up, 0, s - step_of(up), pieces)

    def project(group):
        at = slice(groups[group][0] * KEY, groups[group][1] * KEY)
        from_late = span_at(late_source, depth)
        with scope(f"wait_w{group}"):
            block = weights.at[pl.ds(0, half), at]
            tally(block, wy_out, wy_in.at[1 + group]).wait_recv()

        def one(q, carry):
            more = jnp.dot(
                acts[q, :, from_late], weights[from_late, at], preferred_element_type=f32
            )
            proj[q, :, at] = (begun[q, :, at] + more).astype(bf16)
            return carry

        with scope(f"project{group}"):
            lax.fori_loop(0, seqs, one, 0)

    def begin(q, carry):
        total = None
        for i in range(1, n_sp):
            rows_now = span_at(lax.rem(late_source + i, n_sp), depth)
            more = jnp.dot(acts[q, :, rows_now], weights[rows_now, :], preferred_element_type=f32)
            total = more if total is None else total + more
        begun[q] = total
        return carry

    with scope("joined"):
        tally(acts.at[pl.ds(0, seqs // CORES)], ac_out, ac_in).wait_recv()
        here = weights.at[own_rows, :]
        pltpu.make_async_copy(here, here, load_sem.at[2]).wait()
    with scope("wait_w"):
        tally(weights.at[pl.ds(0, (last - 1) * half), :], wy_out, wy_in.at[0]).wait_recv()
    with scope("take_part_end"):
        take_late(range(BITS // 2), at_end)
    with scope("begin"):
        lax.fori_loop(0, seqs, begin, 0)
    for group in every_group:
        with scope(f"swap_late{group}"):
            swap_late(group)
    with scope("take_rest_end"):
        take_late(range(BITS // 2, BITS), at_end)
    project(0)
    project(1)
    with scope("act_drain"):
        tally(acts.at[:, pl.ds(0, n_sp * span), :], ax_out, ax_in.at[0]).wait_send()
        tally(acts.at[pl.ds(0, seqs // CORES)], ac_out, ac_in).wait_send()
        for d in range(last):
            for up in (True, False):

                @pl.when(sends(up, d))
                def _():
                    index = slot(up, d) - 1
                    tally(block(s, t), az_out.at[index], az_in.at[index, 0]).wait_send()

    with scope("take_part"):
        take_late(range(EARLY), jnp.logical_not(at_end))
    project(2)
    with scope("wait_shift"):
        tally(shifts.at[:, pl.ds(0, last * positions), :], sz_out, sz_in).wait_recv()

    targets = [(k, o) for k in range(n_sp) for o in range(CORES) if k or o]

    def m_move(q, k, o):
        return remote(
            mixed.at[q, z_at[k], :, core_at[o]],
            heads.at[:, q, :, lanes(c * n_sp + s, VAL)],
            m_out,
            m_in.at[q // lot],
            (g, z_at[k], x * CORES + core_at[o]),
        )

    def send_mixed(pair, stage):
        for k, o in targets:
            to_end = jnp.logical_or(z_at[k] == 0, z_at[k] == last)
            to_end = jnp.logical_and(to_end, k > 0)
            far = jnp.logical_and(to_end, jnp.abs(z_at[k] - s) > 1)
            if pair < FREE:
                match = stage == 0
            elif stage == 0:
                match = jnp.logical_not(to_end)
            elif stage == 1:
                match = jnp.logical_and(to_end, jnp.logical_not(far))
            else:
                match = far

            @pl.when(match)
            def _():
                for i in range(2):
                    m_move(2 * pair + i, k, o).start()

    def recur(pair, carry):
        for i in range(2):
            q = 2 * pair + i
            value = recur_one(proj, shifts, gap_ref, gain_ref, summed.at[i], q, lanes(s))
            mixed[q] = value.reshape(n_sp, n_x, CORES, span, VAL)
            heads[:, q, :, lanes(c * n_sp + s, VAL)] = mixed[q, s, :, c]
        send_mixed(pair, 0)
        return carry

    def take_second(pieces, where):
        for up in (True, False):

            @pl.when(jnp.logical_and(gets(up, 1), where))
            def _():
                o_take(up, 1, s - 2 * step_of(up), pieces)

    def take_third(pieces):
        each(last - 1, lambda up, d, origin: o_take(up, d, origin, pieces))

    for pair in range(seqs // 2):
        with scope(f"recur{pair}"):
            recur(pair, 0)
        if pair == 0:
            with scope("take_second"):
                take_second(range(EARLY), at_end)
    with scope("take_late"):
        take_late(range(EARLY, BITS), jnp.logical_not(at_end))
    with scope("w_drain"):
        tally(own_shift.at[pl.ds(0, last)], sz_out, sz_in).wait_send()
        every = weights.at[pl.ds(0, last * half), :]
        tally(every, wz_out, wz_in.at[0, 0]).wait_send()
        tally(every, wy_out, wy_in.at[0]).wait_send()
    w_own.wait()

    def p_move(index, origin, rows_now, part):
        at = lanes(origin, width)
        return remote(
            partial.at[1 - x, rows_now, :, at],
            landed.at[rows_now, :, at],
            p_out,
            p_in.at[index, part],
            (g, s, across),
        )

    lots = tuple(slice(h * lot, (h + 1) * lot) for h in range(PIECES))

    def strip(index, origin, rows_now, part):
        at = lanes(origin, width)
        lines = heads[:, rows_now].reshape(-1, heads.shape[-1])
        partial[:, rows_now, :, at] = (
            jnp.dot(lines, matrix[:, at], preferred_element_type=f32)
            .astype(bf16)
            .reshape(n_x, -1, span, width)
        )
        p_move(index, origin, rows_now, part).start()

    def arrived_strip(index, origin):
        at = lanes(origin, width)
        tally(matrix.at[pl.ds(0, depth), at], oc_out, oc_in.at[index]).wait_recv()

    def own_strip(part):
        strip(0, s, lots[part], part)

    def other_strip(d, part):
        def visit(up, d, origin):
            if part == 0:
                arrived_strip(slot(up, d), origin)
            strip(slot(up, d), origin, lots[part], part)

        each(d, visit)

    def mixed_in(part):
        here = heads.at[:, pl.ds(0, lot), :, pl.ds(0, len(targets) * VAL)]
        tally(here, m_out, m_in.at[part]).wait_recv()

    with scope("o_pass1"):
        take_second(range(EARLY, BITS), at_end)
        take_second(range(BITS), jnp.logical_not(at_end))
    for pair in range(FREE, seqs // 2):
        send_mixed(pair, 1)
    with scope("o_pass2a"):
        take_third(range(BITS // 2))
    for pair in range(FREE, seqs // 2):
        send_mixed(pair, 2)
    with scope("o_pass2b"):
        take_third(range(BITS // 2, BITS))
    with scope("o_swapped0"):
        each(0, o_swapped)
    with scope("wait_m0"):
        mixed_in(0)
    with scope("own_strip0"):
        arrived_strip(0, s)
        own_strip(0)
    with scope("near_strip0"):
        other_strip(0, 0)
    for d in range(1, last):
        with scope(f"o_swapped{d}"):
            each(d, o_swapped)
        with scope(f"strip{d}"):
            other_strip(d, 0)
    for part in range(1, PIECES):
        with scope(f"wait_m{part}"):
            mixed_in(part)
        with scope(f"strips{part}"):
            own_strip(part)
            for d in range(last):
                other_strip(d, part)

    def finish(index, origin, parts):
        for part, rows_now in enumerate(parts):
            p_move(index, origin, rows_now, part).wait_recv()
            at = lanes(origin, width)
            total = partial[x, rows_now, :, at].astype(f32) + landed[rows_now, :, at].astype(f32)
            out_ref[rows_now, :, at] = total.astype(bf16)

    with scope("finish"):
        finish(0, s, lots)
        for d in range(last):
            each(d, lambda up, d, origin: finish(slot(up, d), origin, lots))
    with scope("drain"):
        here = heads.at[:, :, :, pl.ds(0, len(targets) * VAL)]
        tally(here, m_out, m_in.at[0]).wait_send()
        strips = matrix.at[pl.ds(0, half), pl.ds(0, last * width)]
        tally(strips, oy_out, oy_in.at[0, 0]).wait_send()
        tally(matrix.at[pl.ds(0, depth), :], oc_out, oc_in.at[0]).wait_send()
        tally(landed, p_out, p_in.at[0, 0]).wait_send()
        for d in range(last):
            for up in (True, False):

                @pl.when(sends(up, d))
                def _():
                    index = slot(up, d) - 1
                    here = matrix.at[pl.ds(0, half), pl.ds(0, width)]
                    tally(here, oz_out.at[index], oz_in.at[index, 0]).wait_send()


def layer(sizes, tokens, norm_gain, shift, sources, gap, gain, w_out):
    n_grp, n_sp, n_tp = sizes
    n_x = n_tp // CORES
    span, seqs, model = tokens.shape
    length = n_sp * n_tp * span
    count = len(sources)
    depth, width = w_out.shape
    slots = 2 * n_sp - 1
    dma = pltpu.SemaphoreType.DMA
    hbm = pl.BlockSpec(memory_space=pltpu.HBM)
    vmem = pl.BlockSpec(memory_space=pltpu.VMEM)
    bf16 = jnp.bfloat16
    return pl.pallas_call(
        functools.partial(layer_kernel, sizes),
        out_shape=jax.ShapeDtypeStruct((seqs, span, n_sp * width), bf16),
        in_specs=[hbm, vmem] + [hbm] * (1 + count) + [vmem, vmem, hbm],
        out_specs=vmem,
        scratch_shapes=[
            pltpu.VMEM(tokens.shape, bf16),
            pltpu.VMEM(tokens.shape, jnp.float32),
            pltpu.VMEM(shift.shape, shift.dtype),
            pltpu.VMEM((n_sp, seqs, n_tp * span, KEY), bf16),
            pltpu.VMEM((seqs, length, KEY), bf16),
            pltpu.VMEM((seqs, length, model), bf16),
            pltpu.VMEM((model, count * KEY), bf16),
            pltpu.VMEM((seqs, length, count * KEY), jnp.float32),
            pltpu.VMEM((seqs, length, count * KEY), bf16),
            pltpu.VMEM((2, length, VAL), jnp.float32),
            pltpu.VMEM((seqs, n_sp, n_x, CORES, span, VAL), bf16),
            pltpu.VMEM((n_x, seqs, span, CORES * depth), bf16),
            pltpu.VMEM((CORES * depth, n_sp * width), bf16),
            pltpu.VMEM((n_x, seqs, span, n_sp * width), bf16),
            pltpu.VMEM((seqs, span, n_sp * width), bf16),
            dma((4,)),
            dma((slots - 1,)),
            dma((slots - 1, PIECES)),
            dma,
            dma((slots,)),
            dma,
            dma,
            dma,
            dma((n_sp - 1, count)),
            dma,
            dma((4,)),
            dma,
            dma,
            dma((slots - 1,)),
            dma((slots - 1, BITS)),
            dma,
            dma((slots - 1, BITS)),
            dma,
            dma((slots,)),
            dma,
            dma((PIECES,)),
            dma,
            dma((slots, PIECES)),
        ],
        compiler_params=pltpu.CompilerParams(
            collective_id=0, has_side_effects=True, vmem_limit_bytes=107 * 512 * 1024
        ),
    )(tokens, norm_gain, shift, *sources, gap, gain, w_out)


def head_shards(
    sizes,
    tokens,
    norm_gain,
    w_query,
    w_value,
    w_fwd_gate,
    w_bwd_gate,
    w_out_gate,
    floor_gap,
    decay_shift,
    head_gain,
    w_out,
):
    return layer(
        sizes,
        tokens,
        norm_gain.reshape(1, 1, -1),
        decay_shift,
        (w_query, w_value, w_fwd_gate, w_bwd_gate, w_out_gate),
        floor_gap,
        head_gain.reshape(1, VAL),
        w_out,
    ).transpose(1, 0, 2)


def by_heads(mesh):
    n_sp, n_tp = mesh.shape["sp"], mesh.shape["tp"]

    def run(*arrays):
        tokens, w_query = arrays[0], arrays[2]
        heads_here = w_query.shape[1] // KEY // n_tp
        span = tokens.shape[0] // (n_sp * n_tp)
        sizes = (mesh.shape["grp"], n_sp, n_tp)
        fits = heads_here == n_sp and n_sp == CORES * 2 and n_tp == 2 * CORES and span % 16 == 0
        fits = fits and sizes[0] == 2 and tokens.shape[1] // sizes[0] % PIECES == 0
        fits = fits and tokens.shape[0] % BLOCK == 0 and tokens.shape[0] <= 512
        body = functools.partial(head_shards, sizes) if fits else shards
        return mapped(body, mesh)(*arrays)

    return run


def mapped(body, mesh):
    return jax.shard_map(
        body,
        mesh=mesh,
        in_specs=(
            P(("sp", "tp"), "grp", None),
            P(),
            P("sp", "tp"),
            P("sp", "tp"),
            P("sp", "tp"),
            P("sp", "tp"),
            P("sp", "tp"),
            P(None, "tp"),
            P("sp", "grp", "tp"),
            P(),
            P("tp", "sp"),
        ),
        out_specs=P(("sp", "tp"), "grp", None),
        check_vma=False,
    )


def solution(mesh):
    return by_heads(mesh)
```

```python
import functools

import jax
import jax.numpy as jnp
from jax import lax
from jax.experimental import pallas as pl
from jax.experimental.pallas import tpu as pltpu
from jax.sharding import PartitionSpec as P

KEY = 128
VAL = 128
BLOCK = 64


norm_eps = 1e-06
highest = lax.Precision.HIGHEST


def carried_in(x, axis, join, neutral, backward):
    count = lax.axis_size(axis)
    place = lax.axis_index(axis)
    ahead = count - 1 - place if backward else place
    gathered = jax.tree.map(
        lambda a, kind: lax.all_gather(a.astype(kind), axis), x, (jnp.bfloat16, jnp.bfloat16)
    )
    state = jax.tree.map(lambda a, e: jnp.zeros_like(a) + jnp.asarray(e, a.dtype), x, neutral)

    def one(turn, state):
        source = count - 1 - turn if backward else turn
        return join(
            state,
            jax.tree.map(
                lambda a, own: lax.dynamic_index_in_dim(a, source, 0, False).astype(own.dtype),
                gathered,
                x,
            ),
        )

    return lax.fori_loop(0, ahead, one, state)


def split_blocks(array):
    return array.reshape(array.shape[0] // BLOCK, BLOCK, *array.shape[1:])


def prepare_chain(queries, key_cols, values, log_decay):
    query_blocks = split_blocks(queries)
    key_blocks = split_blocks(key_cols)
    value_blocks = split_blocks(values)
    running = jnp.cumsum(split_blocks(log_decay), axis=1)
    block_end = running[:, -1]
    block_state = jnp.einsum(
        "nsbhk,nsbhe->nbhke",
        key_blocks * jnp.exp(block_end[:, None] - running),
        value_blocks,
        precision=highest,
    )
    carry_state = jnp.zeros_like(block_state[0])
    log_total = jnp.zeros_like(block_end[0])
    offsets = [log_total]
    carry_state = jnp.exp(block_end[0])[..., None] * carry_state + block_state[0]
    log_total = block_end[0]
    return (
        query_blocks,
        key_blocks,
        value_blocks,
        running,
        block_state,
        jnp.stack(offsets),
        log_total,
        carry_state,
    )


def local_pass(chain, carry_state):
    query_blocks, key_blocks, value_blocks, running, block_state = (
        chain[0],
        chain[1],
        chain[2],
        chain[3],
        chain[4],
    )
    block_len = running.shape[1]
    earlier_mask = jnp.arange(block_len)[:, None] >= jnp.arange(block_len)[None, :]
    here = running[0]
    anchor = here[:1]
    query_scaled = query_blocks[0] * jnp.exp(here - anchor)
    key_scaled = key_blocks[0] * jnp.exp(anchor - here)
    scores = jnp.einsum("tbhk,sbhk->bhts", query_scaled, key_scaled, precision=highest)
    scores = jnp.where(earlier_mask, scores, 0.0)
    within = jnp.einsum("bhts,sbhe->tbhe", scores, value_blocks[0], precision=highest)
    carried = jnp.einsum(
        "tbhk,bhke->tbhe", query_blocks[0] * jnp.exp(here), carry_state, precision=highest
    )
    outputs = within + carried
    return outputs


def combine(earlier, later):
    return (earlier[0] + later[0], jnp.exp(later[0])[..., None] * earlier[1] + later[1])


def group_sums(flat_mixed, weight_lines, group_count):
    group_width = flat_mixed.shape[1] // group_count
    accumulated_total = jnp.zeros((flat_mixed.shape[0], weight_lines.shape[1]), jnp.float32)
    for tp_group in range(group_count):
        first_column = tp_group * group_width
        partial_value = jnp.dot(
            flat_mixed[:, first_column : first_column + group_width],
            weight_lines[first_column : first_column + group_width],
            preferred_element_type=jnp.float32,
        ).astype(jnp.bfloat16)
        accumulated_total = accumulated_total + lax.optimization_barrier(partial_value).astype(
            jnp.float32
        )
    return accumulated_total


def shards(
    tokens,
    norm_gain,
    w_query,
    w_value,
    w_fwd_gate,
    w_bwd_gate,
    w_out_gate,
    floor_gap,
    decay_shift,
    head_gain,
    w_out,
):
    token_f32 = tokens.astype(jnp.float32)
    scale_rows = lax.rsqrt(jnp.mean(token_f32 * token_f32, axis=-1, keepdims=True) + norm_eps)
    normed = (token_f32 * scale_rows * norm_gain).astype(jnp.bfloat16)
    weights = (
        lax.all_gather(w_query, "sp", axis=0, tiled=True),
        lax.all_gather(w_value, "sp", axis=0, tiled=True),
        lax.all_gather(w_fwd_gate, "sp", axis=0, tiled=True),
        lax.all_gather(w_bwd_gate, "sp", axis=0, tiled=True),
        lax.all_gather(w_out_gate, "sp", axis=0, tiled=True),
    )
    piece_rows = lax.all_gather(normed, "tp", axis=0, tiled=True)
    flat_rows = piece_rows.reshape(-1, piece_rows.shape[2])
    columns = [
        jnp.dot(flat_rows, matrix, preferred_element_type=jnp.float32).astype(jnp.bfloat16)
        for matrix in weights
    ]
    projected = lax.optimization_barrier(
        jnp.concatenate(columns, axis=1).reshape(piece_rows.shape[0], piece_rows.shape[1], -1)
    )
    key_width = w_query.shape[1]
    value_width = w_value.shape[1]
    heads_here = key_width // KEY
    extent_rows = projected.shape[0]
    seq_count = projected.shape[1]
    bounds_list = [
        0,
        key_width,
        key_width + value_width,
        2 * key_width + value_width,
        3 * key_width + value_width,
        3 * key_width + 2 * value_width,
    ]

    def section_part(position, feature_lanes):
        picked = projected[:, :, bounds_list[position] : bounds_list[position + 1]].astype(
            jnp.float32
        )
        return picked.reshape(extent_rows, seq_count, heads_here, feature_lanes)

    queries = jax.nn.silu(section_part(0, KEY))
    values = section_part(1, VAL)
    shift = decay_shift.reshape(extent_rows, seq_count, heads_here, KEY)
    key_fwd = floor_gap[0].reshape(heads_here, KEY) * jax.nn.sigmoid(-section_part(2, KEY))
    key_bwd = floor_gap[1].reshape(heads_here, KEY) * jax.nn.sigmoid(-section_part(3, KEY))
    decay_fwd = jnp.log1p(-key_fwd) + shift
    decay_bwd = jnp.log1p(-key_bwd) + shift
    fwd_chain = prepare_chain(queries, key_fwd, values, decay_fwd)
    bwd_chain = prepare_chain(queries[::-1], key_bwd[::-1], values[::-1], decay_bwd[::-1])
    identity_pair = (jnp.zeros_like(fwd_chain[6]), jnp.zeros_like(fwd_chain[7]))
    fwd_in = carried_in((fwd_chain[6], fwd_chain[7]), "sp", combine, identity_pair, False)[1]
    bwd_in = carried_in((bwd_chain[6], bwd_chain[7]), "sp", combine, identity_pair, True)[1]
    out_fwd = local_pass(fwd_chain, fwd_in)
    out_bwd = local_pass(bwd_chain, bwd_in)
    combined = out_fwd + out_bwd[::-1]
    head_normed = (
        combined
        * lax.rsqrt(jnp.mean(combined * combined, axis=-1, keepdims=True) + norm_eps)
        * head_gain
    )
    gate_value = jax.nn.silu(projected[:, :, bounds_list[4] : bounds_list[5]].astype(jnp.float32))
    mixed = (head_normed.reshape(extent_rows, seq_count, value_width) * gate_value).astype(
        jnp.bfloat16
    )
    token_rows = lax.all_to_all(mixed, "tp", split_axis=0, concat_axis=2, tiled=True)
    flat_mixed = token_rows.reshape(-1, token_rows.shape[2])
    group_count = lax.axis_size("tp")
    w_columns = lax.all_gather(w_out, "sp", axis=1, tiled=True)
    w_full = lax.all_gather(w_columns, "tp", axis=0, tiled=True)
    accumulated_total = group_sums(flat_mixed, w_full, group_count)
    result = accumulated_total.reshape(token_rows.shape[0], token_rows.shape[1], -1)
    return result.astype(jnp.bfloat16)


MESH = pl.DeviceIdType.MESH
CORES = 2
PIECES = 2
BITS = 4
EARLY = 3
VL = 56
TRIG = 2
FREE = 1
scope = jax.named_scope


def recur_one(proj_ref, shift_ref, gap_ref, gain_ref, out_ref, i, own):
    f32 = jnp.float32
    bf16 = jnp.bfloat16
    length = proj_ref.shape[1]

    def cols(p):
        return proj_ref[i, :, p * KEY : (p + 1) * KEY]

    queries = cols(0).astype(f32)
    queries = queries * jax.nn.sigmoid(queries)
    values = cols(1)
    shift = shift_ref[i].astype(f32)
    row = lax.broadcasted_iota(jnp.int32, (length, length), 0)
    col = lax.broadcasted_iota(jnp.int32, (length, length), 1)
    near = row // BLOCK == col // BLOCK
    row = lax.broadcasted_iota(jnp.int32, (BLOCK, BLOCK), 0)
    col_b = lax.broadcasted_iota(jnp.int32, (BLOCK, BLOCK), 1)
    seen = [row >= col_b, row <= col_b]
    row_l = lax.broadcasted_iota(jnp.int32, (length, length), 0)
    order = [row_l >= col, row_l <= col]
    blocks = length // BLOCK
    keys, here = [], []
    for d in range(2):
        key = gap_ref[d : d + 1, own] * jax.nn.sigmoid(-cols(2 + d).astype(f32))
        decay = jnp.log1p(-key) + shift
        high = decay.astype(bf16)
        rest = decay - high.astype(f32)
        middle = rest.astype(bf16)
        low = (rest - middle.astype(f32)).astype(bf16)
        tri = jnp.where(jnp.logical_and(near, order[d]), 1.0, 0.0).astype(bf16)
        sums = jnp.dot(
            tri, jnp.concatenate([high, middle, low], axis=1), preferred_element_type=f32
        )
        here.append(sums[:, :KEY] + (sums[:, KEY : 2 * KEY] + sums[:, 2 * KEY :]))
        keys.append(key)
    state = [None, None]
    outs = [[None, None] for _ in range(blocks)]
    for step in range(blocks):
        for d in range(2):
            n = step if d == 0 else blocks - 1 - step
            at = slice(n * BLOCK, (n + 1) * BLOCK)
            q, k, v, h = queries[at], keys[d][at], values[at], here[d][at]
            edge = h[BLOCK - 1 : BLOCK] if d == 0 else h[0:1]
            anchor = h[BLOCK // 2 : BLOCK // 2 + 1]
            scores = lax.dot_general(
                (q * jnp.exp(h - anchor)).astype(bf16),
                (k * jnp.exp(anchor - h)).astype(bf16),
                (((1,), (1,)), ((), ())),
                preferred_element_type=f32,
            )
            scores = jnp.where(seen[d], scores, 0.0).astype(bf16)
            out = jnp.dot(scores, v, preferred_element_type=f32)
            if state[d] is not None:
                out = out + lax.dot_general(
                    (q * jnp.exp(h)).astype(bf16),
                    state[d].astype(bf16),
                    (((1,), (1,)), ((), ())),
                    preferred_element_type=f32,
                )
            outs[n][d] = out
            if step < blocks - 1:
                fresh = lax.dot_general(
                    v,
                    (k * jnp.exp(edge - h)).astype(bf16),
                    (((0,), (0,)), ((), ())),
                    preferred_element_type=f32,
                )
                state[d] = fresh if state[d] is None else state[d] * jnp.exp(edge) + fresh
    for n in range(blocks):
        out_ref[n * BLOCK : (n + 1) * BLOCK] = outs[n][0] + outs[n][1]
    combined = out_ref[...]
    normed = combined * lax.rsqrt(jnp.mean(combined * combined, axis=-1, keepdims=True) + norm_eps)
    gate = cols(4).astype(f32)
    return (normed * gain_ref[...] * (gate * jax.nn.sigmoid(gate))).astype(bf16)


def layer_kernel(
    sizes,
    token_ref,
    norm_hbm,
    shift_ref,
    wq_ref,
    wv_ref,
    wf_ref,
    wb_ref,
    wg_ref,
    gap_hbm,
    gain_hbm,
    w_ref,
    out_ref,
    norm_ref,
    gap_ref,
    gain_ref,
    rows_in,
    wide,
    raw_shift,
    own_shift,
    shifts,
    acts,
    weights,
    begun,
    proj,
    summed,
    mixed,
    heads,
    matrix,
    partial,
    landed,
    load_sem,
    az_out,
    az_in,
    ax_out,
    ax_in,
    ac_out,
    ac_in,
    wz_out,
    wz_in,
    wy_out,
    wy_in,
    sz_out,
    sz_in,
    oz_out,
    oz_in,
    oy_out,
    oy_in,
    oc_out,
    oc_in,
    m_out,
    m_in,
    p_out,
    p_in,
):
    bf16 = jnp.bfloat16
    f32 = jnp.float32
    n_grp, n_sp, n_tp = sizes
    n_x = n_tp // CORES
    g = lax.axis_index("grp")
    s = lax.axis_index("sp")
    t = lax.axis_index("tp")
    x = t // CORES
    c = t % CORES
    twin = x * CORES + (1 - c)
    across = (1 - x) * CORES + c
    seqs = acts.shape[0]
    span = token_ref.shape[0]
    positions = n_tp * span
    depth = wq_ref.shape[0]
    half = depth // n_grp
    width = w_ref.shape[1]
    lot = seqs // PIECES
    bit = half // BITS
    sources = (wq_ref, wv_ref, wf_ref, wb_ref, wg_ref)
    count = len(sources)
    groups = ((0, 2), (2, 4), (4, 5))
    last = n_sp - 1
    z_at = [lax.rem(s + k, n_sp) for k in range(n_sp)]
    z_from = [lax.rem(s + n_sp - k, n_sp) for k in range(n_sp)]
    core_at = [c, 1 - c]

    def span_at(where, size):
        return pl.ds(pl.multiple_of(where * size, size), size)

    def lanes(where, size=KEY):
        return span_at(where, size)

    def remote(src, dst, out_sem, in_sem, peer):
        return pltpu.make_async_remote_copy(
            src_ref=src,
            dst_ref=dst,
            send_sem=out_sem,
            recv_sem=in_sem,
            device_id=peer,
            device_id_type=MESH,
        )

    def tally(ref, out_sem, in_sem):
        return remote(ref, ref, out_sem, in_sem, (g, s, twin))

    def inside(place):
        return jnp.logical_and(place >= 0, place < n_sp)

    def step_of(up):
        return 1 if up else -1

    def slot(up, d):
        return 1 + d if up else n_sp + d

    def end(up):
        return 0 if up else last

    def sends(up, d):
        return jnp.logical_and(inside(s + step_of(up)), inside(s - step_of(up) * d))

    def gets(up, d):
        return inside(s - step_of(up) * (d + 1))

    def each(d, visit):
        for up in (True, False):

            @pl.when(gets(up, d))
            def _():
                visit(up, d, s - step_of(up) * (d + 1))

    load_rows = pltpu.make_async_copy(token_ref, rows_in, load_sem.at[0])
    load_shift = pltpu.make_async_copy(shift_ref, raw_shift, load_sem.at[1])
    load_rows.start()
    small = [
        pltpu.make_async_copy(src, dst, load_sem.at[4 + i])
        for i, (src, dst) in enumerate(
            ((norm_hbm, norm_ref), (gap_hbm, gap_ref), (gain_hbm, gain_ref))
        )
    ]
    for copy in small:
        copy.start()
    load_shift.start()
    peers = [(g, z_at[k], x * CORES + core_at[o]) for k in range(n_sp) for o in range(CORES)]
    peers = peers[1:] + [(g, s, across), (1 - g, s, t)]
    barrier = pltpu.get_barrier_semaphore()
    for peer in peers:
        pl.semaphore_signal(barrier, inc=1, device_id=peer, device_id_type=MESH)
    own_rows = span_at(s, depth)
    for p, w in enumerate(sources):
        pltpu.make_async_copy(
            w.at[:, lanes(s)], weights.at[own_rows, pl.ds(p * KEY, KEY)], load_sem.at[2]
        ).start()
    w_rows = span_at(c, depth)
    w_own = pltpu.make_async_copy(w_ref, matrix.at[w_rows, lanes(s, width)], load_sem.at[3])
    w_own.start()

    here_rows = span_at(s * n_tp + t, span)
    with scope("wait_rows"):
        load_rows.wait()
        for copy in small:
            copy.wait()
    rows = rows_in[...].astype(f32)
    scale = lax.rsqrt(jnp.mean(rows * rows, axis=-1, keepdims=True) + norm_eps)
    wide[...] = rows * scale * norm_ref[...]
    for q in range(seqs):
        acts[q, here_rows, :] = wide[:, q, :].astype(bf16)
    with scope("barrier"):
        pl.semaphore_wait(barrier, len(peers))

    def block(where_s, where_t):
        return acts.at[:, span_at(where_s * n_tp + where_t, span), :]

    def act_z(up, d, piece):
        at = span_at((s - step_of(up) * d) * n_tp + t, span)
        here = acts.at[pl.ds(piece * lot, lot), at, :]
        index = slot(up, d) - 1
        peer = (g, s + step_of(up), t)
        return remote(here, here, az_out.at[index], az_in.at[index, piece], peer)

    def act_x(index, origin):
        here = block(origin, t)
        return remote(here, here, ax_out, ax_in.at[index], (g, s, across))

    def act_c(far, origin):
        here = block(origin, across if far else t)
        return remote(here, here, ac_out, ac_in, (g, s, twin))

    part = span_at(g, half)

    def w_z(k, p):
        src = sources[p].at[part, lanes(z_at[k])]
        dst = weights.at[span_at(s * n_grp + g, half), pl.ds(p * KEY, KEY)]
        return remote(src, dst, wz_out, wz_in.at[k - 1, p], (g, z_at[k], t))

    def w_block(k, p):
        return weights.at[span_at(z_from[k] * n_grp + g, half), pl.ds(p * KEY, KEY)]

    def w_y(k, p, index):
        here = w_block(k, p)
        return remote(here, here, wy_out, wy_in.at[index], (1 - g, s, t))

    place = span_at(s, positions)

    def s_z(k):
        return remote(own_shift.at[z_at[k]], shifts.at[:, place, :], sz_out, sz_in, (g, z_at[k], t))

    def o_block(where_s, where_g, where_c, piece):
        at = pl.multiple_of(where_c * depth + where_g * half + piece * bit, bit)
        return matrix.at[pl.ds(at, bit), lanes(where_s, width)]

    def o_z(up, d, piece):
        here = o_block(s - step_of(up) * d, g, c, piece)
        src = w_ref.at[span_at(g * BITS + piece, bit), :] if d == 0 else here
        index = slot(up, d) - 1
        peer = (g, s + step_of(up), t)
        return remote(src, here, oz_out.at[index], oz_in.at[index, piece], peer)

    def o_y(index, origin, piece):
        here = o_block(origin, g, c, piece)
        return remote(here, here, oy_out, oy_in.at[index - 1, piece], (1 - g, s, t))

    def o_c(far, index, origin, piece):
        here = o_block(origin, 1 - g if far else g, c, piece)
        return remote(here, here, oc_out, oc_in.at[index], (g, s, twin))

    def ahead(up, hops, groups_now):
        for hop in hops:
            k = hop if up else n_sp - hop
            go_up = s + k < n_sp

            @pl.when(go_up if up else jnp.logical_not(go_up))
            def _():
                for group in groups_now:
                    if group is None:
                        s_z(k).start()
                    else:
                        for p in range(*groups[group]):
                            w_z(k, p).start()

    every_group = range(len(groups))
    every_hop = range(1, n_sp)

    def neighbour(up):
        return s == (1 if up else last - 1)

    def o_first(up, pieces):
        @pl.when(sends(up, 0))
        def _():
            for piece in pieces:
                o_z(up, 0, piece).start()

    def issue(up):
        @pl.when(s == end(up))
        def _():
            o_first(up, range(BITS))
            ahead(up, (1,), every_group)

        @pl.when(neighbour(not up))
        def _():
            ahead(up, every_hop[::-1], every_group)
            o_first(up, range(BITS))
            ahead(up, every_hop, (None,))

        @pl.when(neighbour(up))
        def _():
            ahead(up, every_hop[::-1], every_group)
            o_first(up, range(EARLY))
            ahead(up, every_hop, (None,))
            o_first(up, range(EARLY, BITS))

    def issue_far():
        for up in (True, False):

            @pl.when(s == end(up))
            def _():
                ahead(up, every_hop[1:], every_group)
                ahead(up, every_hop, (None,))

    for piece in range(PIECES):
        for up in (True, False):

            @pl.when(sends(up, 0))
            def _():
                act_z(up, 0, piece).start()

    act_x(0, s).start()
    act_c(0, s).start()
    with scope("wait_shift_load"):
        load_shift.wait()
    for q in range(seqs):
        values = raw_shift[:, q, :].astype(bf16)
        for k in range(n_sp):
            own_shift[k, q] = values[:, k * KEY : (k + 1) * KEY]
    shifts[:, place, :] = own_shift[s]
    for up in (True, False):

        @pl.when(s == end(up))
        def _():
            issue(up)

    def swap(d, pieces, match=True, late=None):
        for up in (True, False):

            @pl.when(jnp.logical_and(gets(up, d), match))
            def _():
                k = d + 1 if up else last - d
                for p in pieces:
                    tally(w_block(k, p), wz_out, wz_in.at[k - 1, p]).wait_recv()
                    w_y(k, p, 0 if late is None else 1 + late).start()

    at_end = jnp.logical_or(s == 0, s == last)
    late_source = jnp.where(at_end, last - s, lax.rem(s + 2, n_sp))

    def swap_late(group):
        swap(last - 1, range(*groups[group]), at_end, group)
        swap(last - 2, range(*groups[group]), jnp.logical_not(at_end), group)

    for d in range(last):
        if d == last - 1:
            with scope("swap_end"):
                for hop in range(last - 2, 0, -1):
                    swap(hop, range(count), at_end)
        for piece in range(PIECES):

            def arrived(up, d, origin):
                act_z(up, d, piece).wait_recv()
                if d + 1 < last:

                    @pl.when(sends(up, d + 1))
                    def _():
                        act_z(up, d + 1, piece).start()

                if piece == PIECES - 1:
                    act_x(slot(up, d), origin).start()
                    act_c(0, origin).start()

            with scope(f"act_z{d}_{piece}"):
                each(d, arrived)
        if d + 1 < last:
            for up in (True, False):

                @pl.when(s == (d + 1 if up else last - 1 - d))
                def _():
                    issue(up)

    o_own = remote(w_ref, matrix.at[w_rows, lanes(s, width)], oc_out, oc_in.at[0], (g, s, twin))
    o_own.start()

    def relay(index, origin):
        act_x(index, origin).wait_recv()
        act_c(1, origin).start()

    def o_take(up, d, origin, pieces=range(BITS)):
        for piece in pieces:
            o_z(up, d, piece).wait_recv()
            if d + 1 < last:

                @pl.when(sends(up, d + 1))
                def _():
                    o_z(up, d + 1, piece).start()

            o_y(slot(up, d), origin, piece).start()
            o_c(0, slot(up, d), origin, piece).start()

    def o_swapped(up, d, origin):
        for piece in range(BITS):
            o_y(slot(up, d), origin, piece).wait_recv()
            o_c(1, slot(up, d), origin, piece).start()

    with scope("take_early"):
        for up in (True, False):

            @pl.when(neighbour(up))
            def _():
                o_take(up, 0, s - step_of(up))

    with scope("swap_near0"):
        swap(0, range(TRIG))
    issue_far()
    with scope("swap_near1"):
        swap(0, range(TRIG, count))
    with scope("relay"):
        relay(0, s)
        for d in range(last):
            each(d, lambda up, d, origin: relay(slot(up, d), origin))

    def take_late(pieces, where):
        for up in (True, False):
            match = jnp.logical_and(gets(up, 0), jnp.logical_not(neighbour(up)))

            @pl.when(jnp.logical_and(match, where))
            def _():
                o_take(up, 0, s - step_of(up), pieces)

    def project(group):
        at = slice(groups[group][0] * KEY, groups[group][1] * KEY)
        from_late = span_at(late_source, depth)
        with scope(f"wait_w{group}"):
            block = weights.at[pl.ds(0, half), at]
            tally(block, wy_out, wy_in.at[1 + group]).wait_recv()

        def one(q, carry):
            more = jnp.dot(
                acts[q, :, from_late], weights[from_late, at], preferred_element_type=f32
            )
            proj[q, :, at] = (begun[q, :, at] + more).astype(bf16)
            return carry

        with scope(f"project{group}"):
            lax.fori_loop(0, seqs, one, 0)

    def begin(q, carry):
        total = None
        for i in range(1, n_sp):
            rows_now = span_at(lax.rem(late_source + i, n_sp), depth)
            more = jnp.dot(acts[q, :, rows_now], weights[rows_now, :], preferred_element_type=f32)
            total = more if total is None else total + more
        begun[q] = total
        return carry

    with scope("joined"):
        tally(acts.at[pl.ds(0, seqs // CORES)], ac_out, ac_in).wait_recv()
        here = weights.at[own_rows, :]
        pltpu.make_async_copy(here, here, load_sem.at[2]).wait()
    with scope("wait_w"):
        tally(weights.at[pl.ds(0, (last - 1) * half), :], wy_out, wy_in.at[0]).wait_recv()
    with scope("take_part_end"):
        take_late(range(BITS // 2), at_end)
    with scope("begin"):
        lax.fori_loop(0, seqs, begin, 0)
    for group in every_group:
        with scope(f"swap_late{group}"):
            swap_late(group)
    with scope("take_rest_end"):
        take_late(range(BITS // 2, BITS), at_end)
    project(0)
    project(1)
    with scope("act_drain"):
        tally(acts.at[:, pl.ds(0, n_sp * span), :], ax_out, ax_in.at[0]).wait_send()
        tally(acts.at[pl.ds(0, seqs // CORES)], ac_out, ac_in).wait_send()
        for d in range(last):
            for up in (True, False):

                @pl.when(sends(up, d))
                def _():
                    index = slot(up, d) - 1
                    tally(block(s, t), az_out.at[index], az_in.at[index, 0]).wait_send()

    with scope("take_part"):
        take_late(range(EARLY), jnp.logical_not(at_end))
    project(2)
    with scope("wait_shift"):
        tally(shifts.at[:, pl.ds(0, last * positions), :], sz_out, sz_in).wait_recv()

    targets = [(k, o) for k in range(n_sp) for o in range(CORES) if k or o]

    def m_move(q, k, o):
        return remote(
            mixed.at[q, z_at[k], :, core_at[o]],
            heads.at[:, q, :, lanes(c * n_sp + s, VAL)],
            m_out,
            m_in.at[q // lot],
            (g, z_at[k], x * CORES + core_at[o]),
        )

    def send_mixed(pair, stage):
        for k, o in targets:
            to_end = jnp.logical_or(z_at[k] == 0, z_at[k] == last)
            to_end = jnp.logical_and(to_end, k > 0)
            far = jnp.logical_and(to_end, jnp.abs(z_at[k] - s) > 1)
            if pair < FREE:
                match = stage == 0
            elif stage == 0:
                match = jnp.logical_not(to_end)
            elif stage == 1:
                match = jnp.logical_and(to_end, jnp.logical_not(far))
            else:
                match = far

            @pl.when(match)
            def _():
                for i in range(2):
                    m_move(2 * pair + i, k, o).start()

    def recur(pair, carry):
        for i in range(2):
            q = 2 * pair + i
            value = recur_one(proj, shifts, gap_ref, gain_ref, summed.at[i], q, lanes(s))
            mixed[q] = value.reshape(n_sp, n_x, CORES, span, VAL)
            heads[:, q, :, lanes(c * n_sp + s, VAL)] = mixed[q, s, :, c]
        send_mixed(pair, 0)
        return carry

    def take_second(pieces, where):
        for up in (True, False):

            @pl.when(jnp.logical_and(gets(up, 1), where))
            def _():
                o_take(up, 1, s - 2 * step_of(up), pieces)

    def take_third(pieces):
        each(last - 1, lambda up, d, origin: o_take(up, d, origin, pieces))

    for pair in range(seqs // 2):
        with scope(f"recur{pair}"):
            recur(pair, 0)
        if pair == 0:
            with scope("take_second"):
                take_second(range(EARLY), at_end)
    with scope("take_late"):
        take_late(range(EARLY, BITS), jnp.logical_not(at_end))
    with scope("w_drain"):
        tally(own_shift.at[pl.ds(0, last)], sz_out, sz_in).wait_send()
        every = weights.at[pl.ds(0, last * half), :]
        tally(every, wz_out, wz_in.at[0, 0]).wait_send()
        tally(every, wy_out, wy_in.at[0]).wait_send()
    w_own.wait()

    def p_move(index, origin, rows_now, part):
        at = lanes(origin, width)
        return remote(
            partial.at[1 - x, rows_now, :, at],
            landed.at[rows_now, :, at],
            p_out,
            p_in.at[index, part],
            (g, s, across),
        )

    lots = tuple(slice(h * lot, (h + 1) * lot) for h in range(PIECES))

    def strip(index, origin, rows_now, part):
        at = lanes(origin, width)
        lines = heads[:, rows_now].reshape(-1, heads.shape[-1])
        partial[:, rows_now, :, at] = (
            jnp.dot(lines, matrix[:, at], preferred_element_type=f32)
            .astype(bf16)
            .reshape(n_x, -1, span, width)
        )
        p_move(index, origin, rows_now, part).start()

    def arrived_strip(index, origin):
        at = lanes(origin, width)
        tally(matrix.at[pl.ds(0, depth), at], oc_out, oc_in.at[index]).wait_recv()

    def own_strip(part):
        strip(0, s, lots[part], part)

    def other_strip(d, part):
        def visit(up, d, origin):
            if part == 0:
                arrived_strip(slot(up, d), origin)
            strip(slot(up, d), origin, lots[part], part)

        each(d, visit)

    def mixed_in(part):
        here = heads.at[:, pl.ds(0, lot), :, pl.ds(0, len(targets) * VAL)]
        tally(here, m_out, m_in.at[part]).wait_recv()

    with scope("o_pass1"):
        take_second(range(EARLY, BITS), at_end)
        take_second(range(BITS), jnp.logical_not(at_end))
    for pair in range(FREE, seqs // 2):
        send_mixed(pair, 1)
    with scope("o_pass2a"):
        take_third(range(BITS // 2))
    for pair in range(FREE, seqs // 2):
        send_mixed(pair, 2)
    def second_swapped(where):
        for up in (True, False):

            @pl.when(jnp.logical_and(gets(up, 1), where))
            def _():
                o_swapped(up, 1, s - 2 * step_of(up))

    with scope("o_swapped0"):
        each(0, o_swapped)
    with scope("o_swapped1e"):
        second_swapped(at_end)
    with scope("wait_m0"):
        mixed_in(0)
    with scope("own_strip0"):
        arrived_strip(0, s)
        own_strip(0)
    with scope("near_strip0"):
        other_strip(0, 0)
    with scope("o_pass2b"):
        take_third(range(BITS // 2, BITS))
    for part in range(1, PIECES):
        with scope(f"wait_m{part}"):
            mixed_in(part)
        with scope(f"strips{part}"):
            own_strip(part)
            other_strip(0, part)
    with scope("o_swapped1m"):
        second_swapped(jnp.logical_not(at_end))
    for d in range(1, last):
        if d > 1:
            with scope(f"o_swapped{d}"):
                each(d, o_swapped)
        with scope(f"strip{d}"):
            for part in range(PIECES):
                other_strip(d, part)

    def finish(index, origin, parts):
        for part, rows_now in enumerate(parts):
            p_move(index, origin, rows_now, part).wait_recv()
            at = lanes(origin, width)
            total = partial[x, rows_now, :, at].astype(f32) + landed[rows_now, :, at].astype(f32)
            out_ref[rows_now, :, at] = total.astype(bf16)

    with scope("finish"):
        finish(0, s, lots)
        for d in range(last):
            each(d, lambda up, d, origin: finish(slot(up, d), origin, lots))
    with scope("drain"):
        here = heads.at[:, :, :, pl.ds(0, len(targets) * VAL)]
        tally(here, m_out, m_in.at[0]).wait_send()
        strips = matrix.at[pl.ds(0, half), pl.ds(0, last * width)]
        tally(strips, oy_out, oy_in.at[0, 0]).wait_send()
        tally(matrix.at[pl.ds(0, depth), :], oc_out, oc_in.at[0]).wait_send()
        tally(landed, p_out, p_in.at[0, 0]).wait_send()
        for d in range(last):
            for up in (True, False):

                @pl.when(sends(up, d))
                def _():
                    index = slot(up, d) - 1
                    here = matrix.at[pl.ds(0, half), pl.ds(0, width)]
                    tally(here, oz_out.at[index], oz_in.at[index, 0]).wait_send()


def layer(sizes, tokens, norm_gain, shift, sources, gap, gain, w_out):
    n_grp, n_sp, n_tp = sizes
    n_x = n_tp // CORES
    span, seqs, model = tokens.shape
    length = n_sp * n_tp * span
    count = len(sources)
    depth, width = w_out.shape
    slots = 2 * n_sp - 1
    dma = pltpu.SemaphoreType.DMA
    hbm = pl.BlockSpec(memory_space=pltpu.HBM)
    vmem = pl.BlockSpec(memory_space=pltpu.VMEM)
    bf16 = jnp.bfloat16
    return pl.pallas_call(
        functools.partial(layer_kernel, sizes),
        out_shape=jax.ShapeDtypeStruct((seqs, span, n_sp * width), bf16),
        in_specs=[hbm] * (6 + count),
        out_specs=vmem,
        scratch_shapes=[
            pltpu.VMEM(norm_gain.shape, norm_gain.dtype),
            pltpu.VMEM(gap.shape, gap.dtype),
            pltpu.VMEM(gain.shape, gain.dtype),
            pltpu.VMEM(tokens.shape, bf16),
            pltpu.VMEM(tokens.shape, jnp.float32),
            pltpu.VMEM(shift.shape, shift.dtype),
            pltpu.VMEM((n_sp, seqs, n_tp * span, KEY), bf16),
            pltpu.VMEM((seqs, length, KEY), bf16),
            pltpu.VMEM((seqs, length, model), bf16),
            pltpu.VMEM((model, count * KEY), bf16),
            pltpu.VMEM((seqs, length, count * KEY), jnp.float32),
            pltpu.VMEM((seqs, length, count * KEY), bf16),
            pltpu.VMEM((2, length, VAL), jnp.float32),
            pltpu.VMEM((seqs, n_sp, n_x, CORES, span, VAL), bf16),
            pltpu.VMEM((n_x, seqs, span, CORES * depth), bf16),
            pltpu.VMEM((CORES * depth, n_sp * width), bf16),
            pltpu.VMEM((n_x, seqs, span, n_sp * width), bf16),
            pltpu.VMEM((seqs, span, n_sp * width), bf16),
            dma((7,)),
            dma((slots - 1,)),
            dma((slots - 1, PIECES)),
            dma,
            dma((slots,)),
            dma,
            dma,
            dma,
            dma((n_sp - 1, count)),
            dma,
            dma((4,)),
            dma,
            dma,
            dma((slots - 1,)),
            dma((slots - 1, BITS)),
            dma,
            dma((slots - 1, BITS)),
            dma,
            dma((slots,)),
            dma,
            dma((PIECES,)),
            dma,
            dma((slots, PIECES)),
        ],
        compiler_params=pltpu.CompilerParams(
            collective_id=0, has_side_effects=True, vmem_limit_bytes=int(VL * 1024 * 1024)
        ),
    )(tokens, norm_gain, shift, *sources, gap, gain, w_out)


def head_shards(
    sizes,
    tokens,
    norm_gain,
    w_query,
    w_value,
    w_fwd_gate,
    w_bwd_gate,
    w_out_gate,
    floor_gap,
    decay_shift,
    head_gain,
    w_out,
):
    return layer(
        sizes,
        tokens,
        norm_gain.reshape(1, 1, -1),
        decay_shift,
        (w_query, w_value, w_fwd_gate, w_bwd_gate, w_out_gate),
        floor_gap,
        head_gain.reshape(1, VAL),
        w_out,
    ).transpose(1, 0, 2)


def by_heads(mesh):
    n_sp, n_tp = mesh.shape["sp"], mesh.shape["tp"]

    def run(*arrays):
        tokens, w_query = arrays[0], arrays[2]
        heads_here = w_query.shape[1] // KEY // n_tp
        span = tokens.shape[0] // (n_sp * n_tp)
        sizes = (mesh.shape["grp"], n_sp, n_tp)
        fits = heads_here == n_sp and n_sp == CORES * 2 and n_tp == 2 * CORES and span % 16 == 0
        fits = fits and sizes[0] == 2 and tokens.shape[1] // sizes[0] % PIECES == 0
        fits = fits and tokens.shape[0] % BLOCK == 0 and tokens.shape[0] <= 512
        body = functools.partial(head_shards, sizes) if fits else shards
        return mapped(body, mesh)(*arrays)

    return run


def mapped(body, mesh):
    return jax.shard_map(
        body,
        mesh=mesh,
        in_specs=(
            P(("sp", "tp"), "grp", None),
            P(),
            P("sp", "tp"),
            P("sp", "tp"),
            P("sp", "tp"),
            P("sp", "tp"),
            P("sp", "tp"),
            P(None, "tp"),
            P("sp", "grp", "tp"),
            P(),
            P("tp", "sp"),
        ),
        out_specs=P(("sp", "tp"), "grp", None),
        check_vma=False,
    )


def solution(mesh):
    return by_heads(mesh)
```

```python
import functools

import jax
import jax.numpy as jnp
from jax import lax
from jax.experimental import pallas as pl
from jax.experimental.pallas import tpu as pltpu
from jax.sharding import PartitionSpec as P

KEY = 128
VAL = 128
BLOCK = 64


norm_eps = 1e-06
highest = lax.Precision.HIGHEST


def carried_in(x, axis, join, neutral, backward):
    count = lax.axis_size(axis)
    place = lax.axis_index(axis)
    ahead = count - 1 - place if backward else place
    gathered = jax.tree.map(
        lambda a, kind: lax.all_gather(a.astype(kind), axis), x, (jnp.bfloat16, jnp.bfloat16)
    )
    state = jax.tree.map(lambda a, e: jnp.zeros_like(a) + jnp.asarray(e, a.dtype), x, neutral)

    def one(turn, state):
        source = count - 1 - turn if backward else turn
        return join(
            state,
            jax.tree.map(
                lambda a, own: lax.dynamic_index_in_dim(a, source, 0, False).astype(own.dtype),
                gathered,
                x,
            ),
        )

    return lax.fori_loop(0, ahead, one, state)


def split_blocks(array):
    return array.reshape(array.shape[0] // BLOCK, BLOCK, *array.shape[1:])


def prepare_chain(queries, key_cols, values, log_decay):
    query_blocks = split_blocks(queries)
    key_blocks = split_blocks(key_cols)
    value_blocks = split_blocks(values)
    running = jnp.cumsum(split_blocks(log_decay), axis=1)
    block_end = running[:, -1]
    block_state = jnp.einsum(
        "nsbhk,nsbhe->nbhke",
        key_blocks * jnp.exp(block_end[:, None] - running),
        value_blocks,
        precision=highest,
    )
    carry_state = jnp.zeros_like(block_state[0])
    log_total = jnp.zeros_like(block_end[0])
    offsets = [log_total]
    carry_state = jnp.exp(block_end[0])[..., None] * carry_state + block_state[0]
    log_total = block_end[0]
    return (
        query_blocks,
        key_blocks,
        value_blocks,
        running,
        block_state,
        jnp.stack(offsets),
        log_total,
        carry_state,
    )


def local_pass(chain, carry_state):
    query_blocks, key_blocks, value_blocks, running, block_state = (
        chain[0],
        chain[1],
        chain[2],
        chain[3],
        chain[4],
    )
    block_len = running.shape[1]
    earlier_mask = jnp.arange(block_len)[:, None] >= jnp.arange(block_len)[None, :]
    here = running[0]
    anchor = here[:1]
    query_scaled = query_blocks[0] * jnp.exp(here - anchor)
    key_scaled = key_blocks[0] * jnp.exp(anchor - here)
    scores = jnp.einsum("tbhk,sbhk->bhts", query_scaled, key_scaled, precision=highest)
    scores = jnp.where(earlier_mask, scores, 0.0)
    within = jnp.einsum("bhts,sbhe->tbhe", scores, value_blocks[0], precision=highest)
    carried = jnp.einsum(
        "tbhk,bhke->tbhe", query_blocks[0] * jnp.exp(here), carry_state, precision=highest
    )
    outputs = within + carried
    return outputs


def combine(earlier, later):
    return (earlier[0] + later[0], jnp.exp(later[0])[..., None] * earlier[1] + later[1])


def group_sums(flat_mixed, weight_lines, group_count):
    group_width = flat_mixed.shape[1] // group_count
    accumulated_total = jnp.zeros((flat_mixed.shape[0], weight_lines.shape[1]), jnp.float32)
    for tp_group in range(group_count):
        first_column = tp_group * group_width
        partial_value = jnp.dot(
            flat_mixed[:, first_column : first_column + group_width],
            weight_lines[first_column : first_column + group_width],
            preferred_element_type=jnp.float32,
        ).astype(jnp.bfloat16)
        accumulated_total = accumulated_total + lax.optimization_barrier(partial_value).astype(
            jnp.float32
        )
    return accumulated_total


def shards(
    tokens,
    norm_gain,
    w_query,
    w_value,
    w_fwd_gate,
    w_bwd_gate,
    w_out_gate,
    floor_gap,
    decay_shift,
    head_gain,
    w_out,
):
    token_f32 = tokens.astype(jnp.float32)
    scale_rows = lax.rsqrt(jnp.mean(token_f32 * token_f32, axis=-1, keepdims=True) + norm_eps)
    normed = (token_f32 * scale_rows * norm_gain).astype(jnp.bfloat16)
    weights = (
        lax.all_gather(w_query, "sp", axis=0, tiled=True),
        lax.all_gather(w_value, "sp", axis=0, tiled=True),
        lax.all_gather(w_fwd_gate, "sp", axis=0, tiled=True),
        lax.all_gather(w_bwd_gate, "sp", axis=0, tiled=True),
        lax.all_gather(w_out_gate, "sp", axis=0, tiled=True),
    )
    piece_rows = lax.all_gather(normed, "tp", axis=0, tiled=True)
    flat_rows = piece_rows.reshape(-1, piece_rows.shape[2])
    columns = [
        jnp.dot(flat_rows, matrix, preferred_element_type=jnp.float32).astype(jnp.bfloat16)
        for matrix in weights
    ]
    projected = lax.optimization_barrier(
        jnp.concatenate(columns, axis=1).reshape(piece_rows.shape[0], piece_rows.shape[1], -1)
    )
    key_width = w_query.shape[1]
    value_width = w_value.shape[1]
    heads_here = key_width // KEY
    extent_rows = projected.shape[0]
    seq_count = projected.shape[1]
    bounds_list = [
        0,
        key_width,
        key_width + value_width,
        2 * key_width + value_width,
        3 * key_width + value_width,
        3 * key_width + 2 * value_width,
    ]

    def section_part(position, feature_lanes):
        picked = projected[:, :, bounds_list[position] : bounds_list[position + 1]].astype(
            jnp.float32
        )
        return picked.reshape(extent_rows, seq_count, heads_here, feature_lanes)

    queries = jax.nn.silu(section_part(0, KEY))
    values = section_part(1, VAL)
    shift = decay_shift.reshape(extent_rows, seq_count, heads_here, KEY)
    key_fwd = floor_gap[0].reshape(heads_here, KEY) * jax.nn.sigmoid(-section_part(2, KEY))
    key_bwd = floor_gap[1].reshape(heads_here, KEY) * jax.nn.sigmoid(-section_part(3, KEY))
    decay_fwd = jnp.log1p(-key_fwd) + shift
    decay_bwd = jnp.log1p(-key_bwd) + shift
    fwd_chain = prepare_chain(queries, key_fwd, values, decay_fwd)
    bwd_chain = prepare_chain(queries[::-1], key_bwd[::-1], values[::-1], decay_bwd[::-1])
    identity_pair = (jnp.zeros_like(fwd_chain[6]), jnp.zeros_like(fwd_chain[7]))
    fwd_in = carried_in((fwd_chain[6], fwd_chain[7]), "sp", combine, identity_pair, False)[1]
    bwd_in = carried_in((bwd_chain[6], bwd_chain[7]), "sp", combine, identity_pair, True)[1]
    out_fwd = local_pass(fwd_chain, fwd_in)
    out_bwd = local_pass(bwd_chain, bwd_in)
    combined = out_fwd + out_bwd[::-1]
    head_normed = (
        combined
        * lax.rsqrt(jnp.mean(combined * combined, axis=-1, keepdims=True) + norm_eps)
        * head_gain
    )
    gate_value = jax.nn.silu(projected[:, :, bounds_list[4] : bounds_list[5]].astype(jnp.float32))
    mixed = (head_normed.reshape(extent_rows, seq_count, value_width) * gate_value).astype(
        jnp.bfloat16
    )
    token_rows = lax.all_to_all(mixed, "tp", split_axis=0, concat_axis=2, tiled=True)
    flat_mixed = token_rows.reshape(-1, token_rows.shape[2])
    group_count = lax.axis_size("tp")
    w_columns = lax.all_gather(w_out, "sp", axis=1, tiled=True)
    w_full = lax.all_gather(w_columns, "tp", axis=0, tiled=True)
    accumulated_total = group_sums(flat_mixed, w_full, group_count)
    result = accumulated_total.reshape(token_rows.shape[0], token_rows.shape[1], -1)
    return result.astype(jnp.bfloat16)


MESH = pl.DeviceIdType.MESH
CORES = 2
PIECES = 2
BITS = 4
EARLY = 3
VL = 56
TRIG = 2
FREE = 1
scope = jax.named_scope


def recur_one(proj_ref, shift_ref, gap_ref, gain_ref, out_ref, i, own):
    f32 = jnp.float32
    bf16 = jnp.bfloat16
    length = proj_ref.shape[1]

    def cols(p):
        return proj_ref[i, :, p * KEY : (p + 1) * KEY]

    queries = cols(0).astype(f32)
    queries = queries * jax.nn.sigmoid(queries)
    values = cols(1)
    shift = shift_ref[i].astype(f32)
    row = lax.broadcasted_iota(jnp.int32, (length, length), 0)
    col = lax.broadcasted_iota(jnp.int32, (length, length), 1)
    near = row // BLOCK == col // BLOCK
    row = lax.broadcasted_iota(jnp.int32, (BLOCK, BLOCK), 0)
    col_b = lax.broadcasted_iota(jnp.int32, (BLOCK, BLOCK), 1)
    seen = [row >= col_b, row <= col_b]
    row_l = lax.broadcasted_iota(jnp.int32, (length, length), 0)
    order = [row_l >= col, row_l <= col]
    blocks = length // BLOCK
    keys, here = [], []
    for d in range(2):
        key = gap_ref[d : d + 1, own] * jax.nn.sigmoid(-cols(2 + d).astype(f32))
        decay = jnp.log1p(-key) + shift
        high = decay.astype(bf16)
        rest = decay - high.astype(f32)
        middle = rest.astype(bf16)
        low = (rest - middle.astype(f32)).astype(bf16)
        tri = jnp.where(jnp.logical_and(near, order[d]), 1.0, 0.0).astype(bf16)
        sums = jnp.dot(
            tri, jnp.concatenate([high, middle, low], axis=1), preferred_element_type=f32
        )
        here.append(sums[:, :KEY] + (sums[:, KEY : 2 * KEY] + sums[:, 2 * KEY :]))
        keys.append(key)
    state = [None, None]
    outs = [[None, None] for _ in range(blocks)]
    for step in range(blocks):
        for d in range(2):
            n = step if d == 0 else blocks - 1 - step
            at = slice(n * BLOCK, (n + 1) * BLOCK)
            q, k, v, h = queries[at], keys[d][at], values[at], here[d][at]
            edge = h[BLOCK - 1 : BLOCK] if d == 0 else h[0:1]
            anchor = h[BLOCK // 2 : BLOCK // 2 + 1]
            scores = lax.dot_general(
                (q * jnp.exp(h - anchor)).astype(bf16),
                (k * jnp.exp(anchor - h)).astype(bf16),
                (((1,), (1,)), ((), ())),
                preferred_element_type=f32,
            )
            scores = jnp.where(seen[d], scores, 0.0).astype(bf16)
            out = jnp.dot(scores, v, preferred_element_type=f32)
            if state[d] is not None:
                out = out + lax.dot_general(
                    (q * jnp.exp(h)).astype(bf16),
                    state[d].astype(bf16),
                    (((1,), (1,)), ((), ())),
                    preferred_element_type=f32,
                )
            outs[n][d] = out
            if step < blocks - 1:
                fresh = lax.dot_general(
                    v,
                    (k * jnp.exp(edge - h)).astype(bf16),
                    (((0,), (0,)), ((), ())),
                    preferred_element_type=f32,
                )
                state[d] = fresh if state[d] is None else state[d] * jnp.exp(edge) + fresh
    for n in range(blocks):
        out_ref[n * BLOCK : (n + 1) * BLOCK] = outs[n][0] + outs[n][1]
    combined = out_ref[...]
    normed = combined * lax.rsqrt(jnp.mean(combined * combined, axis=-1, keepdims=True) + norm_eps)
    gate = cols(4).astype(f32)
    return (normed * gain_ref[...] * (gate * jax.nn.sigmoid(gate))).astype(bf16)


def layer_kernel(
    sizes,
    token_ref,
    norm_hbm,
    shift_ref,
    wq_ref,
    wv_ref,
    wf_ref,
    wb_ref,
    wg_ref,
    gap_hbm,
    gain_hbm,
    w_ref,
    out_ref,
    norm_ref,
    gap_ref,
    gain_ref,
    rows_in,
    wide,
    raw_shift,
    own_shift,
    shifts,
    acts,
    weights,
    begun,
    proj,
    summed,
    mixed,
    heads,
    matrix,
    partial,
    landed,
    load_sem,
    az_out,
    az_in,
    ax_out,
    ax_in,
    ac_out,
    ac_in,
    wz_out,
    wz_in,
    wy_out,
    wy_in,
    sz_out,
    sz_in,
    oz_out,
    oz_in,
    oy_out,
    oy_in,
    oc_out,
    oc_in,
    m_out,
    m_in,
    p_out,
    p_in,
):
    bf16 = jnp.bfloat16
    f32 = jnp.float32
    n_grp, n_sp, n_tp = sizes
    n_x = n_tp // CORES
    g = lax.axis_index("grp")
    s = lax.axis_index("sp")
    t = lax.axis_index("tp")
    x = t // CORES
    c = t % CORES
    twin = x * CORES + (1 - c)
    across = (1 - x) * CORES + c
    seqs = acts.shape[0]
    span = token_ref.shape[0]
    positions = n_tp * span
    depth = wq_ref.shape[0]
    half = depth // n_grp
    width = w_ref.shape[1]
    lot = seqs // PIECES
    bit = half // BITS
    sources = (wq_ref, wv_ref, wf_ref, wb_ref, wg_ref)
    count = len(sources)
    groups = ((0, 2), (2, 4), (4, 5))
    last = n_sp - 1
    z_at = [lax.rem(s + k, n_sp) for k in range(n_sp)]
    z_from = [lax.rem(s + n_sp - k, n_sp) for k in range(n_sp)]
    core_at = [c, 1 - c]

    def span_at(where, size):
        return pl.ds(pl.multiple_of(where * size, size), size)

    def lanes(where, size=KEY):
        return span_at(where, size)

    def remote(src, dst, out_sem, in_sem, peer):
        return pltpu.make_async_remote_copy(
            src_ref=src,
            dst_ref=dst,
            send_sem=out_sem,
            recv_sem=in_sem,
            device_id=peer,
            device_id_type=MESH,
        )

    def tally(ref, out_sem, in_sem):
        return remote(ref, ref, out_sem, in_sem, (g, s, twin))

    def inside(place):
        return jnp.logical_and(place >= 0, place < n_sp)

    def step_of(up):
        return 1 if up else -1

    def slot(up, d):
        return 1 + d if up else n_sp + d

    def end(up):
        return 0 if up else last

    def sends(up, d):
        return jnp.logical_and(inside(s + step_of(up)), inside(s - step_of(up) * d))

    def gets(up, d):
        return inside(s - step_of(up) * (d + 1))

    def each(d, visit):
        for up in (True, False):

            @pl.when(gets(up, d))
            def _():
                visit(up, d, s - step_of(up) * (d + 1))

    load_rows = pltpu.make_async_copy(token_ref, rows_in, load_sem.at[0])
    load_shift = pltpu.make_async_copy(shift_ref, raw_shift, load_sem.at[1])
    load_rows.start()
    small = [
        pltpu.make_async_copy(src, dst, load_sem.at[4 + i])
        for i, (src, dst) in enumerate(
            ((norm_hbm, norm_ref), (gap_hbm, gap_ref), (gain_hbm, gain_ref))
        )
    ]
    for copy in small:
        copy.start()
    load_shift.start()
    peers = [(g, z_at[k], x * CORES + core_at[o]) for k in range(n_sp) for o in range(CORES)]
    peers = peers[1:] + [(g, s, across), (1 - g, s, t)]
    barrier = pltpu.get_barrier_semaphore()
    for peer in peers:
        pl.semaphore_signal(barrier, inc=1, device_id=peer, device_id_type=MESH)
    own_rows = span_at(s, depth)
    for p, w in enumerate(sources):
        pltpu.make_async_copy(
            w.at[:, lanes(s)], weights.at[own_rows, pl.ds(p * KEY, KEY)], load_sem.at[2]
        ).start()
    w_rows = span_at(c, depth)
    w_own = pltpu.make_async_copy(w_ref, matrix.at[w_rows, lanes(s, width)], load_sem.at[3])
    w_own.start()

    here_rows = span_at(s * n_tp + t, span)
    with scope("wait_rows"):
        load_rows.wait()
        for copy in small:
            copy.wait()
    rows = rows_in[...].astype(f32)
    scale = lax.rsqrt(jnp.mean(rows * rows, axis=-1, keepdims=True) + norm_eps)
    wide[...] = rows * scale * norm_ref[...]
    for q in range(seqs):
        acts[q, here_rows, :] = wide[:, q, :].astype(bf16)
    with scope("barrier"):
        pl.semaphore_wait(barrier, len(peers))

    def block(where_s, where_t):
        return acts.at[:, span_at(where_s * n_tp + where_t, span), :]

    def act_z(up, d, piece):
        at = span_at((s - step_of(up) * d) * n_tp + t, span)
        here = acts.at[pl.ds(piece * lot, lot), at, :]
        index = slot(up, d) - 1
        peer = (g, s + step_of(up), t)
        return remote(here, here, az_out.at[index], az_in.at[index, piece], peer)

    def act_x(index, origin):
        here = block(origin, t)
        return remote(here, here, ax_out, ax_in.at[index], (g, s, across))

    def act_c(far, origin):
        here = block(origin, across if far else t)
        return remote(here, here, ac_out, ac_in, (g, s, twin))

    part = span_at(g, half)

    def w_z(k, p):
        src = sources[p].at[part, lanes(z_at[k])]
        dst = weights.at[span_at(s * n_grp + g, half), pl.ds(p * KEY, KEY)]
        return remote(src, dst, wz_out, wz_in.at[k - 1, p], (g, z_at[k], t))

    def w_block(k, p):
        return weights.at[span_at(z_from[k] * n_grp + g, half), pl.ds(p * KEY, KEY)]

    def w_y(k, p, index):
        here = w_block(k, p)
        return remote(here, here, wy_out, wy_in.at[index], (1 - g, s, t))

    place = span_at(s, positions)

    def s_z(k):
        return remote(own_shift.at[z_at[k]], shifts.at[:, place, :], sz_out, sz_in, (g, z_at[k], t))

    def o_block(where_s, where_g, where_c, piece):
        at = pl.multiple_of(where_c * depth + where_g * half + piece * bit, bit)
        return matrix.at[pl.ds(at, bit), lanes(where_s, width)]

    def o_z(up, d, piece):
        here = o_block(s - step_of(up) * d, g, c, piece)
        src = w_ref.at[span_at(g * BITS + piece, bit), :] if d == 0 else here
        index = slot(up, d) - 1
        peer = (g, s + step_of(up), t)
        return remote(src, here, oz_out.at[index], oz_in.at[index, piece], peer)

    def o_y(index, origin, piece):
        here = o_block(origin, g, c, piece)
        return remote(here, here, oy_out, oy_in.at[index - 1, piece // 2], (1 - g, s, t))

    def o_c(far, index, origin, piece):
        here = o_block(origin, 1 - g if far else g, c, piece)
        return remote(here, here, oc_out, oc_in.at[index], (g, s, twin))

    def ahead(up, hops, groups_now):
        for hop in hops:
            k = hop if up else n_sp - hop
            go_up = s + k < n_sp

            @pl.when(go_up if up else jnp.logical_not(go_up))
            def _():
                for group in groups_now:
                    if group is None:
                        s_z(k).start()
                    else:
                        for p in range(*groups[group]):
                            w_z(k, p).start()

    every_group = range(len(groups))
    every_hop = range(1, n_sp)

    def neighbour(up):
        return s == (1 if up else last - 1)

    def o_first(up, pieces):
        @pl.when(sends(up, 0))
        def _():
            for piece in pieces:
                o_z(up, 0, piece).start()

    def issue(up):
        @pl.when(s == end(up))
        def _():
            o_first(up, range(BITS))
            ahead(up, (1,), every_group)

        @pl.when(neighbour(not up))
        def _():
            ahead(up, every_hop[::-1], every_group)
            o_first(up, range(BITS))
            ahead(up, every_hop, (None,))

        @pl.when(neighbour(up))
        def _():
            ahead(up, every_hop[::-1], every_group)
            o_first(up, range(EARLY))
            ahead(up, every_hop, (None,))
            o_first(up, range(EARLY, BITS))

    def issue_far():
        for up in (True, False):

            @pl.when(s == end(up))
            def _():
                ahead(up, every_hop[1:], every_group)
                ahead(up, every_hop, (None,))

    for piece in range(PIECES):
        for up in (True, False):

            @pl.when(sends(up, 0))
            def _():
                act_z(up, 0, piece).start()

    act_x(0, s).start()
    act_c(0, s).start()
    with scope("wait_shift_load"):
        load_shift.wait()
    for q in range(seqs):
        values = raw_shift[:, q, :].astype(bf16)
        for k in range(n_sp):
            own_shift[k, q] = values[:, k * KEY : (k + 1) * KEY]
    shifts[:, place, :] = own_shift[s]
    for up in (True, False):

        @pl.when(s == end(up))
        def _():
            issue(up)

    def swap(d, pieces, match=True, late=None):
        for up in (True, False):

            @pl.when(jnp.logical_and(gets(up, d), match))
            def _():
                k = d + 1 if up else last - d
                for p in pieces:
                    tally(w_block(k, p), wz_out, wz_in.at[k - 1, p]).wait_recv()
                    w_y(k, p, 0 if late is None else 1 + late).start()

    at_end = jnp.logical_or(s == 0, s == last)
    late_source = jnp.where(at_end, last - s, lax.rem(s + 2, n_sp))

    def swap_late(group):
        swap(last - 1, range(*groups[group]), at_end, group)
        swap(last - 2, range(*groups[group]), jnp.logical_not(at_end), group)

    for d in range(last):
        if d == last - 1:
            with scope("swap_end"):
                for hop in range(last - 2, 0, -1):
                    swap(hop, range(count), at_end)
        for piece in range(PIECES):

            def arrived(up, d, origin):
                act_z(up, d, piece).wait_recv()
                if d + 1 < last:

                    @pl.when(sends(up, d + 1))
                    def _():
                        act_z(up, d + 1, piece).start()

                if piece == PIECES - 1:
                    act_x(slot(up, d), origin).start()
                    act_c(0, origin).start()

            with scope(f"act_z{d}_{piece}"):
                each(d, arrived)
        if d + 1 < last:
            for up in (True, False):

                @pl.when(s == (d + 1 if up else last - 1 - d))
                def _():
                    issue(up)

    o_own = remote(w_ref, matrix.at[w_rows, lanes(s, width)], oc_out, oc_in.at[0], (g, s, twin))
    o_own.start()

    def relay(index, origin):
        act_x(index, origin).wait_recv()
        act_c(1, origin).start()

    def o_take(up, d, origin, pieces=range(BITS)):
        for piece in pieces:
            o_z(up, d, piece).wait_recv()
            if d + 1 < last:

                @pl.when(sends(up, d + 1))
                def _():
                    o_z(up, d + 1, piece).start()

            o_y(slot(up, d), origin, piece).start()
            o_c(0, slot(up, d), origin, piece).start()

    def o_swapped(up, d, origin):
        for first in range(0, BITS, 2):
            at = pl.multiple_of(c * depth + (1 - g) * half + first * bit, bit)
            here = matrix.at[pl.ds(at, 2 * bit), lanes(origin, width)]
            index = slot(up, d)
            tally(here, oy_out, oy_in.at[index - 1, first // 2]).wait_recv()
            remote(here, here, oc_out, oc_in.at[index], (g, s, twin)).start()

    with scope("take_early"):
        for up in (True, False):

            @pl.when(neighbour(up))
            def _():
                o_take(up, 0, s - step_of(up))

    with scope("swap_near0"):
        swap(0, range(TRIG))
    issue_far()
    with scope("swap_near1"):
        swap(0, range(TRIG, count))
    with scope("relay"):
        relay(0, s)
        for d in range(last):
            each(d, lambda up, d, origin: relay(slot(up, d), origin))

    def take_late(pieces, where):
        for up in (True, False):
            match = jnp.logical_and(gets(up, 0), jnp.logical_not(neighbour(up)))

            @pl.when(jnp.logical_and(match, where))
            def _():
                o_take(up, 0, s - step_of(up), pieces)

    def project(group):
        at = slice(groups[group][0] * KEY, groups[group][1] * KEY)
        from_late = span_at(late_source, depth)
        with scope(f"wait_w{group}"):
            block = weights.at[pl.ds(0, half), at]
            tally(block, wy_out, wy_in.at[1 + group]).wait_recv()

        def one(q, carry):
            more = jnp.dot(
                acts[q, :, from_late], weights[from_late, at], preferred_element_type=f32
            )
            proj[q, :, at] = (begun[q, :, at] + more).astype(bf16)
            return carry

        with scope(f"project{group}"):
            lax.fori_loop(0, seqs, one, 0)

    def begin(q, carry):
        total = None
        for i in range(1, n_sp):
            rows_now = span_at(lax.rem(late_source + i, n_sp), depth)
            more = jnp.dot(acts[q, :, rows_now], weights[rows_now, :], preferred_element_type=f32)
            total = more if total is None else total + more
        begun[q] = total
        return carry

    with scope("joined"):
        tally(acts.at[pl.ds(0, seqs // CORES)], ac_out, ac_in).wait_recv()
        here = weights.at[own_rows, :]
        pltpu.make_async_copy(here, here, load_sem.at[2]).wait()
    with scope("wait_w"):
        tally(weights.at[pl.ds(0, (last - 1) * half), :], wy_out, wy_in.at[0]).wait_recv()
    with scope("take_part_end"):
        take_late(range(BITS // 2), at_end)
    with scope("begin"):
        lax.fori_loop(0, seqs, begin, 0)
    for group in every_group:
        with scope(f"swap_late{group}"):
            swap_late(group)
    with scope("take_rest_end"):
        take_late(range(BITS // 2, BITS), at_end)
    project(0)
    project(1)
    with scope("act_drain"):
        tally(acts.at[:, pl.ds(0, n_sp * span), :], ax_out, ax_in.at[0]).wait_send()
        tally(acts.at[pl.ds(0, seqs // CORES)], ac_out, ac_in).wait_send()
        for d in range(last):
            for up in (True, False):

                @pl.when(sends(up, d))
                def _():
                    index = slot(up, d) - 1
                    tally(block(s, t), az_out.at[index], az_in.at[index, 0]).wait_send()

    with scope("take_part"):
        take_late(range(EARLY), jnp.logical_not(at_end))
    project(2)
    with scope("wait_shift"):
        tally(shifts.at[:, pl.ds(0, last * positions), :], sz_out, sz_in).wait_recv()

    targets = [(k, o) for k in range(n_sp) for o in range(CORES) if k or o]

    def m_move(q, k, o):
        return remote(
            mixed.at[q, z_at[k], :, core_at[o]],
            heads.at[:, q, :, lanes(c * n_sp + s, VAL)],
            m_out,
            m_in.at[q // lot],
            (g, z_at[k], x * CORES + core_at[o]),
        )

    def send_mixed(pair, stage):
        for k, o in targets:
            to_end = jnp.logical_or(z_at[k] == 0, z_at[k] == last)
            to_end = jnp.logical_and(to_end, k > 0)
            far = jnp.logical_and(to_end, jnp.abs(z_at[k] - s) > 1)
            if pair < FREE:
                match = stage == 0
            elif stage == 0:
                match = jnp.logical_not(to_end)
            elif stage == 1:
                match = jnp.logical_and(to_end, jnp.logical_not(far))
            else:
                match = far

            @pl.when(match)
            def _():
                for i in range(2):
                    m_move(2 * pair + i, k, o).start()

    def recur(pair, carry):
        for i in range(2):
            q = 2 * pair + i
            value = recur_one(proj, shifts, gap_ref, gain_ref, summed.at[i], q, lanes(s))
            mixed[q] = value.reshape(n_sp, n_x, CORES, span, VAL)
            heads[:, q, :, lanes(c * n_sp + s, VAL)] = mixed[q, s, :, c]
        send_mixed(pair, 0)
        return carry

    def take_second(pieces, where):
        for up in (True, False):

            @pl.when(jnp.logical_and(gets(up, 1), where))
            def _():
                o_take(up, 1, s - 2 * step_of(up), pieces)

    def take_third(pieces):
        each(last - 1, lambda up, d, origin: o_take(up, d, origin, pieces))

    for pair in range(seqs // 2):
        with scope(f"recur{pair}"):
            recur(pair, 0)
        if pair == 0:
            with scope("take_second"):
                take_second(range(EARLY), at_end)
    with scope("take_late"):
        take_late(range(EARLY, BITS), jnp.logical_not(at_end))
    with scope("w_drain"):
        tally(own_shift.at[pl.ds(0, last)], sz_out, sz_in).wait_send()
        every = weights.at[pl.ds(0, last * half), :]
        tally(every, wz_out, wz_in.at[0, 0]).wait_send()
        tally(every, wy_out, wy_in.at[0]).wait_send()
    w_own.wait()

    def p_move(index, origin, rows_now, part):
        at = lanes(origin, width)
        return remote(
            partial.at[1 - x, rows_now, :, at],
            landed.at[rows_now, :, at],
            p_out,
            p_in.at[index, part],
            (g, s, across),
        )

    lots = tuple(slice(h * lot, (h + 1) * lot) for h in range(PIECES))

    def strip(index, origin, rows_now, part):
        at = lanes(origin, width)
        lines = heads[:, rows_now].reshape(-1, heads.shape[-1])
        partial[:, rows_now, :, at] = (
            jnp.dot(lines, matrix[:, at], preferred_element_type=f32)
            .astype(bf16)
            .reshape(n_x, -1, span, width)
        )
        p_move(index, origin, rows_now, part).start()

    def arrived_strip(index, origin):
        at = lanes(origin, width)
        tally(matrix.at[pl.ds(0, depth), at], oc_out, oc_in.at[index]).wait_recv()

    def own_strip(part):
        strip(0, s, lots[part], part)

    def other_strip(d, part):
        def visit(up, d, origin):
            if part == 0:
                arrived_strip(slot(up, d), origin)
            strip(slot(up, d), origin, lots[part], part)

        each(d, visit)

    def mixed_in(part):
        here = heads.at[:, pl.ds(0, lot), :, pl.ds(0, len(targets) * VAL)]
        tally(here, m_out, m_in.at[part]).wait_recv()

    with scope("o_pass1"):
        take_second(range(EARLY, BITS), at_end)
        take_second(range(BITS), jnp.logical_not(at_end))
    for pair in range(FREE, seqs // 2):
        send_mixed(pair, 1)
    with scope("o_pass2a"):
        take_third(range(BITS // 2))
    for pair in range(FREE, seqs // 2):
        send_mixed(pair, 2)
    def second_swapped(where):
        for up in (True, False):

            @pl.when(jnp.logical_and(gets(up, 1), where))
            def _():
                o_swapped(up, 1, s - 2 * step_of(up))

    with scope("o_swapped0"):
        each(0, o_swapped)
    with scope("o_swapped1e"):
        second_swapped(at_end)
    with scope("wait_m0"):
        mixed_in(0)
    with scope("own_strip0"):
        arrived_strip(0, s)
        own_strip(0)
    with scope("near_strip0"):
        other_strip(0, 0)
    with scope("o_pass2b"):
        take_third(range(BITS // 2, BITS))
    for part in range(1, PIECES):
        with scope(f"wait_m{part}"):
            mixed_in(part)
        with scope(f"strips{part}"):
            own_strip(part)
            other_strip(0, part)
    with scope("o_swapped1m"):
        second_swapped(jnp.logical_not(at_end))
    for d in range(1, last):
        if d > 1:
            with scope(f"o_swapped{d}"):
                each(d, o_swapped)
        with scope(f"strip{d}"):
            for part in range(PIECES):
                other_strip(d, part)

    def finish(index, origin, parts):
        for part, rows_now in enumerate(parts):
            p_move(index, origin, rows_now, part).wait_recv()
            at = lanes(origin, width)
            total = partial[x, rows_now, :, at].astype(f32) + landed[rows_now, :, at].astype(f32)
            out_ref[rows_now, :, at] = total.astype(bf16)

    with scope("finish"):
        finish(0, s, lots)
        for d in range(last):
            each(d, lambda up, d, origin: finish(slot(up, d), origin, lots))
    with scope("drain"):
        here = heads.at[:, :, :, pl.ds(0, len(targets) * VAL)]
        tally(here, m_out, m_in.at[0]).wait_send()
        strips = matrix.at[pl.ds(0, half), pl.ds(0, last * width)]
        tally(strips, oy_out, oy_in.at[0, 0]).wait_send()
        tally(matrix.at[pl.ds(0, depth), :], oc_out, oc_in.at[0]).wait_send()
        tally(landed, p_out, p_in.at[0, 0]).wait_send()
        for d in range(last):
            for up in (True, False):

                @pl.when(sends(up, d))
                def _():
                    index = slot(up, d) - 1
                    here = matrix.at[pl.ds(0, half), pl.ds(0, width)]
                    tally(here, oz_out.at[index], oz_in.at[index, 0]).wait_send()


def layer(sizes, tokens, norm_gain, shift, sources, gap, gain, w_out):
    n_grp, n_sp, n_tp = sizes
    n_x = n_tp // CORES
    span, seqs, model = tokens.shape
    length = n_sp * n_tp * span
    count = len(sources)
    depth, width = w_out.shape
    slots = 2 * n_sp - 1
    dma = pltpu.SemaphoreType.DMA
    hbm = pl.BlockSpec(memory_space=pltpu.HBM)
    vmem = pl.BlockSpec(memory_space=pltpu.VMEM)
    bf16 = jnp.bfloat16
    return pl.pallas_call(
        functools.partial(layer_kernel, sizes),
        out_shape=jax.ShapeDtypeStruct((seqs, span, n_sp * width), bf16),
        in_specs=[hbm] * (6 + count),
        out_specs=vmem,
        scratch_shapes=[
            pltpu.VMEM(norm_gain.shape, norm_gain.dtype),
            pltpu.VMEM(gap.shape, gap.dtype),
            pltpu.VMEM(gain.shape, gain.dtype),
            pltpu.VMEM(tokens.shape, bf16),
            pltpu.VMEM(tokens.shape, jnp.float32),
            pltpu.VMEM(shift.shape, shift.dtype),
            pltpu.VMEM((n_sp, seqs, n_tp * span, KEY), bf16),
            pltpu.VMEM((seqs, length, KEY), bf16),
            pltpu.VMEM((seqs, length, model), bf16),
            pltpu.VMEM((model, count * KEY), bf16),
            pltpu.VMEM((seqs, length, count * KEY), jnp.float32),
            pltpu.VMEM((seqs, length, count * KEY), bf16),
            pltpu.VMEM((2, length, VAL), jnp.float32),
            pltpu.VMEM((seqs, n_sp, n_x, CORES, span, VAL), bf16),
            pltpu.VMEM((n_x, seqs, span, CORES * depth), bf16),
            pltpu.VMEM((CORES * depth, n_sp * width), bf16),
            pltpu.VMEM((n_x, seqs, span, n_sp * width), bf16),
            pltpu.VMEM((seqs, span, n_sp * width), bf16),
            dma((7,)),
            dma((slots - 1,)),
            dma((slots - 1, PIECES)),
            dma,
            dma((slots,)),
            dma,
            dma,
            dma,
            dma((n_sp - 1, count)),
            dma,
            dma((4,)),
            dma,
            dma,
            dma((slots - 1,)),
            dma((slots - 1, BITS)),
            dma,
            dma((slots - 1, BITS // 2)),
            dma,
            dma((slots,)),
            dma,
            dma((PIECES,)),
            dma,
            dma((slots, PIECES)),
        ],
        compiler_params=pltpu.CompilerParams(
            collective_id=0, has_side_effects=True, vmem_limit_bytes=int(VL * 1024 * 1024)
        ),
    )(tokens, norm_gain, shift, *sources, gap, gain, w_out)


def head_shards(
    sizes,
    tokens,
    norm_gain,
    w_query,
    w_value,
    w_fwd_gate,
    w_bwd_gate,
    w_out_gate,
    floor_gap,
    decay_shift,
    head_gain,
    w_out,
):
    return layer(
        sizes,
        tokens,
        norm_gain.reshape(1, 1, -1),
        decay_shift,
        (w_query, w_value, w_fwd_gate, w_bwd_gate, w_out_gate),
        floor_gap,
        head_gain.reshape(1, VAL),
        w_out,
    ).transpose(1, 0, 2)


def by_heads(mesh):
    n_sp, n_tp = mesh.shape["sp"], mesh.shape["tp"]

    def run(*arrays):
        tokens, w_query = arrays[0], arrays[2]
        heads_here = w_query.shape[1] // KEY // n_tp
        span = tokens.shape[0] // (n_sp * n_tp)
        sizes = (mesh.shape["grp"], n_sp, n_tp)
        fits = heads_here == n_sp and n_sp == CORES * 2 and n_tp == 2 * CORES and span % 16 == 0
        fits = fits and sizes[0] == 2 and tokens.shape[1] // sizes[0] % PIECES == 0
        fits = fits and tokens.shape[0] % BLOCK == 0 and tokens.shape[0] <= 512
        body = functools.partial(head_shards, sizes) if fits else shards
        return mapped(body, mesh)(*arrays)

    return run


def mapped(body, mesh):
    return jax.shard_map(
        body,
        mesh=mesh,
        in_specs=(
            P(("sp", "tp"), "grp", None),
            P(),
            P("sp", "tp"),
            P("sp", "tp"),
            P("sp", "tp"),
            P("sp", "tp"),
            P("sp", "tp"),
            P(None, "tp"),
            P("sp", "grp", "tp"),
            P(),
            P("tp", "sp"),
        ),
        out_specs=P(("sp", "tp"), "grp", None),
        check_vma=False,
    )


def solution(mesh):
    return by_heads(mesh)
```
